32 devices in a mesh: sp: 8 (over z, x), tp: 4 (over y, core).
Axes of the slice: x: 2, y: 2, z: 4, core: 2. Of those that a mesh axis runs over, the one named last changes fastest.
Arguments:
- layer_input: bfloat16 [1024, 2048], P('sp', 'tp'), may hold values from -6 to 6
- cotangent: bfloat16 [1024, 2048], P('sp', 'tp'), may hold values from -6 to 6
- routes: int32 [1024, 2], P('sp'), may hold values from 0 to 7, all different within a row; in each aligned block of 128 rows (0 to 127, 128 to 255, ...) at most 48 rows name the same one
- route_weight: float32 [1024, 2], P('sp'), may hold values from 0.1 to 0.6
- gate_weight: bfloat16 [8, 2048, 1024], P('sp', None, 'tp'), may hold values from -0.125 to 0.125
- up_weight: bfloat16 [8, 2048, 1024], P('sp', None, 'tp'), may hold values from -0.125 to 0.125
- down_weight: bfloat16 [8, 1024, 2048], P('sp', 'tp'), may hold values from -0.1875 to 0.1875
- heads_value: bfloat16 [1024, 2048], P('sp', 'tp'), may hold values from -6 to 6
- output_gate: bfloat16 [1024, 2048], P('sp', 'tp'), may hold values from -8 to 8
- mixer_saved: bfloat16 [1024, 2048], P('sp', 'tp'), may hold values from -6 to 6
- proj_weight: bfloat16 [2048, 2048], P(None, 'tp'), may hold values from -0.125 to 0.125
- state_write: bfloat16 [1024, 512], P('sp', 'tp'), may hold values from -0.5 to 0.5
- state_read: bfloat16 [1024, 512], P('sp', 'tp'), may hold values from -0.5 to 0.5
- decay_rate: float32 [1024, 32], P('sp', 'tp'), may hold values from 0 to 1.1, as said below
Outputs:
- gate_grad: bfloat16 [8, 2048, 1024], P('sp', None, 'tp')
- up_grad: bfloat16 [8, 2048, 1024], P('sp', None, 'tp')
- down_grad: bfloat16 [8, 1024, 2048], P('sp', 'tp')
- proj_grad: float32 [2048, 2048], P('sp', 'tp')
- value_grad: bfloat16 [1024, 2048], P('sp', 'tp')
- write_gradient: bfloat16 [1024, 512], P('sp', 'tp')
- read_gradient: bfloat16 [1024, 512], P('sp', 'tp')
- outgate_grad: bfloat16 [1024, 2048], P('sp', 'tp')
The draws below stay inside these ranges and needn't reach their ends.
Inputs may be any that keep to these rules, and one draw needn't show every extreme that they name: `routes`: each row names 2 different experts; within the rows of one aligned block of 128 tokens no expert is named by more than 48 rows, a bound that some block reaches. `decay_rate`: positive log-decays.
All inputs are finite; a program needn't handle non-finite values.
Results may differ from the reference program's by a relative error of at most 0.017.
Values may be sent and summed in bfloat16 or wider, within the bound.
A program may use at most 128 MiB of HBM per device.

```python
import math
import jax
import jax.numpy as jnp
import numpy as np
from jax import lax

D = 2048
BLENDER_CHANNEL = 32
HEAD_DIM = 64
GROUPS = 4
STATE = 128
EXP_HIDDEN = 1024
TOPK = 2
TOK_DEV = 128
SERIES_ENTRIES = 1024
EXPERTS = 8
CAP = 48
SSD_W = 2048
N_SP = 8
N_TP = 4


def draw_decay_rate(key, part):
    address_rows = jax.random.split(jax.random.fold_in(key, 11), 5)
    share = 0.5
    fast_heads = jax.random.uniform(address_rows[0], (BLENDER_CHANNEL,), jnp.float32) < share
    random_noise = jax.random.uniform(address_rows[1], (SERIES_ENTRIES, BLENDER_CHANNEL), jnp.float32, 0.5, 1.5)
    block_multiplier = jax.random.uniform(address_rows[2], (SERIES_ENTRIES // TOK_DEV, 1, 1), jnp.float32, 0.5, 1.5)
    block_multiplier = jnp.broadcast_to(block_multiplier, (SERIES_ENTRIES // TOK_DEV, TOK_DEV, 1)).reshape(SERIES_ENTRIES, 1)
    baseline_rate = jnp.where(fast_heads, 0.03, 0.5 / SERIES_ENTRIES)[None, :]
    interval_starts = jax.random.randint(address_rows[3], (2, BLENDER_CHANNEL), 0, SERIES_ENTRIES)
    interval_spans = jax.random.uniform(address_rows[4], (2, BLENDER_CHANNEL), jnp.float32, 0.22, 0.5)
    entry_indices = jnp.arange(SERIES_ENTRIES, dtype=jnp.int32)[:, None]
    pulse_clusters = jnp.where(entry_indices == interval_starts[0][None, :], interval_spans[0][None, :], 0.0)
    pulse_clusters = pulse_clusters + jnp.where(entry_indices == interval_starts[1][None, :], interval_spans[1][None, :], 0.0)
    pulse_clusters = jnp.where(fast_heads[None, :], 0.0, pulse_clusters)
    return (baseline_rate * random_noise * block_multiplier + pulse_clusters).astype(jnp.float32)


def raised(result, rng, source, target, shards_of, factor):
    def block_of(dim):
        return (jnp.arange(result.shape[dim]) // (result.shape[dim] // shards_of)).reshape((-1,) + (1,) * (result.ndim - 1 - dim))

    first = jax.random.permutation(rng, shards_of)[block_of(target)]
    second = (block_of(target) + shards_of // 2) % shards_of
    return jnp.where((block_of(source) == first) | (block_of(source) == second), factor * result, result)


def steps_of(rng, shape, cuts, least, high):
    def one(dim, blocks):
        heights = jax.random.uniform(jax.random.fold_in(jax.random.fold_in(rng, 6), dim), (blocks,), jnp.float32, least / len(cuts), high / len(cuts))
        return jnp.repeat(jnp.exp(heights), shape[dim] // blocks).reshape((-1,) + (1,) * (len(shape) - dim - 1))

    gain = one(*cuts[0])
    for cut in cuts[1:]:
        gain = gain * one(*cut)
    return gain


def deal_out(rng, own, number, rows, count, top, reach, skew):
    order = jax.random.permutation(rng, count)
    heavy_load, usual = shares(count, rows * top, reach, skew, True), shares(count, rows * top, reach, skew, False)
    places = jnp.arange(count)

    def named(tallies, offset_by):
        used = int((tallies > 0).sum())
        fixed = max(1, used // 4)
        moved = fixed + (places - fixed + offset_by * (used - fixed)) % max(1, count - fixed)
        return jnp.zeros((count,), jnp.int32).at[order[jnp.where(places < fixed, places, moved)]].set(jnp.asarray(tallies, jnp.int32))

    tallies = jnp.where(number % 4 == 0, named(heavy_load, number // 4), named(usual, number - number // 4 - 1))
    mixed = jax.random.permutation(jax.random.fold_in(own, 3), count)
    donor, taker = mixed[0:count // 2 * 2:2], mixed[1:count // 2 * 2:2]
    room = jnp.minimum(tallies[donor] - 1, reach - tallies[taker]) // 2
    room = jnp.where((donor == order[0]) | (taker == order[0]) | (tallies[taker] == 0), 0, jnp.maximum(room, 0))
    moved = jax.random.randint(jax.random.fold_in(own, 4), (count // 2,), 0, 1 << 20) % (room + 1)
    tallies = tallies.at[donor].add(-moved).at[taker].add(moved)
    items = jnp.searchsorted(jnp.cumsum(tallies), jnp.arange(rows * top), side="right").astype(jnp.int32)
    grid = items.reshape(top, rows).T
    grid = grid[jax.random.permutation(jax.random.fold_in(own, 1), rows)]
    offset_by = jax.random.randint(jax.random.fold_in(own, 2), (rows, 1), 0, top)
    return jnp.take_along_axis(grid, (jnp.arange(top)[None, :] + offset_by) % top, axis=1)


def shares(number_of, total, most, lean, full):
    weights = [(1 << 20) // math.isqrt(standing ** lean) + 1 for standing in range(1, number_of + 1)]
    largest = most if full else min(most, max(-(-total // number_of), total * weights[0] // sum(weights)))
    least = 1 if total - largest >= number_of - 1 else 0
    counts, surplus = [largest] + [least] * (number_of - 1), total - largest - least * (number_of - 1)
    while surplus > 0:
        free = [i for i in range(1, number_of) if counts[i] < largest] or [i for i in range(1, number_of) if counts[i] < most]
        pool, left = sum([weights[i] for i in free]), surplus
        for i in free:
            addition = min(most - counts[i], max(1, left * weights[i] // pool), surplus)
            counts[i] = counts[i] + addition
            surplus = surplus - addition
    return np.array(counts)


def gaussian(key, shape, deviation, limit, cuts=(), held_as=jnp.bfloat16):
    drawn = deviation * jax.random.normal(key, shape, jnp.float32)
    if cuts:
        drawn = drawn * steps_of(key, shape, cuts, -0.22, 0.18)
    return jnp.clip(drawn, -limit, limit).astype(held_as)


def heavy_noise(own_key, extent, deviation, reach, shards, heavy, held_as=jnp.bfloat16):
    array = deviation * jax.random.normal(own_key, extent, jnp.float32)
    if shards:
        array = array * steps_of(own_key, extent, shards, -0.22, 0.18)
    return jnp.clip(raised(array, jax.random.fold_in(own_key, 3), *heavy), -reach, reach).astype(held_as)


def setup_inputs(seed: int = 0) -> dict:
    seeds = jax.random.split(jax.random.key(seed), 15)
    layer_input = gaussian(seeds[0], (SERIES_ENTRIES, D), 1.0, 6.0, ((0, 8), (1, 4)))
    cotangent = heavy_noise(seeds[1], (SERIES_ENTRIES, D), 1.0, 6.0, ((0, 8), (1, 4)), (0, 1, 8, 2.0))
    routes_keys = jax.random.split(jax.random.fold_in(seeds[2], 1), SERIES_ENTRIES // TOK_DEV)
    routes_turns = jax.random.permutation(jax.random.fold_in(seeds[2], 3), SERIES_ENTRIES // TOK_DEV)
    routes = jax.vmap(lambda own, number: deal_out(jax.random.fold_in(seeds[2], 2), own, number, TOK_DEV, EXPERTS, TOPK, CAP, 1))(routes_keys, routes_turns).reshape((SERIES_ENTRIES, TOPK))
    route_weight = jnp.clip(0.1 + 0.5 * jax.random.uniform(seeds[3], (SERIES_ENTRIES, TOPK), jnp.float32) ** steps_of(seeds[3], (SERIES_ENTRIES, TOPK), ((0, 8),), -0.2, 0.2), 0.1, 0.6)
    gate_weight = gaussian(seeds[4], (EXPERTS, D, EXP_HIDDEN), D ** -0.5, 0.125, ((0, 8), (2, 4)))
    up_weight = gaussian(seeds[5], (EXPERTS, D, EXP_HIDDEN), D ** -0.5, 0.125, ((0, 8), (2, 4)))
    down_weight = gaussian(seeds[6], (EXPERTS, EXP_HIDDEN, D), EXP_HIDDEN ** -0.5, 0.1875, ((0, 8), (1, 4)))
    heads_value = gaussian(seeds[7], (SERIES_ENTRIES, SSD_W), 1.0, 6.0, ((0, 8), (1, 4)))
    output_gate = gaussian(seeds[8], (SERIES_ENTRIES, SSD_W), 1.5, 8.0, ((0, 8), (1, 4)))
    mixer_saved = gaussian(seeds[9], (SERIES_ENTRIES, SSD_W), 1.0, 6.0, ((0, 8), (1, 4)))
    proj_weight = gaussian(seeds[10], (D, SSD_W), SSD_W ** -0.5, 0.125, ((1, 4),))
    state_write = gaussian(seeds[11], (SERIES_ENTRIES, GROUPS * STATE), 0.08, 0.5, ((0, 8), (1, 4)))
    state_read = gaussian(seeds[12], (SERIES_ENTRIES, GROUPS * STATE), 0.08, 0.5, ((0, 8), (1, 4)))
    decay_rate = draw_decay_rate(jax.random.fold_in(seeds[14], 71), 0)
    return dict(layer_input=layer_input, cotangent=cotangent, routes=routes, route_weight=route_weight, gate_weight=gate_weight, up_weight=up_weight, down_weight=down_weight, heads_value=heads_value, output_gate=output_gate, mixer_saved=mixer_saved, proj_weight=proj_weight, state_write=state_write, state_read=state_read, decay_rate=decay_rate)


maximal_value = lax.Precision.HIGHEST


def silu_parts(value):
    sigma = jax.nn.sigmoid(value)
    return value * sigma, sigma * (1.0 + value * (1.0 - sigma))


def slot_index(flat_routes):
    onehot = (flat_routes[:, None] == jnp.arange(EXPERTS, dtype=jnp.int32)[None, :]).astype(jnp.int32)
    before = jnp.cumsum(onehot, axis=0, dtype=jnp.int32) - onehot
    ranks = jnp.sum(before * onehot, axis=1, dtype=jnp.int32)
    return (flat_routes * CAP + ranks).astype(jnp.int32)


def block_sums(block):
    value_vectors, step_deltas, write_vectors, read_vectors, rates = block
    repeat = BLENDER_CHANNEL // GROUPS
    cumul = jnp.cumsum(rates, axis=0)
    total = cumul[-1]
    to_end = jnp.exp(cumul - total)
    to_start = jnp.exp(-cumul)
    write_heads = jnp.repeat(write_vectors, repeat, axis=1)
    read_heads = jnp.repeat(read_vectors, repeat, axis=1)
    write_end = jnp.einsum('shn,shp->hnp', write_heads * to_end[:, :, None], value_vectors, precision=maximal_value)
    read_end = jnp.einsum('shn,shp->hnp', read_heads * to_end[:, :, None], step_deltas, precision=maximal_value)
    write_start = jnp.einsum('shn,shp->hnp', write_heads * to_start[:, :, None], value_vectors, precision=maximal_value)
    read_start = jnp.einsum('shn,shp->hnp', read_heads * to_start[:, :, None], step_deltas, precision=maximal_value)
    return total, write_end, read_end, write_start, read_start


def block_grads(item):
    value_vectors, step_deltas, write_vectors, read_vectors, rates, write_low, read_low, write_high, read_high = item
    repeat = BLENDER_CHANNEL // GROUPS
    length = value_vectors.shape[0]
    cumul = jnp.cumsum(rates, axis=0)
    to_end = jnp.exp(cumul - cumul[-1])
    to_start = jnp.exp(-cumul)
    write_heads = jnp.repeat(write_vectors, repeat, axis=1)
    read_heads = jnp.repeat(read_vectors, repeat, axis=1)
    mixing_kernel = jnp.exp(-jnp.abs(cumul.T[:, :, None] - cumul.T[:, None, :]))
    common_part = jnp.repeat(jnp.einsum('tgn,sgn->gts', read_vectors, write_vectors, precision=maximal_value), repeat, axis=0)
    match_scores = jnp.einsum('thp,shp->hts', step_deltas, value_vectors, precision=maximal_value)
    weighted_values = mixing_kernel * match_scores
    value_g = jnp.einsum('hts,thp->shp', mixing_kernel * common_part, step_deltas, precision=maximal_value)
    write_g = jnp.einsum('hts,thn->shn', weighted_values, read_heads, precision=maximal_value)
    read_g = jnp.einsum('hts,shn->thn', weighted_values, write_heads, precision=maximal_value)
    value_g = value_g + jnp.einsum('hnp,thn->thp', read_low, write_heads, precision=maximal_value) * to_start[:, :, None]
    value_g = value_g + jnp.einsum('hnp,thn->thp', read_high, write_heads, precision=maximal_value) * to_end[:, :, None]
    write_g = write_g + jnp.einsum('hnp,thp->thn', read_low, value_vectors * to_start[:, :, None], precision=maximal_value)
    write_g = write_g + jnp.einsum('hnp,thp->thn', read_high, value_vectors * to_end[:, :, None], precision=maximal_value)
    read_g = read_g + jnp.einsum('hnp,thp->thn', write_low, step_deltas * to_start[:, :, None], precision=maximal_value)
    read_g = read_g + jnp.einsum('hnp,thp->thn', write_high, step_deltas * to_end[:, :, None], precision=maximal_value)
    write_g = write_g.reshape(length, GROUPS, repeat, STATE).sum(axis=2)
    read_g = read_g.reshape(length, GROUPS, repeat, STATE).sum(axis=2)
    return value_g, write_g, read_g


def reference(layer_input, cotangent, routes, route_weight, gate_weight, up_weight, down_weight,
              heads_value, output_gate, mixer_saved, proj_weight, state_write, state_read, decay_rate):
    flat = routes.reshape(N_SP, TOK_DEV * TOPK)
    slots = jax.vmap(slot_index)(flat)
    owners = jnp.arange(TOK_DEV * TOPK, dtype=jnp.int32) // TOPK
    offsets = (jnp.arange(N_SP, dtype=jnp.int32) * TOK_DEV)[:, None]

    def slot_tokens(slot_row, offset_row):
        return jnp.full((EXPERTS * CAP,), SERIES_ENTRIES, jnp.int32).at[slot_row].set(owners + offset_row)

    def slot_weights(slot_row, weight_row):
        return jnp.zeros((EXPERTS * CAP,), jnp.float32).at[slot_row].set(weight_row)

    token_table = jax.vmap(slot_tokens)(slots, offsets)
    weight_table = jax.vmap(slot_weights)(slots, route_weight.reshape(N_SP, TOK_DEV * TOPK))
    token_table = token_table.reshape(N_SP, EXPERTS, CAP).transpose(1, 0, 2).reshape(EXPERTS, N_SP * CAP)
    weight_table = weight_table.reshape(N_SP, EXPERTS, CAP).transpose(1, 0, 2).reshape(EXPERTS, N_SP * CAP)
    inputs_pad = jnp.concatenate([layer_input, jnp.zeros((1, D), layer_input.dtype)], axis=0)
    cotangent_pad = jnp.concatenate([cotangent, jnp.zeros((1, D), cotangent.dtype)], axis=0)
    width = EXP_HIDDEN // N_TP

    def expert_step(item):
        rows, weights, gate_one, up_one, down_one = item
        inputs = inputs_pad[rows]
        sent = (cotangent_pad[rows].astype(jnp.float32) * weights[:, None]).astype(jnp.bfloat16)
        pre_gate = jnp.dot(inputs, gate_one, preferred_element_type=jnp.float32)
        pre_up = jnp.dot(inputs, up_one, preferred_element_type=jnp.float32)
        active, slope = silu_parts(pre_gate)
        hidden = (active * pre_up).astype(jnp.bfloat16)
        hidden_grad = jnp.dot(sent, down_one.T, preferred_element_type=jnp.float32)
        gate_delta = (hidden_grad * pre_up * slope).astype(jnp.bfloat16)
        up_delta = (hidden_grad * active).astype(jnp.bfloat16)
        down_g = jnp.dot(hidden.T, sent, preferred_element_type=jnp.float32).astype(jnp.bfloat16)
        gate_g = jnp.dot(inputs.T, gate_delta, preferred_element_type=jnp.float32).astype(jnp.bfloat16)
        up_g = jnp.dot(inputs.T, up_delta, preferred_element_type=jnp.float32).astype(jnp.bfloat16)
        parts = jnp.einsum('rjk,djk->jrd', gate_delta.reshape(-1, N_TP, width).astype(jnp.float32),
                           gate_one.reshape(D, N_TP, width).astype(jnp.float32))
        parts = parts + jnp.einsum('rjk,djk->jrd', up_delta.reshape(-1, N_TP, width).astype(jnp.float32),
                                   up_one.reshape(D, N_TP, width).astype(jnp.float32))
        rounded = lax.optimization_barrier(parts.astype(jnp.bfloat16)).astype(jnp.float32)
        returned = jnp.sum(rounded, axis=0).astype(jnp.bfloat16)
        return gate_g, up_g, down_g, returned

    gate_grad, up_grad, down_grad, returned = lax.map(
        expert_step, (token_table, weight_table, gate_weight, up_weight, down_weight))
    expert_of = slots // CAP
    rank_of = slots % CAP
    sources = jnp.arange(N_SP, dtype=jnp.int32)[:, None]
    position = (expert_of * (N_SP * CAP) + sources * CAP + rank_of).astype(jnp.int32).reshape(-1)
    moe_grad = returned.reshape(-1, D)[position].astype(jnp.float32).reshape(SERIES_ENTRIES, TOPK, D).sum(axis=1)
    layer_grad = (cotangent.astype(jnp.float32) + moe_grad).astype(jnp.bfloat16)

    out_delta = jnp.dot(layer_grad, proj_weight, preferred_element_type=jnp.float32).astype(jnp.bfloat16)
    active_gate, slope_gate = silu_parts(output_gate.astype(jnp.float32))
    saved = mixer_saved.astype(jnp.float32)
    gated = (saved * active_gate).astype(jnp.bfloat16)
    proj_grad = jnp.dot(layer_grad.T, gated, preferred_element_type=jnp.float32)
    outgate_grad = (out_delta.astype(jnp.float32) * saved * slope_gate).astype(jnp.bfloat16)
    mixer_delta = out_delta.astype(jnp.float32) * active_gate

    blk = math.gcd(TOK_DEV, 256)
    count = SERIES_ENTRIES // blk
    value_vectors = heads_value.astype(jnp.float32).reshape(count, blk, BLENDER_CHANNEL, HEAD_DIM)
    step_deltas = mixer_delta.reshape(count, blk, BLENDER_CHANNEL, HEAD_DIM)
    write_vectors = state_write.astype(jnp.float32).reshape(count, blk, GROUPS, STATE)
    read_vectors = state_read.astype(jnp.float32).reshape(count, blk, GROUPS, STATE)
    rates = decay_rate.astype(jnp.float32).reshape(count, blk, BLENDER_CHANNEL)
    totals, write_end, read_end, write_start, read_start = lax.map(block_sums, (value_vectors, step_deltas, write_vectors, read_vectors, rates))
    zero_state = jnp.zeros((BLENDER_CHANNEL, STATE, HEAD_DIM), jnp.float32)

    def carry_on(state, item):
        total, write_part, read_part = item
        fade = jnp.exp(-total)[:, None, None]
        return (fade * state[0] + write_part, fade * state[1] + read_part), state

    _, (write_low, read_low) = lax.scan(carry_on, (zero_state, zero_state), (totals, write_end, read_end))
    _, (write_high, read_high) = lax.scan(carry_on, (zero_state, zero_state), (totals, write_start, read_start), reverse=True)
    value_g, write_g, read_g = lax.map(block_grads, (value_vectors, step_deltas, write_vectors, read_vectors, rates,
                                                     write_low, read_low, write_high, read_high))
    return (gate_grad, up_grad, down_grad, proj_grad,
            value_g.reshape(SERIES_ENTRIES, SSD_W).astype(jnp.bfloat16),
            write_g.reshape(SERIES_ENTRIES, GROUPS * STATE).astype(jnp.bfloat16),
            read_g.reshape(SERIES_ENTRIES, GROUPS * STATE).astype(jnp.bfloat16),
            outgate_grad)
```

```python
import functools

import jax
import jax.numpy as jnp
from jax import lax
from jax.experimental import pallas as pl
from jax.experimental.pallas import tpu as pltpu
from jax.sharding import PartitionSpec as P

HEAD_DIM = 64
STATE = 128
MESH = pl.DeviceIdType.MESH
LAST = (((1,), (1,)), ((), ()))
FIRST = (((0,), (0,)), ((), ()))
F32 = jnp.float32
BF16 = jnp.bfloat16
VMEM = pltpu.VMEM
DMA = pltpu.SemaphoreType.DMA


def silu_parts(value):
    sigma = jax.nn.sigmoid(value)
    return (value * sigma, sigma * (1.0 + value * (1.0 - sigma)))


def dot_first(a, b):
    return lax.dot_general(a, b, FIRST, preferred_element_type=F32)


def dot_last(a, b):
    return lax.dot_general(a, b, LAST, preferred_element_type=F32)


def dot(a, b):
    return jnp.dot(a, b, preferred_element_type=F32)


def flip(a, b, n):
    out, bit = 0, 1
    while bit < n:
        out = out + lax.rem(lax.div(a, bit) + lax.div(b, bit), 2) * bit
        bit *= 2
    return out


class Place:
    def __init__(self, n, t):
        self.n, self.t = n, t
        self.sp = lax.axis_index("sp")
        self.tp = lax.axis_index("tp")
        self.across = lax.rem(self.tp + t // 2, t)
        self.beside = self.tp + 1 - 2 * lax.rem(self.tp, 2)
        self.cross = lax.rem(self.beside + t // 2, t)

    def mate(self, m):
        return flip(self.sp, jnp.int32(m), self.n)

    def to(self, src, dst, send, recv, sp=None, tp=None):
        return pltpu.make_async_remote_copy(
            src_ref=src,
            dst_ref=dst,
            send_sem=send,
            recv_sem=recv,
            device_id=(self.sp if sp is None else sp, self.tp if tp is None else tp),
            device_id_type=MESH,
        )

    def greet(self, sp_too=True):
        barrier = pltpu.get_barrier_semaphore()
        for tp in (self.across, self.beside):
            pl.semaphore_signal(barrier, inc=1, device_id=(self.sp, tp), device_id_type=MESH)
        count = 2
        if sp_too:
            for o in range(1, self.n):
                pl.semaphore_signal(
                    barrier,
                    inc=1,
                    device_id=(lax.rem(self.sp + o, self.n), self.tp),
                    device_id_type=MESH,
                )
            count += self.n - 1
        pl.semaphore_wait(barrier, count)


def loop(lo, hi, body):
    def step(i, carry):
        body(i)
        return carry

    lax.fori_loop(lo, hi, step, 0)


def expert_kernel(
    n, t, cap,
    routes, rweight, x_ref, c_ref, a_ref, gate_hbm, up_hbm, down_hbm,
    full, gate_grad, up_grad, down_grad, ao,
    snd, got, gate, up, down, pg, pu, hidden, gd, ud, part, pair, summed, other, final, arr, pick,
    w_sem, s_a2a, r_a2a, s_sh, r_sh, s_d, r_d, s_p, r_p, s_y, r_y, s_b, r_b, s_r, r_r,
):
    at = Place(n, t)
    tokens, d = x_ref.shape
    top = routes.shape[1]
    slots = n * cap
    half = n // 2
    duo = 2 * cap
    col = lambda tp: pl.ds(pl.multiple_of(tp * d, d), d)

    loads = [
        pltpu.make_async_copy(src.at[0], dst, w_sem.at[i])
        for i, (src, dst) in enumerate(((gate_hbm, gate), (up_hbm, up), (down_hbm, down)))
    ]
    for load in loads:
        load.start()

    barrier = pltpu.get_barrier_semaphore()
    for tp in (at.across, at.beside):
        pl.semaphore_signal(barrier, inc=1, device_id=(at.sp, tp), device_id_type=MESH)

    def hello(o):
        pl.semaphore_signal(
            barrier, inc=1, device_id=(lax.rem(at.sp + o, n), at.tp), device_id_type=MESH
        )

    loop(1, n, hello)

    named = routes[...]
    lanes = lax.broadcasted_iota(jnp.int32, (tokens, n), 1)
    onehot = [(named[:, k : k + 1] == lanes).astype(F32) for k in range(top)]
    lower = (
        lax.broadcasted_iota(jnp.int32, (tokens, tokens), 0)
        > lax.broadcasted_iota(jnp.int32, (tokens, tokens), 1)
    ).astype(F32)
    before = dot(lower.astype(BF16), sum(onehot).astype(BF16))
    slot_lane = lax.broadcasted_iota(jnp.int32, (tokens, slots), 1)
    picks = []
    for k in range(top):
        rank = jnp.sum(before * onehot[k], axis=1, keepdims=True).astype(jnp.int32)
        picks.append((named[:, k : k + 1] * cap + rank == slot_lane).astype(F32).astype(BF16))
    pick[...] = sum(picks)
    snd[0] = dot_first(pick[...], x_ref[...]).astype(BF16).reshape(n, cap, d)
    cot = c_ref[...].astype(F32)
    weights = rweight[...]
    weighted = [(cot * weights[:, k : k + 1]).astype(BF16) for k in range(top)]
    snd[1] = dot_first(
        jnp.concatenate(picks, axis=0), jnp.concatenate(weighted, axis=0)
    ).astype(BF16).reshape(n, cap, d)
    for k in (0, 1):
        got[k, 0, :, col(at.tp)] = snd[k, at.sp]
    ao[at.sp] = a_ref[...]
    pl.semaphore_wait(barrier, n + 1)

    def place_of(i):
        return jnp.where(i < 2, i, n + 1 - i)

    def spread(k, m):
        mate = at.mate(m)
        return at.to(
            snd.at[k, mate], got.at[k, m, :, col(at.tp)], s_a2a.at[k, m], r_a2a.at[k, m], sp=mate
        )

    def decay(m):
        mate = at.mate(m)
        return at.to(a_ref, ao.at[at.sp], s_d.at[m], r_d.at[m], sp=mate)

    def share(k, m, j):
        here = got.at[k, m, :, col(at.across if j == 2 else at.tp)]
        return at.to(
            here, here, s_sh.at[k, j, m], r_sh.at[k, j, m], tp=at.across if j == 0 else at.beside
        )

    for k in (0, 1):
        loop(1, n, lambda i: spread(k, place_of(i)).start())
    for k in (0, 1):
        share(k, 0, 0).start()
        share(k, 0, 1).start()
    loop(1, n, lambda m: decay(m).start())

    lag = 2

    def forward(q):
        k, i = lax.div(q, n), lax.rem(q, n)
        m = place_of(i)

        @pl.when(i > 0)
        def _():
            spread(k, m).wait_recv()
            share(k, m, 0).start()
            share(k, m, 1).start()

        @pl.when(q >= lag)
        def _():
            relay(q - lag)

    def relay(q):
        k, m = lax.div(q, n), place_of(lax.rem(q, n))
        share(k, m, 0).wait_recv()
        share(k, m, 2).start()

    def base_of(j):
        return jnp.where(j < 1, 0, half - j)

    def settled(k, base):
        for m in (2 * base, 2 * base + 1):
            share(k, m, 1).wait_recv()
            share(k, m, 2).wait_recv()

    def rows_of(base):
        return pl.ds(pl.multiple_of(base * duo, duo), duo)

    def ahead(j):
        base = base_of(j)
        settled(0, base)
        rows = rows_of(base)
        inputs = got[0, pl.ds(2 * base, 2)].reshape(duo, t * d)
        pg[rows, :] = dot(inputs, gate[...])
        pu[rows, :] = dot(inputs, up[...])

    def behind(j):
        base = base_of(j)
        settled(1, base)
        rows = rows_of(base)
        sent = got[1, pl.ds(2 * base, 2)].reshape(duo, t * d)
        grad = dot_last(sent, down[...])
        active, slope = silu_parts(pg[rows, :])
        ups = pu[rows, :]
        hidden[rows, :] = (active * ups).astype(BF16)
        gd[rows, :] = (grad * ups * slope).astype(BF16)
        ud[rows, :] = (grad * active).astype(BF16)

    loop(1, n, forward)
    for load in loads:
        load.wait()

    def second(j):
        forward(n + 2 * j)
        forward(n + 2 * j + 1)
        ahead(j)

        @pl.when(j > 0)
        def _():
            behind(j - 1)

    loop(0, half, second)
    loop(2 * n - lag, 2 * n, relay)
    behind(half - 1)

    def halves(m, k):
        c = at.cross if k == 0 else at.beside
        return at.to(
            part.at[m, :, col(c)], pair.at[k, m], s_p.at[k, m], r_p.at[k, m], tp=at.beside
        )

    def over(m):
        return at.to(summed.at[m], other.at[m], s_y.at[m], r_y.at[m], tp=at.across)

    def back(m):
        return at.to(final.at[m], arr.at[at.sp], s_b.at[m], r_b.at[m], sp=at.mate(m))

    def produce(jj):
        base = half - 1 - jj
        rows = rows_of(base)
        for c in range(t):
            cols = slice(c * d, (c + 1) * d)
            value = dot_last(gd[rows, :], gate[cols, :]) + dot_last(ud[rows, :], up[cols, :])
            part[pl.ds(2 * base, 2), :, cols] = value.astype(BF16).reshape(2, cap, d)
        for m in (2 * base + 1, 2 * base):
            for k in (0, 1):
                halves(m, k).start()

    def pass_over(jj):
        base = half - 1 - jj
        for m in (2 * base + 1, 2 * base):
            halves(m, 0).wait_recv()
            summed[m] = (
                part[m, :, col(at.across)].astype(F32) + pair[0, m].astype(F32)
            ).astype(BF16)
            over(m).start()

    def total(jj):
        base = half - 1 - jj
        for m in (2 * base + 1, 2 * base):
            halves(m, 1).wait_recv()
            over(m).wait_recv()
            final[m] = (
                part[m, :, col(at.tp)].astype(F32) + pair[1, m].astype(F32) + other[m].astype(F32)
            ).astype(BF16)

            @pl.when(m > 0)
            def _():
                back(m).start()

    def first_turn(jj):
        produce(jj)

        @pl.when(jj > 0)
        def _():
            pass_over(jj - 1)

    def weight_grads(c):
        cols = pl.ds(pl.multiple_of(c * d, d), d)
        inputs = got[0, :, :, cols].reshape(slots, d)
        gate_grad[cols, :] = dot_first(inputs, gd[...]).astype(BF16)
        up_grad[cols, :] = dot_first(inputs, ud[...]).astype(BF16)
        sent = got[1, :, :, cols].reshape(slots, d)
        down_grad[:, cols] = dot_first(hidden[...], sent).astype(BF16)

    loop(0, half, first_turn)
    pass_over(half - 1)

    def last_turn(jj):
        total(jj)

        @pl.when(jj < t)
        def _():
            weight_grads(jj)

    loop(0, half, last_turn)
    for c in range(half, t):
        weight_grads(c)
    arr[at.sp] = final[0]
    loop(1, n, lambda i: back(n - i).wait_recv())

    moe_grad = dot(pick[...], arr[...].reshape(slots, d))
    full[:, col(at.tp)] = (c_ref[...].astype(F32) + moe_grad).astype(BF16)

    def rows_to(j):
        here = full.at[:, col(at.across if j == 2 else at.tp)]
        return at.to(here, here, s_r.at[j], r_r.at[j], tp=at.across if j == 0 else at.beside)

    rows_to(0).start()
    rows_to(1).start()
    rows_to(0).wait_recv()
    rows_to(2).start()

    def finish(m):
        for k in (0, 1):
            for j in (0, 1, 2):
                share(k, m, j).wait_send()
            halves(m, k).wait_send()
        over(m).wait_send()

    loop(0, n, finish)

    def finish_sp(m):
        for k in (0, 1):
            spread(k, m).wait_send()
        back(m).wait_send()
        decay(m).wait()

    loop(1, n, finish_sp)
    rows_to(1).wait_recv()
    rows_to(2).wait_recv()
    for j in (0, 1, 2):
        rows_to(j).wait_send()


def late_kernel(n, t, *refs):
    wide = (1, 2)
    count = 5
    ins, g_ref, outs, gall = refs[:count], refs[count], refs[6 : 6 + count], refs[11]
    s_g, r_g, s_sh, r_sh, s_x, r_x, s_l, r_l, s_t, r_t, own = refs[12:]
    at = Place(n, t)
    q = g_ref.shape[1] // t
    row = lambda tp: pl.ds(pl.multiple_of(tp * q, q), q)
    length = n // 2
    z = at.sp // 2
    bit = lax.rem(at.sp, 2)
    twin = z * 2 + 1 - bit
    at.greet()
    keeps = [
        pltpu.make_async_copy(ins[a], outs[a].at[at.sp], own.at[a]) for a in range(count)
    ]
    keeps.append(pltpu.make_async_copy(g_ref.at[at.sp], gall.at[at.sp], own.at[count]))
    for keep in keeps:
        keep.start()
    pairs = [
        at.to(ins[a], outs[a].at[at.sp], s_x.at[a], r_x.at[a], sp=twin) for a in range(count)
    ]

    def spread(o):
        peer = lax.rem(at.sp + o, n)
        return at.to(
            g_ref.at[peer, row(at.tp), :],
            gall.at[at.sp, row(at.tp), :],
            s_g.at[o],
            r_g.at[o],
            sp=peer,
        )

    def share(o, j):
        here = gall.at[lax.rem(at.sp + n - o, n), row(at.across if j == 2 else at.tp), :]
        return at.to(
            here, here, s_sh.at[j, o], r_sh.at[j, o], tp=at.across if j == 0 else at.beside
        )

    def block_of(up, k, same):
        return (z - k if up else z + k) * 2 + (bit if same else 1 - bit)

    def hop(a, up, k, same):
        here = outs[a].at[block_of(up, k, same)]
        i, j = (0 if up else 1), (0 if same else 1)
        peer = z + 1 if up else z - 1
        return at.to(here, here, s_l.at[a, i, j, k], r_l.at[a, i, j, k], sp=peer * 2 + bit)

    def came(a, up, k, same):
        here = outs[a].at[block_of(up, k, same)]
        i, j = (0 if up else 1), (0 if same else 1)
        return at.to(here, here, s_l.at[a, i, j, k], r_l.at[a, i, j, k - 1], sp=twin)

    def side(a, up, k):
        here = outs[a].at[block_of(up, k, True)]
        i = 0 if up else 1
        return at.to(here, here, s_t.at[a, i, k], r_t.at[a, i, k], sp=twin)

    def sides_of(a):
        return (True,) if a in wide else (True, False)

    for a in range(count):
        if a not in wide:
            pairs[a].start()
    loop(1, n, lambda o: spread(o).start())
    order = wide + tuple(a for a in range(count) if a not in wide)

    def begin(a, same):
        @pl.when(z < length - 1)
        def _():
            hop(a, True, 0, same).start()

        @pl.when(z > 0)
        def _():
            hop(a, False, 0, same).start()

    for a in order:
        keeps[a].wait()
        begin(a, True)
    for a in order:
        if a in wide:
            pairs[a].start()
        else:
            pairs[a].wait_recv()
            begin(a, False)

    def arrive(o):
        spread(o).wait_recv()
        share(o, 0).start()
        share(o, 1).start()

    def advance(k):
        for a in order:
            for same in sides_of(a):

                @pl.when(z - k >= 0)
                def _():
                    came(a, True, k, same).wait_recv()

                    @pl.when(z < length - 1)
                    def _():
                        hop(a, True, k, same).start()

                    if a in wide:
                        side(a, True, k).start()

                @pl.when(z + k < length)
                def _():
                    came(a, False, k, same).wait_recv()

                    @pl.when(z > 0)
                    def _():
                        hop(a, False, k, same).start()

                    if a in wide:
                        side(a, False, k).start()

    loop(1, length, advance)
    keeps[count].wait()
    loop(1, n, arrive)

    def onward(o):
        share(o, 0).wait_recv()
        share(o, 2).start()

    loop(1, n, onward)

    def finish(o):
        share(o, 1).wait_recv()
        share(o, 2).wait_recv()
        for j in (0, 1, 2):
            share(o, j).wait_send()
        spread(o).wait_send()

    loop(1, n, finish)

    def drain(k):
        for a in order:
            for same in sides_of(a):

                @pl.when(jnp.logical_and(z - k >= 0, z < length - 1))
                def _():
                    hop(a, True, k, same).wait_send()

                @pl.when(jnp.logical_and(z + k < length, z > 0))
                def _():
                    hop(a, False, k, same).wait_send()

    loop(0, length, drain)

    def settle(k):
        for a in wide:

            @pl.when(z - k >= 0)
            def _():
                side(a, True, k).wait()

            @pl.when(z + k < length)
            def _():
                side(a, False, k).wait()

    loop(1, length, settle)
    for a in range(count):
        if a in wide:
            pairs[a].wait_recv()
        pairs[a].wait_send()


def mixer_kernel(chunk, dall, vall, rall, wall, arow, acol, dl, vl, rl, wl, vg, wg, rg):
    heads = acol.shape[1]
    per = heads * STATE // wl.shape[1]
    total = dall.shape[0]
    vg_sum = [jnp.zeros((dl.shape[0], HEAD_DIM), F32) for _ in range(heads)]
    wg_sum = [jnp.zeros((dl.shape[0], STATE), F32) for _ in range(heads // per)]
    rg_sum = [jnp.zeros((dl.shape[0], STATE), F32) for _ in range(heads // per)]

    def dot_last(a, b):
        return lax.dot_general(a, b, LAST, preferred_element_type=F32)

    def step(i, carry):
        vg_sum, wg_sum, rg_sum = carry
        vg_sum, wg_sum, rg_sum = list(vg_sum), list(wg_sum), list(rg_sum)
        rows = pl.ds(pl.multiple_of(i * chunk, chunk), chunk)
        for g in range(heads // per):
            wide = slice(g * STATE, (g + 1) * STATE)
            read, write = rall[rows, wide], wall[rows, wide]
            common = dot_last(wl[:, wide], read)
            q1 = jnp.zeros((dl.shape[0], chunk), F32)
            q2 = jnp.zeros((dl.shape[0], chunk), F32)
            for h in range(g * per, (g + 1) * per):
                cols = slice(h * HEAD_DIM, (h + 1) * HEAD_DIM)
                delta, value = dall[rows, cols], vall[rows, cols]
                fade = jnp.exp(-jnp.abs(acol[:, h : h + 1] - arow[h : h + 1, rows]))
                vg_sum[h] += jnp.dot(
                    (fade * common).astype(BF16), delta, preferred_element_type=F32
                )
                q1 += fade * dot_last(vl[:, cols], delta)
                q2 += fade * dot_last(dl[:, cols], value)
            wg_sum[g] += jnp.dot(q1.astype(BF16), read, preferred_element_type=F32)
            rg_sum[g] += jnp.dot(q2.astype(BF16), write, preferred_element_type=F32)
        return tuple(vg_sum), tuple(wg_sum), tuple(rg_sum)

    vg_sum, wg_sum, rg_sum = lax.fori_loop(
        0, total // chunk, step, (tuple(vg_sum), tuple(wg_sum), tuple(rg_sum))
    )
    for h in range(heads):
        vg[:, h * HEAD_DIM : (h + 1) * HEAD_DIM] = vg_sum[h].astype(BF16)
    for g in range(heads // per):
        wg[:, g * STATE : (g + 1) * STATE] = wg_sum[g].astype(BF16)
        rg[:, g * STATE : (g + 1) * STATE] = rg_sum[g].astype(BF16)


def call(kernel, ident, ins, outs, scratch, operands, name, any_from=None):
    vm = pl.BlockSpec(memory_space=pltpu.VMEM)
    return pl.pallas_call(
        kernel,
        out_shape=outs,
        in_specs=[
            vm if any_from is None or i < any_from else pl.BlockSpec(memory_space=pl.ANY)
            for i in range(len(operands))
        ],
        out_specs=jax.tree.map(lambda _: vm, outs),
        scratch_shapes=scratch,
        compiler_params=pltpu.CompilerParams(
            collective_id=ident,
            has_side_effects=ident is not None,
            vmem_limit_bytes=56 * 1024 * 1024,
        ),
        cost_estimate=pl.CostEstimate(
            flops=4_000_000_000, bytes_accessed=8_000_000, transcendentals=0
        ),
        name=name,
    )(*operands)


def on_device(
    layer_input,
    cotangent,
    routes,
    route_weight,
    gate_weight,
    up_weight,
    down_weight,
    heads_value,
    output_gate,
    mixer_saved,
    proj_weight,
    state_write,
    state_read,
    decay_rate,
):
    n = lax.axis_size("sp")
    t = lax.axis_size("tp")
    me = lax.axis_index("sp")
    tokens, d = layer_input.shape
    top = routes.shape[1]
    capacity = -(-max(2, 3 * tokens * top // (2 * n)) // 16) * 16
    slots_all = n * capacity
    sds = jax.ShapeDtypeStruct

    active_gate, slope_gate = silu_parts(output_gate.astype(F32))
    saved = mixer_saved.astype(F32)
    gated = (saved * active_gate).astype(BF16)
    decay_sum = jnp.cumsum(decay_rate, axis=0).T
    heads = decay_sum.shape[0]
    hid = gate_weight.shape[2]
    block = (n, capacity, d)
    full_grad, gate_grad, up_grad, down_grad, decays = call(
        functools.partial(expert_kernel, n, t, capacity),
        1,
        5,
        (
            sds((tokens, t * d), BF16),
            sds((t * d, hid), BF16),
            sds((t * d, hid), BF16),
            sds((hid, t * d), BF16),
            sds((n, heads, tokens), F32),
        ),
        [
            VMEM((2,) + block, BF16),
            VMEM((2, n, capacity, t * d), BF16),
            VMEM((t * d, hid), BF16),
            VMEM((t * d, hid), BF16),
            VMEM((hid, t * d), BF16),
            VMEM((slots_all, hid), F32),
            VMEM((slots_all, hid), F32),
            VMEM((slots_all, hid), BF16),
            VMEM((slots_all, hid), BF16),
            VMEM((slots_all, hid), BF16),
            VMEM((n, capacity, t * d), BF16),
            VMEM((2,) + block, BF16),
            VMEM(block, BF16),
            VMEM(block, BF16),
            VMEM(block, BF16),
            VMEM(block, BF16),
            VMEM((tokens, slots_all), BF16),
            DMA((3,)),
            DMA((2, n)),
            DMA((2, n)),
            DMA((2, 3, n)),
            DMA((2, 3, n)),
            DMA((n,)),
            DMA((n,)),
            DMA((2, n)),
            DMA((2, n)),
            DMA((n,)),
            DMA((n,)),
            DMA((n,)),
            DMA((n,)),
            DMA((3,)),
            DMA((3,)),
        ],
        (routes, route_weight, layer_input, cotangent, decay_sum, gate_weight, up_weight, down_weight),
        "experts",
        any_from=5,
    )
    out_delta = jnp.dot(full_grad, proj_weight, preferred_element_type=F32).astype(BF16)
    outgate_grad = (out_delta.astype(F32) * saved * slope_gate).astype(BF16)
    mixer_delta = (out_delta.astype(F32) * active_gate).astype(BF16)
    width = t * d // n
    by_owner = full_grad.reshape(tokens, n, width).transpose(1, 0, 2)
    length = max(1, n // 2)
    gathered = (mixer_delta, heads_value, gated, state_write, state_read)
    *gathered_all, all_grad = call(
        functools.partial(late_kernel, n, t),
        4,
        6,
        tuple(sds((n,) + x.shape, BF16) for x in gathered) + (sds((n, tokens, width), BF16),),
        [
            DMA((n,)),
            DMA((n,)),
            DMA((3, n)),
            DMA((3, n)),
            DMA((5,)),
            DMA((5,)),
            DMA((5, 2, 2, length)),
            DMA((5, 2, 2, length)),
            DMA((5, 2, length)),
            DMA((5, 2, length)),
            DMA((6,)),
        ],
        gathered + (by_owner,),
        "late",
    )
    all_delta, all_value, all_gated, all_write, all_read = (
        x.reshape(n * tokens, -1) for x in gathered_all
    )

    state_w = state_write.shape[1]
    proj_grad = lax.dot_general(
        all_grad.reshape(n * tokens, width), all_gated, FIRST, preferred_element_type=F32
    )
    totals = decays[:, :, -1]
    start = jnp.cumsum(totals, axis=0) - totals
    decay_row = (decays + start[:, :, None]).transpose(1, 0, 2)
    decay_here = lax.dynamic_index_in_dim(decay_row, me, axis=1, keepdims=False).T
    chunk = min(4, n) * tokens
    value_grad, write_gradient, read_gradient = call(
        functools.partial(mixer_kernel, chunk),
        None,
        10,
        (sds((tokens, d), BF16), sds((tokens, state_w), BF16), sds((tokens, state_w), BF16)),
        [],
        (
            all_delta,
            all_value,
            all_read,
            all_write,
            decay_row.reshape(heads, n * tokens),
            decay_here,
            mixer_delta,
            heads_value,
            state_read,
            state_write,
        ),
        "mixer",
    )
    return (
        gate_grad[None],
        up_grad[None],
        down_grad[None],
        proj_grad,
        value_grad,
        write_gradient,
        read_gradient,
        outgate_grad,
    )


def solution(mesh):
    split = P("sp", "tp")
    in_specs = (
        split,
        split,
        P("sp", None),
        P("sp", None),
        P("sp", None, "tp"),
        P("sp", None, "tp"),
        P("sp", "tp", None),
        split,
        split,
        split,
        P(None, "tp"),
        split,
        split,
        split,
    )
    out_specs = (
        P("sp", None, "tp"),
        P("sp", None, "tp"),
        P("sp", "tp", None),
        split,
        split,
        split,
        split,
        split,
    )
    return jax.shard_map(
        on_device, mesh=mesh, in_specs=in_specs, out_specs=out_specs, check_vma=False
    )
```

```python
import functools

import jax
import jax.numpy as jnp
from jax import lax
from jax.experimental import pallas as pl
from jax.experimental.pallas import tpu as pltpu
from jax.sharding import PartitionSpec as P

HEAD_DIM = 64
STATE = 128
MESH = pl.DeviceIdType.MESH
LAST = (((1,), (1,)), ((), ()))
FIRST = (((0,), (0,)), ((), ()))
F32 = jnp.float32
BF16 = jnp.bfloat16
VMEM = pltpu.VMEM
DMA = pltpu.SemaphoreType.DMA


def silu_parts(value):
    sigma = jax.nn.sigmoid(value)
    return (value * sigma, sigma * (1.0 + value * (1.0 - sigma)))


def dot_first(a, b):
    return lax.dot_general(a, b, FIRST, preferred_element_type=F32)


def dot_last(a, b):
    return lax.dot_general(a, b, LAST, preferred_element_type=F32)


def dot(a, b):
    return jnp.dot(a, b, preferred_element_type=F32)


def exact(a, b, dims=(((1,), (0,)), ((), ()))):
    return lax.dot_general(
        a, b, dims, precision=lax.Precision.HIGHEST, preferred_element_type=F32
    )


def flip(a, b, n):
    out, bit = 0, 1
    while bit < n:
        out = out + lax.rem(lax.div(a, bit) + lax.div(b, bit), 2) * bit
        bit *= 2
    return out


class Place:
    def __init__(self, n, t):
        self.n, self.t = n, t
        self.sp = lax.axis_index("sp")
        self.tp = lax.axis_index("tp")
        self.across = lax.rem(self.tp + t // 2, t)
        self.beside = self.tp + 1 - 2 * lax.rem(self.tp, 2)
        self.cross = lax.rem(self.beside + t // 2, t)

    def mate(self, m):
        return flip(self.sp, jnp.int32(m), self.n)

    def to(self, src, dst, send, recv, sp=None, tp=None):
        return pltpu.make_async_remote_copy(
            src_ref=src,
            dst_ref=dst,
            send_sem=send,
            recv_sem=recv,
            device_id=(self.sp if sp is None else sp, self.tp if tp is None else tp),
            device_id_type=MESH,
        )


def loop(lo, hi, body):
    def step(i, carry):
        body(i)
        return carry

    lax.fori_loop(lo, hi, step, 0)


def layer_kernel(
    n, t, cap,
    routes, rweight, rates, x_ref, c_ref, vl, og, ms, wl, rl, gate_hbm, up_hbm, down_hbm, pw_hbm,
    gate_out, up_out, down_out, proj, vg, wg, rg, outg,
    snd, got, gate, up, down, pw, pg, pu, hidden, gd, ud, part, pair, summed, other, final, arr,
    pick, gate_grad, up_grad, down_grad, trow, acol, ends, twins, joint, lined, lowhigh, delta,
    ga, full, by, gall,
    w_sem, o_sem, s_a2a, r_a2a, s_sh, r_sh, s_d, r_d, s_p, r_p, s_y, r_y, s_b, r_b, s_r, r_r,
    s_t1, r_t1, s_t2, r_t2, s_t3, r_t3, s_z, r_z, s_l, r_l, s_ls, r_ls, s_x, r_x, s_g, r_g,
    s_gs, r_gs,
):
    at = Place(n, t)
    tokens, d = x_ref.shape
    top = routes.shape[0]
    slots = n * cap
    half = n // 2
    duo = 2 * cap
    heads = rates.shape[0]
    per = heads * STATE // wl.shape[1]
    span = per * HEAD_DIM
    groups = heads // per
    z = lax.div(at.sp, 2)
    bit = lax.rem(at.sp, 2)
    twin = at.sp + 1 - 2 * bit
    col = lambda tp: pl.ds(pl.multiple_of(tp * d, d), d)
    hcol = lambda b: pl.ds(pl.multiple_of(b * (d // 2), d // 2), d // 2)

    weights_in = ((gate_hbm.at[0], gate), (up_hbm.at[0], up), (down_hbm.at[0], down), (pw_hbm, pw))
    loads = [
        pltpu.make_async_copy(src, dst, w_sem.at[i]) for i, (src, dst) in enumerate(weights_in)
    ]
    for load in loads:
        load.start()

    barrier = pltpu.get_barrier_semaphore()
    for tp in (at.across, at.beside):
        pl.semaphore_signal(barrier, inc=1, device_id=(at.sp, tp), device_id_type=MESH)

    def hello(o):
        pl.semaphore_signal(
            barrier, inc=1, device_id=(lax.rem(at.sp + o, n), at.tp), device_id_type=MESH
        )

    loop(1, n, hello)

    row_id = lax.broadcasted_iota(jnp.int32, (tokens, tokens), 0)
    col_id = lax.broadcasted_iota(jnp.int32, (tokens, tokens), 1)
    eye = (row_id == col_id).astype(F32)
    named = exact(eye, routes[...].astype(F32), LAST)
    weights = exact(eye, rweight[...], LAST)
    lanes = lax.broadcasted_iota(jnp.int32, (tokens, n), 1).astype(F32)
    onehot = [(named[:, k : k + 1] == lanes).astype(F32) for k in range(top)]
    lower = (row_id > col_id).astype(F32)
    before = dot(lower.astype(BF16), sum(onehot).astype(BF16))
    slot_lane = lax.broadcasted_iota(jnp.int32, (tokens, slots), 1).astype(F32)
    picks = []
    for k in range(top):
        rank = jnp.sum(before * onehot[k], axis=1, keepdims=True)
        picks.append((named[:, k : k + 1] * cap + rank == slot_lane).astype(F32).astype(BF16))
    pick[...] = sum(picks)
    snd[0] = dot_first(pick[...], x_ref[...]).astype(BF16).reshape(n, cap, d)
    cot = c_ref[...].astype(F32)
    weighted = [(cot * weights[:, k : k + 1]).astype(BF16) for k in range(top)]
    snd[1] = dot_first(
        jnp.concatenate(picks, axis=0), jnp.concatenate(weighted, axis=0)
    ).astype(BF16).reshape(n, cap, d)
    for k in (0, 1):
        got[k, 0, :, col(at.tp)] = snd[k, at.sp]
    pl.semaphore_wait(barrier, n + 1)


    def to_columns(value):
        lane = lax.broadcasted_iota(jnp.int32, (heads, d), 1)
        lead = lax.broadcasted_iota(jnp.int32, (heads, d), 0) * HEAD_DIM
        spread_heads = jnp.logical_and(lane >= lead, lane < lead + HEAD_DIM).astype(F32)
        return exact(value, spread_heads, FIRST)

    def prepare():
        upto = (row_id >= col_id).astype(F32)
        acol[...] = exact(upto, to_columns(rates[...]))
        trow[at.sp] = acol[tokens - 1 : tokens, :]
        ga[at.sp] = (
            ms[...].astype(F32) * silu_parts(og[...].astype(F32))[0]
        ).astype(BF16)

    def states(kind, left, right):
        a = acol[...]
        value = right[...].astype(F32)
        for i, fade in enumerate((jnp.exp(a - a[tokens - 1 : tokens, :]), jnp.exp(-a))):
            faded = (value * fade).astype(BF16)
            for g in range(groups):
                ends[kind, i, :, g * span : (g + 1) * span] = dot_first(
                    left[:, g * STATE : (g + 1) * STATE], faded[:, g * span : (g + 1) * span]
                ).astype(BF16)

    def totals(m):
        mate = at.mate(m)
        return at.to(trow.at[at.sp], trow.at[at.sp], s_d.at[m], r_d.at[m], sp=mate)

    def twin_first(kind):
        cols = hcol(1 - bit)
        return at.to(
            ends.at[kind, :, :, cols], twins.at[kind, :, :, cols], s_t1.at[kind], r_t1.at[kind],
            sp=twin,
        )

    def twin_rest(kind):
        cols = hcol(bit)
        return at.to(
            ends.at[kind, bit, :, cols], twins.at[kind, bit, :, cols], s_t2.at[kind],
            r_t2.at[kind], sp=twin,
        )

    def along(kind, o):
        there = lax.rem(z + o, half)
        return at.to(
            joint.at[kind, jnp.where(there > z, 0, 1)], lined.at[kind, z], s_z.at[kind, o],
            r_z.at[kind, o], sp=there * 2 + bit,
        )

    def twin_last(kind):
        here = lowhigh.at[kind, :, :, hcol(bit)]
        return at.to(here, here, s_t3.at[kind], r_t3.at[kind], sp=twin)

    def join(kind):
        cols = hcol(bit)
        mine = jnp.exp(-trow[at.sp, :, cols])
        his = jnp.exp(-trow[twin, :, cols])
        second = (bit == 1).astype(F32)
        keep_end = second + (1.0 - second) * his
        his_end = (1.0 - second) + second * mine
        keep_start = (1.0 - second) + second * his
        his_start = second + (1.0 - second) * mine
        own = ends[kind, :, :, cols].astype(F32)
        got_twin = twins[kind, :, :, cols].astype(F32)
        joint[kind, 0] = (own[0] * keep_end + got_twin[0] * his_end).astype(BF16)
        joint[kind, 1] = (own[1] * keep_start + got_twin[1] * his_start).astype(BF16)

    def send_along(kind):
        loop(1, half, lambda o: along(kind, o).start())

    def gather_states(kind):
        cols = hcol(bit)
        loop(1, half, lambda o: along(kind, o).wait_recv())

        def both(y):
            return trow[2 * y, :, cols] + trow[2 * y + 1, :, cols]

        zero = jnp.zeros((STATE, d // 2), F32)

        def before_me(i, carry):
            total, fade = carry
            y = z - 1 - i
            total = total + jnp.exp(-fade) * lined[kind, y].astype(F32)
            return total, fade + both(y)

        def after_me(i, carry):
            total, fade = carry
            y = z + 1 + i
            total = total + jnp.exp(-fade) * lined[kind, y].astype(F32)
            return total, fade + both(y)

        none = jnp.zeros((1, d // 2), F32)
        low, _ = lax.fori_loop(0, z, before_me, (zero, none))
        high, _ = lax.fori_loop(0, half - 1 - z, after_me, (zero, none))
        lowhigh[kind, 0, :, cols] = low.astype(BF16)
        lowhigh[kind, 1, :, cols] = high.astype(BF16)

    def reach(kind):
        his = jnp.exp(-trow[twin])
        second = (bit == 1).astype(F32)
        extra = twins[kind, 1 - bit].astype(F32)
        low = lowhigh[kind, 0].astype(F32) * (1.0 - second + second * his) + extra * second
        high = lowhigh[kind, 1].astype(F32) * (second + (1.0 - second) * his) + extra * (
            1.0 - second
        )
        return low.astype(BF16), high.astype(BF16)

    def hop(up, k):
        here = ga.at[(z - k if up else z + k) * 2 + bit]
        i = 0 if up else 1
        peer = z + 1 if up else z - 1
        return at.to(here, here, s_l.at[i, k], r_l.at[i, k], sp=peer * 2 + bit)

    def came(up, k):
        here = ga.at[(z - k if up else z + k) * 2 + bit]
        i = 0 if up else 1
        return at.to(here, here, s_l.at[i, k], r_l.at[i, k - 1], sp=twin)

    def side(up, k):
        here = ga.at[(z - k if up else z + k) * 2 + bit]
        i = 0 if up else 1
        return at.to(here, here, s_ls.at[i, k], r_ls.at[i, k], sp=twin)

    def pair_gated():
        return at.to(ga.at[at.sp], ga.at[at.sp], s_x.at[0], r_x.at[0], sp=twin)

    def begin_gated():
        @pl.when(z < half - 1)
        def _():
            hop(True, 0).start()

        @pl.when(z > 0)
        def _():
            hop(False, 0).start()

        pair_gated().start()

    def advance(k):
        @pl.when(z - k >= 0)
        def _():
            came(True, k).wait_recv()

            @pl.when(z < half - 1)
            def _():
                hop(True, k).start()

            side(True, k).start()

        @pl.when(z + k < half)
        def _():
            came(False, k).wait_recv()

            @pl.when(z > 0)
            def _():
                hop(False, k).start()

            side(False, k).start()

    def place_of(i):
        return jnp.where(i < 2, i, n + 1 - i)

    def spread(k, m):
        mate = at.mate(m)
        return at.to(
            snd.at[k, mate], got.at[k, m, :, col(at.tp)], s_a2a.at[k, m], r_a2a.at[k, m], sp=mate
        )

    def share(k, m, j):
        here = got.at[k, m, :, col(at.across if j == 2 else at.tp)]
        return at.to(
            here, here, s_sh.at[k, j, m], r_sh.at[k, j, m], tp=at.across if j == 0 else at.beside
        )

    for k in (0, 1):
        loop(1, n, lambda i: spread(k, place_of(i)).start())
    for k in (0, 1):
        share(k, 0, 0).start()
        share(k, 0, 1).start()
    prepare()
    states(0, wl, vl)
    loop(1, n, lambda m: totals(m).start())
    twin_first(0).start()
    twin_rest(0).start()

    lag = 2

    def forward(q):
        k, i = lax.div(q, n), lax.rem(q, n)
        m = place_of(i)

        @pl.when(i > 0)
        def _():
            spread(k, m).wait_recv()
            share(k, m, 0).start()
            share(k, m, 1).start()

        @pl.when(q >= lag)
        def _():
            relay(q - lag)

    def relay(q):
        k, m = lax.div(q, n), place_of(lax.rem(q, n))
        share(k, m, 0).wait_recv()
        share(k, m, 2).start()

    def base_of(j):
        return jnp.where(j < 1, 0, half - j)

    def settled(k, base):
        for m in (2 * base, 2 * base + 1):
            share(k, m, 1).wait_recv()
            share(k, m, 2).wait_recv()

    def rows_of(base):
        return pl.ds(pl.multiple_of(base * duo, duo), duo)

    def ahead(j):
        base = base_of(j)
        settled(0, base)
        rows = rows_of(base)
        inputs = got[0, pl.ds(2 * base, 2)].reshape(duo, t * d)
        pg[rows, :] = dot(inputs, gate[...])
        pu[rows, :] = dot(inputs, up[...])

    def behind(j):
        base = base_of(j)
        settled(1, base)
        rows = rows_of(base)
        sent = got[1, pl.ds(2 * base, 2)].reshape(duo, t * d)
        grad = dot_last(sent, down[...])
        active, slope = silu_parts(pg[rows, :])
        ups = pu[rows, :]
        hidden[rows, :] = (active * ups).astype(BF16)
        gd[rows, :] = (grad * ups * slope).astype(BF16)
        ud[rows, :] = (grad * active).astype(BF16)

    loop(1, n, forward)
    loop(1, n, lambda m: totals(m).wait_recv())
    twin_first(0).wait_recv()
    join(0)
    for load in loads[:3]:
        load.wait()

    def second(j):
        forward(n + 2 * j)
        forward(n + 2 * j + 1)
        ahead(j)

        @pl.when(j > 0)
        def _():
            behind(j - 1)

    loop(0, half, second)
    send_along(0)
    begin_gated()
    loop(2 * n - lag, 2 * n, relay)
    behind(half - 1)

    def halves(m, k):
        c = at.cross if k == 0 else at.beside
        return at.to(
            part.at[m, :, col(c)], pair.at[k, m], s_p.at[k, m], r_p.at[k, m], tp=at.beside
        )

    def over(m):
        return at.to(summed.at[m], other.at[m], s_y.at[m], r_y.at[m], tp=at.across)

    def back(m):
        return at.to(final.at[m], arr.at[at.sp], s_b.at[m], r_b.at[m], sp=at.mate(m))

    def produce(jj):
        base = half - 1 - jj
        rows = rows_of(base)
        for c in range(t):
            cols = slice(c * d, (c + 1) * d)
            value = dot_last(gd[rows, :], gate[cols, :]) + dot_last(ud[rows, :], up[cols, :])
            part[pl.ds(2 * base, 2), :, cols] = value.astype(BF16).reshape(2, cap, d)
        for m in (2 * base + 1, 2 * base):
            for k in (0, 1):
                halves(m, k).start()

    def pass_over(jj):
        base = half - 1 - jj
        for m in (2 * base + 1, 2 * base):
            halves(m, 0).wait_recv()
            summed[m] = (
                part[m, :, col(at.across)].astype(F32) + pair[0, m].astype(F32)
            ).astype(BF16)
            over(m).start()

    def total(jj):
        base = half - 1 - jj
        for m in (2 * base + 1, 2 * base):
            halves(m, 1).wait_recv()
            over(m).wait_recv()
            final[m] = (
                part[m, :, col(at.tp)].astype(F32) + pair[1, m].astype(F32) + other[m].astype(F32)
            ).astype(BF16)

            @pl.when(m > 0)
            def _():
                back(m).start()

    def first_turn(jj):
        produce(jj)

        @pl.when(jj > 0)
        def _():
            pass_over(jj - 1)

    def weight_grads(c):
        cols = pl.ds(pl.multiple_of(c * d, d), d)
        inputs = got[0, :, :, cols].reshape(slots, d)
        gate_grad[cols, :] = dot_first(inputs, gd[...]).astype(BF16)
        up_grad[cols, :] = dot_first(inputs, ud[...]).astype(BF16)
        sent = got[1, :, :, cols].reshape(slots, d)
        down_grad[:, cols] = dot_first(hidden[...], sent).astype(BF16)

    loop(0, half, first_turn)
    pass_over(half - 1)

    def last_turn(jj):
        total(jj)

        @pl.when(jj < t)
        def _():
            weight_grads(jj)

        @pl.when(jj + 1 < half)
        def _():
            advance(jj + 1)

    loop(0, half, last_turn)
    for c in range(half, t):
        weight_grads(c)
    stores = [
        pltpu.make_async_copy(src, dst.at[0], o_sem.at[i])
        for i, (src, dst) in enumerate(
            ((gate_grad, gate_out), (up_grad, up_out), (down_grad, down_out))
        )
    ]
    for store in stores:
        store.start()
    gather_states(0)
    twin_last(0).start()
    arr[at.sp] = final[0]
    loop(1, n, lambda i: back(n - i).wait_recv())

    moe_grad = dot(pick[...], arr[...].reshape(slots, d))
    full[:, col(at.tp)] = (c_ref[...].astype(F32) + moe_grad).astype(BF16)

    def rows_to(j):
        here = full.at[:, col(at.across if j == 2 else at.tp)]
        return at.to(here, here, s_r.at[j], r_r.at[j], tp=at.across if j == 0 else at.beside)

    rows_to(0).start()
    rows_to(1).start()
    loads[3].wait()
    twin_last(0).wait_recv()
    twin_rest(0).wait_recv()
    rows_to(0).wait_recv()
    rows_to(2).start()
    rows_to(1).wait_recv()
    rows_to(2).wait_recv()

    q = tokens // t
    width = gall.shape[2]
    row = lambda tp: pl.ds(pl.multiple_of(tp * q, q), q)
    quarter = full[row(at.tp), :]
    for o in range(n):
        by[o] = quarter[:, o * width : (o + 1) * width]

    def spread_g(m):
        mate = at.mate(m)
        return at.to(
            by.at[mate], gall.at[at.sp, row(at.tp), :], s_g.at[m], r_g.at[m], sp=mate
        )

    def share_g(m, j):
        here = gall.at[at.mate(m), row(at.across if j == 2 else at.tp), :]
        return at.to(
            here, here, s_gs.at[j, m], r_gs.at[j, m], tp=at.across if j == 0 else at.beside
        )

    gall[at.sp, row(at.tp), :] = by[at.sp]
    out_delta = dot(full[...], pw[...]).astype(BF16).astype(F32)
    loop(1, n, lambda i: spread_g(place_of(i)).start())
    share_g(0, 0).start()
    share_g(0, 1).start()
    active_gate, slope_gate = silu_parts(og[...].astype(F32))
    delta[...] = (out_delta * active_gate).astype(BF16)
    states(1, rl, delta)
    twin_first(1).start()
    twin_rest(1).start()
    outg[...] = (out_delta * ms[...].astype(F32) * slope_gate).astype(BF16)

    arow = exact(rates[...], (row_id <= col_id).astype(F32))
    inner = []
    scores = []
    for g in range(groups):
        wide = slice(g * STATE, (g + 1) * STATE)
        common = dot_last(wl[:, wide], rl[:, wide])
        score = jnp.zeros((tokens, tokens), F32)
        for h in range(g * per, (g + 1) * per):
            cols = slice(h * HEAD_DIM, (h + 1) * HEAD_DIM)
            fade = jnp.exp(
                -jnp.abs(acol[:, h * HEAD_DIM : h * HEAD_DIM + 1] - arow[h : h + 1, :])
            )
            inner.append(dot((fade * common).astype(BF16), delta[:, cols]))
            score += fade * dot_last(vl[:, cols], delta[:, cols])
        scores.append(score.astype(BF16))

    twin_first(1).wait_recv()
    join(1)
    send_along(1)

    def forward_g(i):
        m = place_of(i)
        spread_g(m).wait_recv()
        share_g(m, 0).start()
        share_g(m, 1).start()

    loop(1, n, forward_g)
    a = acol[...]
    to_end = jnp.exp(a - a[tokens - 1 : tokens, :])
    to_start = jnp.exp(-a)
    w_low, w_high = reach(0)
    value = vl[...].astype(F32)
    moved = delta[...].astype(F32)
    d_start, d_end = (moved * to_start).astype(BF16), (moved * to_end).astype(BF16)
    v_start, v_end = (value * to_start).astype(BF16), (value * to_end).astype(BF16)
    for g in range(groups):
        wide = slice(g * STATE, (g + 1) * STATE)
        cols = slice(g * span, (g + 1) * span)
        rg[:, wide] = (
            dot_first(scores[g], wl[:, wide])
            + dot_last(d_start[:, cols], w_low[:, cols])
            + dot_last(d_end[:, cols], w_high[:, cols])
        ).astype(BF16)

    def relay_g(i):
        m = jnp.where(i < 1, 0, place_of(i))
        share_g(m, 0).wait_recv()
        share_g(m, 2).start()

    loop(0, n, relay_g)
    gather_states(1)
    twin_last(1).start()

    def settle_g(m):
        share_g(m, 1).wait_recv()
        share_g(m, 2).wait_recv()

    loop(0, n, settle_g)
    pair_gated().wait_recv()

    def settle_gated(k):
        @pl.when(z - k >= 0)
        def _():
            side(True, k).wait_recv()

        @pl.when(z + k < half)
        def _():
            side(False, k).wait_recv()

    loop(1, half, settle_gated)
    proj[...] = dot_first(
        gall[...].reshape(n * tokens, width), ga[...].reshape(n * tokens, d)
    )
    twin_rest(1).wait_recv()
    twin_last(1).wait_recv()
    r_low, r_high = reach(1)
    for g in range(groups):
        wide = slice(g * STATE, (g + 1) * STATE)
        cols = slice(g * span, (g + 1) * span)
        wg[:, wide] = (
            dot(scores[g], rl[:, wide])
            + dot_last(v_start[:, cols], r_low[:, cols])
            + dot_last(v_end[:, cols], r_high[:, cols])
        ).astype(BF16)
        vg[:, cols] = (
            jnp.concatenate(inner[g * per : (g + 1) * per], axis=1)
            + dot(wl[:, wide], r_low[:, cols]) * to_start[:, cols]
            + dot(wl[:, wide], r_high[:, cols]) * to_end[:, cols]
        ).astype(BF16)

    def finish(m):
        for k in (0, 1):
            for j in (0, 1, 2):
                share(k, m, j).wait_send()
            halves(m, k).wait_send()
        over(m).wait_send()
        for j in (0, 1, 2):
            share_g(m, j).wait_send()

    loop(0, n, finish)

    def finish_sp(m):
        for k in (0, 1):
            spread(k, m).wait_send()
        back(m).wait_send()
        totals(m).wait_send()
        spread_g(m).wait_send()

    loop(1, n, finish_sp)
    for j in (0, 1, 2):
        rows_to(j).wait_send()
    for kind in (0, 1):
        twin_first(kind).wait_send()
        twin_rest(kind).wait_send()
        twin_last(kind).wait_send()
        loop(1, half, lambda o: along(kind, o).wait_send())
    pair_gated().wait_send()

    def drain(k):
        @pl.when(jnp.logical_and(z - k >= 0, z < half - 1))
        def _():
            hop(True, k).wait_send()

        @pl.when(jnp.logical_and(z + k < half, z > 0))
        def _():
            hop(False, k).wait_send()

    loop(0, half, drain)

    def drain_sides(k):
        @pl.when(z - k >= 0)
        def _():
            side(True, k).wait_send()

        @pl.when(z + k < half)
        def _():
            side(False, k).wait_send()

    loop(1, half, drain_sides)
    for store in stores:
        store.wait()


def on_device(
    layer_input,
    cotangent,
    routes,
    route_weight,
    gate_weight,
    up_weight,
    down_weight,
    heads_value,
    output_gate,
    mixer_saved,
    proj_weight,
    state_write,
    state_read,
    decay_rate,
):
    n = lax.axis_size("sp")
    t = lax.axis_size("tp")
    tokens, d = layer_input.shape
    top = routes.shape[1]
    capacity = -(-max(2, 3 * tokens * top // (2 * n)) // 16) * 16
    slots = n * capacity
    hid = gate_weight.shape[2]
    half = n // 2
    width = t * d // n
    state_w = state_write.shape[1]
    sds = jax.ShapeDtypeStruct
    block = (n, capacity, d)
    vm = pl.BlockSpec(memory_space=pltpu.VMEM)
    hbm = pl.BlockSpec(memory_space=pl.ANY)
    sems = [
        (4,), (3,), (2, n), (2, n), (2, 3, n), (2, 3, n), (n,), (n,), (2, n), (2, n), (n,), (n,),
        (n,), (n,), (3,), (3,),
        (2,), (2,), (2,), (2,), (2,), (2,), (2, half), (2, half), (2, half), (2, half),
        (2, half), (2, half), (1,), (1,), (n,), (n,), (3, n), (3, n),
    ]
    return pl.pallas_call(
        functools.partial(layer_kernel, n, t, capacity),
        out_shape=(
            sds((1, t * d, hid), BF16),
            sds((1, t * d, hid), BF16),
            sds((1, hid, t * d), BF16),
            sds((width, d), F32),
            sds((tokens, d), BF16),
            sds((tokens, state_w), BF16),
            sds((tokens, state_w), BF16),
            sds((tokens, d), BF16),
        ),
        in_specs=[vm] * 10 + [hbm] * 4,
        out_specs=(hbm,) * 3 + (vm,) * 5,
        scratch_shapes=[
            VMEM((2,) + block, BF16),
            VMEM((2, n, capacity, t * d), BF16),
            VMEM((t * d, hid), BF16),
            VMEM((t * d, hid), BF16),
            VMEM((hid, t * d), BF16),
            VMEM((t * d, d), BF16),
            VMEM((slots, hid), F32),
            VMEM((slots, hid), F32),
            VMEM((slots, hid), BF16),
            VMEM((slots, hid), BF16),
            VMEM((slots, hid), BF16),
            VMEM((n, capacity, t * d), BF16),
            VMEM((2,) + block, BF16),
            VMEM(block, BF16),
            VMEM(block, BF16),
            VMEM(block, BF16),
            VMEM(block, BF16),
            VMEM((tokens, slots), BF16),
            VMEM((t * d, hid), BF16),
            VMEM((t * d, hid), BF16),
            VMEM((hid, t * d), BF16),
            VMEM((n, 1, d), F32),
            VMEM((tokens, d), F32),
            VMEM((2, 2, STATE, d), BF16),
            VMEM((2, 2, STATE, d), BF16),
            VMEM((2, 2, STATE, d // 2), BF16),
            VMEM((2, half, STATE, d // 2), BF16),
            VMEM((2, 2, STATE, d), BF16),
            VMEM((tokens, d), BF16),
            VMEM((n, tokens, d), BF16),
            VMEM((tokens, t * d), BF16),
            VMEM((n, tokens // t, width), BF16),
            VMEM((n, tokens, width), BF16),
        ] + [DMA(shape) for shape in sems],
        compiler_params=pltpu.CompilerParams(
            collective_id=1,
            has_side_effects=True,
            vmem_limit_bytes=60 * 1024 * 1024,
        ),
        cost_estimate=pl.CostEstimate(
            flops=4_000_000_000, bytes_accessed=8_000_000, transcendentals=0
        ),
        name="layer",
    )(
        routes.T,
        route_weight.T,
        decay_rate.T,
        layer_input,
        cotangent,
        heads_value,
        output_gate,
        mixer_saved,
        state_write,
        state_read,
        gate_weight,
        up_weight,
        down_weight,
        proj_weight,
    )


def solution(mesh):
    split = P("sp", "tp")
    in_specs = (
        split,
        split,
        P("sp", None),
        P("sp", None),
        P("sp", None, "tp"),
        P("sp", None, "tp"),
        P("sp", "tp", None),
        split,
        split,
        split,
        P(None, "tp"),
        split,
        split,
        split,
    )
    out_specs = (
        P("sp", None, "tp"),
        P("sp", None, "tp"),
        P("sp", "tp", None),
        split,
        split,
        split,
        split,
        split,
    )
    return jax.shard_map(
        on_device, mesh=mesh, in_specs=in_specs, out_specs=out_specs, check_vma=False
    )
```

```python
import functools

import jax
import jax.numpy as jnp
from jax import lax
from jax.experimental import pallas as pl
from jax.experimental.pallas import tpu as pltpu
from jax.sharding import PartitionSpec as P

HEAD_DIM = 64
STATE = 128
MESH = pl.DeviceIdType.MESH
LAST = (((1,), (1,)), ((), ()))
FIRST = (((0,), (0,)), ((), ()))
F32 = jnp.float32
BF16 = jnp.bfloat16
VMEM = pltpu.VMEM
DMA = pltpu.SemaphoreType.DMA
MIB = 1024 * 1024


def silu_parts(value):
    sigma = jax.nn.sigmoid(value)
    return (value * sigma, sigma * (1.0 + value * (1.0 - sigma)))


def dot_first(a, b):
    return lax.dot_general(a, b, FIRST, preferred_element_type=F32)


def dot_last(a, b):
    return lax.dot_general(a, b, LAST, preferred_element_type=F32)


def dot(a, b):
    return jnp.dot(a, b, preferred_element_type=F32)


def exact(a, b, dims=(((1,), (0,)), ((), ()))):
    return lax.dot_general(
        a, b, dims, precision=lax.Precision.HIGHEST, preferred_element_type=F32
    )


def flip(a, b, n):
    out, bit = 0, 1
    while bit < n:
        out = out + lax.rem(lax.div(a, bit) + lax.div(b, bit), 2) * bit
        bit *= 2
    return out


class Place:
    def __init__(self, n, t):
        self.n, self.t = n, t
        self.sp = lax.axis_index("sp")
        self.tp = lax.axis_index("tp")
        self.across = lax.rem(self.tp + t // 2, t)
        self.beside = self.tp + 1 - 2 * lax.rem(self.tp, 2)
        self.cross = lax.rem(self.beside + t // 2, t)

    def mate(self, m):
        return flip(self.sp, jnp.int32(m), self.n)

    def to(self, src, dst, send, recv, sp=None, tp=None):
        return pltpu.make_async_remote_copy(
            src_ref=src,
            dst_ref=dst,
            send_sem=send,
            recv_sem=recv,
            device_id=(self.sp if sp is None else sp, self.tp if tp is None else tp),
            device_id_type=MESH,
        )


def loop(lo, hi, body):
    def step(i, carry):
        body(i)
        return carry

    lax.fori_loop(lo, hi, step, 0)


def layer_kernel(
    n, t, cap,
    routes, rweight, rates, x_ref, c_ref, vl, og, ms, wl, rl, gate_hbm, up_hbm, down_hbm, pw_hbm,
    gate_grad, up_grad, down_grad, proj, vg, wg, rg, outg,
    snd, got, gate, up, down, pw, pg, pu, hidden, gd, ud, part, pair, summed, other, final, arr,
    pick, trow, acol, ends, twins, joint, lined, lowhigh, delta,
    ga, full, by, gall,
    w_sem, s_a2a, r_a2a, s_sh, r_sh, s_d, r_d, s_p, r_p, s_y, r_y, s_b, r_b, s_r, r_r,
    s_t1, r_t1, s_t2, r_t2, s_t3, r_t3, s_z, r_z, s_l, r_l, s_ls, r_ls, s_x, r_x, s_g, r_g,
    s_gs, r_gs,
):
    at = Place(n, t)
    tokens, d = x_ref.shape
    top = routes.shape[0]
    slots = n * cap
    half = n // 2
    duo = 2 * cap
    heads = rates.shape[0]
    per = heads * STATE // wl.shape[1]
    span = per * HEAD_DIM
    groups = heads // per
    z = lax.div(at.sp, 2)
    bit = lax.rem(at.sp, 2)
    twin = at.sp + 1 - 2 * bit
    col = lambda tp: pl.ds(pl.multiple_of(tp * d, d), d)
    hcol = lambda b: pl.ds(pl.multiple_of(b * (d // 2), d // 2), d // 2)

    weights_in = ((gate_hbm.at[0], gate), (up_hbm.at[0], up), (down_hbm.at[0], down), (pw_hbm, pw))
    loads = [
        pltpu.make_async_copy(src, dst, w_sem.at[i]) for i, (src, dst) in enumerate(weights_in)
    ]
    for load in loads:
        load.start()

    barrier = pltpu.get_barrier_semaphore()
    for tp in (at.across, at.beside):
        pl.semaphore_signal(barrier, inc=1, device_id=(at.sp, tp), device_id_type=MESH)

    def hello(o):
        pl.semaphore_signal(
            barrier, inc=1, device_id=(lax.rem(at.sp + o, n), at.tp), device_id_type=MESH
        )

    loop(1, n, hello)

    row_id = lax.broadcasted_iota(jnp.int32, (tokens, tokens), 0)
    col_id = lax.broadcasted_iota(jnp.int32, (tokens, tokens), 1)
    eye = (row_id == col_id).astype(F32)
    named = exact(eye, routes[...].astype(F32), LAST)
    weights = exact(eye, rweight[...], LAST)
    lanes = lax.broadcasted_iota(jnp.int32, (tokens, n), 1).astype(F32)
    onehot = [(named[:, k : k + 1] == lanes).astype(F32) for k in range(top)]
    lower = (row_id > col_id).astype(F32)
    before = dot(lower.astype(BF16), sum(onehot).astype(BF16))
    slot_lane = lax.broadcasted_iota(jnp.int32, (tokens, slots), 1).astype(F32)
    picks = []
    for k in range(top):
        rank = jnp.sum(before * onehot[k], axis=1, keepdims=True)
        picks.append((named[:, k : k + 1] * cap + rank == slot_lane).astype(F32).astype(BF16))
    pick[...] = sum(picks)
    snd[0] = dot_first(pick[...], x_ref[...]).astype(BF16).reshape(n, cap, d)
    cot = c_ref[...].astype(F32)
    weighted = [(cot * weights[:, k : k + 1]).astype(BF16) for k in range(top)]
    snd[1] = dot_first(
        jnp.concatenate(picks, axis=0), jnp.concatenate(weighted, axis=0)
    ).astype(BF16).reshape(n, cap, d)
    for k in (0, 1):
        got[k, 0, :, col(at.tp)] = snd[k, at.sp]
    pl.semaphore_wait(barrier, n + 1)


    def to_columns(value):
        lane = lax.broadcasted_iota(jnp.int32, (heads, d), 1)
        lead = lax.broadcasted_iota(jnp.int32, (heads, d), 0) * HEAD_DIM
        spread_heads = jnp.logical_and(lane >= lead, lane < lead + HEAD_DIM).astype(F32)
        return exact(value, spread_heads, FIRST)

    def prepare():
        upto = (row_id >= col_id).astype(F32)
        acol[...] = exact(upto, to_columns(rates[...]))
        trow[at.sp] = acol[tokens - 1 : tokens, :]
        ga[at.sp] = (
            ms[...].astype(F32) * silu_parts(og[...].astype(F32))[0]
        ).astype(BF16)

    def states(kind, left, right):
        a = acol[...]
        value = right[...].astype(F32)
        for i, fade in enumerate((jnp.exp(a - a[tokens - 1 : tokens, :]), jnp.exp(-a))):
            faded = (value * fade).astype(BF16)
            for g in range(groups):
                ends[kind, i, :, g * span : (g + 1) * span] = dot_first(
                    left[:, g * STATE : (g + 1) * STATE], faded[:, g * span : (g + 1) * span]
                ).astype(BF16)

    def totals(m):
        mate = at.mate(m)
        return at.to(trow.at[at.sp], trow.at[at.sp], s_d.at[m], r_d.at[m], sp=mate)

    def twin_first(kind):
        cols = hcol(1 - bit)
        return at.to(
            ends.at[kind, :, :, cols], twins.at[kind, :, :, cols], s_t1.at[kind], r_t1.at[kind],
            sp=twin,
        )

    def twin_rest(kind):
        cols = hcol(bit)
        return at.to(
            ends.at[kind, bit, :, cols], twins.at[kind, bit, :, cols], s_t2.at[kind],
            r_t2.at[kind], sp=twin,
        )

    def along(kind, o):
        there = lax.rem(z + o, half)
        return at.to(
            joint.at[kind, jnp.where(there > z, 0, 1)], lined.at[kind, z], s_z.at[kind, o],
            r_z.at[kind, o], sp=there * 2 + bit,
        )

    def twin_last(kind):
        here = lowhigh.at[kind, :, :, hcol(bit)]
        return at.to(here, here, s_t3.at[kind], r_t3.at[kind], sp=twin)

    def join(kind):
        cols = hcol(bit)
        mine = jnp.exp(-trow[at.sp, :, cols])
        his = jnp.exp(-trow[twin, :, cols])
        second = (bit == 1).astype(F32)
        keep_end = second + (1.0 - second) * his
        his_end = (1.0 - second) + second * mine
        keep_start = (1.0 - second) + second * his
        his_start = second + (1.0 - second) * mine
        own = ends[kind, :, :, cols].astype(F32)
        got_twin = twins[kind, :, :, cols].astype(F32)
        joint[kind, 0] = (own[0] * keep_end + got_twin[0] * his_end).astype(BF16)
        joint[kind, 1] = (own[1] * keep_start + got_twin[1] * his_start).astype(BF16)

    def send_along(kind):
        loop(1, half, lambda o: along(kind, o).start())

    def gather_states(kind):
        cols = hcol(bit)
        loop(1, half, lambda o: along(kind, o).wait_recv())

        def both(y):
            return trow[2 * y, :, cols] + trow[2 * y + 1, :, cols]

        zero = jnp.zeros((STATE, d // 2), F32)

        def before_me(i, carry):
            total, fade = carry
            y = z - 1 - i
            total = total + jnp.exp(-fade) * lined[kind, y].astype(F32)
            return total, fade + both(y)

        def after_me(i, carry):
            total, fade = carry
            y = z + 1 + i
            total = total + jnp.exp(-fade) * lined[kind, y].astype(F32)
            return total, fade + both(y)

        none = jnp.zeros((1, d // 2), F32)
        low, _ = lax.fori_loop(0, z, before_me, (zero, none))
        high, _ = lax.fori_loop(0, half - 1 - z, after_me, (zero, none))
        lowhigh[kind, 0, :, cols] = low.astype(BF16)
        lowhigh[kind, 1, :, cols] = high.astype(BF16)

    def reach(kind):
        his = jnp.exp(-trow[twin])
        second = (bit == 1).astype(F32)
        extra = twins[kind, 1 - bit].astype(F32)
        low = lowhigh[kind, 0].astype(F32) * (1.0 - second + second * his) + extra * second
        high = lowhigh[kind, 1].astype(F32) * (second + (1.0 - second) * his) + extra * (
            1.0 - second
        )
        return low.astype(BF16), high.astype(BF16)

    def hop(up, k):
        here = ga.at[(z - k if up else z + k) * 2 + bit]
        i = 0 if up else 1
        peer = z + 1 if up else z - 1
        return at.to(here, here, s_l.at[i, k], r_l.at[i, k], sp=peer * 2 + bit)

    def came(up, k):
        here = ga.at[(z - k if up else z + k) * 2 + bit]
        i = 0 if up else 1
        return at.to(here, here, s_l.at[i, k], r_l.at[i, k - 1], sp=twin)

    def side(up, k):
        here = ga.at[(z - k if up else z + k) * 2 + bit]
        i = 0 if up else 1
        return at.to(here, here, s_ls.at[i, k], r_ls.at[i, k], sp=twin)

    def pair_gated():
        return at.to(ga.at[at.sp], ga.at[at.sp], s_x.at[0], r_x.at[0], sp=twin)

    def begin_gated():
        @pl.when(z < half - 1)
        def _():
            hop(True, 0).start()

        @pl.when(z > 0)
        def _():
            hop(False, 0).start()

        pair_gated().start()

    def advance(k):
        @pl.when(z - k >= 0)
        def _():
            came(True, k).wait_recv()

            @pl.when(z < half - 1)
            def _():
                hop(True, k).start()

            side(True, k).start()

        @pl.when(z + k < half)
        def _():
            came(False, k).wait_recv()

            @pl.when(z > 0)
            def _():
                hop(False, k).start()

            side(False, k).start()

    def spread(k, m):
        mate = at.mate(m)
        return at.to(
            snd.at[k, mate], got.at[k, m, :, col(at.tp)], s_a2a.at[k, m], r_a2a.at[k, m], sp=mate
        )

    def share(k, m, j):
        here = got.at[k, m, :, col(at.across if j == 2 else at.tp)]
        return at.to(
            here, here, s_sh.at[k, j, m], r_sh.at[k, j, m], tp=at.across if j == 0 else at.beside
        )

    for k in (0, 1):
        loop(1, n, lambda i: spread(k, i).start())
    for k in (0, 1):
        share(k, 0, 0).start()
        share(k, 0, 1).start()
    prepare()
    states(0, wl, vl)
    loop(1, n, lambda m: totals(m).start())
    twin_first(0).start()
    twin_rest(0).start()

    lag = 2

    def forward(q):
        k, i = lax.div(q, n), lax.rem(q, n)
        m = i

        @pl.when(i > 0)
        def _():
            spread(k, m).wait_recv()
            share(k, m, 0).start()
            share(k, m, 1).start()

        @pl.when(q >= lag)
        def _():
            relay(q - lag)

    def relay(q):
        k, m = lax.div(q, n), lax.rem(q, n)
        share(k, m, 0).wait_recv()
        share(k, m, 2).start()

    def settled(k, base):
        for m in (2 * base, 2 * base + 1):
            share(k, m, 1).wait_recv()
            share(k, m, 2).wait_recv()

    def rows_of(base):
        return pl.ds(pl.multiple_of(base * duo, duo), duo)

    def ahead(j):
        base = j
        settled(0, base)
        rows = rows_of(base)
        inputs = got[0, pl.ds(2 * base, 2)].reshape(duo, t * d)
        pg[rows, :] = dot(inputs, gate[...])
        pu[rows, :] = dot(inputs, up[...])

    def behind(j):
        base = j
        settled(1, base)
        rows = rows_of(base)
        sent = got[1, pl.ds(2 * base, 2)].reshape(duo, t * d)
        grad = dot_last(sent, down[...])
        active, slope = silu_parts(pg[rows, :])
        ups = pu[rows, :]
        hidden[rows, :] = (active * ups).astype(BF16)
        gd[rows, :] = (grad * ups * slope).astype(BF16)
        ud[rows, :] = (grad * active).astype(BF16)

    loop(1, n, forward)
    for load in loads[:3]:
        load.wait()

    def second(j):
        forward(n + 2 * j)
        forward(n + 2 * j + 1)
        ahead(j)

        @pl.when(j > 0)
        def _():
            behind(j - 1)

    loop(0, half, second)
    begin_gated()
    loop(2 * n - lag, 2 * n, relay)
    behind(half - 1)

    def halves(m, k):
        c = at.cross if k == 0 else at.beside
        return at.to(
            part.at[m, :, col(c)], pair.at[k, m], s_p.at[k, m], r_p.at[k, m], tp=at.beside
        )

    def over(m):
        return at.to(summed.at[m], other.at[m], s_y.at[m], r_y.at[m], tp=at.across)

    def back(m):
        return at.to(final.at[m], arr.at[at.sp], s_b.at[m], r_b.at[m], sp=at.mate(m))

    def produce(jj):
        base = half - 1 - jj
        rows = rows_of(base)
        for c in range(t):
            cols = slice(c * d, (c + 1) * d)
            value = dot_last(gd[rows, :], gate[cols, :]) + dot_last(ud[rows, :], up[cols, :])
            part[pl.ds(2 * base, 2), :, cols] = value.astype(BF16).reshape(2, cap, d)
        for m in (2 * base + 1, 2 * base):
            for k in (0, 1):
                halves(m, k).start()

    def pass_over(jj):
        base = half - 1 - jj
        for m in (2 * base + 1, 2 * base):
            halves(m, 0).wait_recv()
            summed[m] = (
                part[m, :, col(at.across)].astype(F32) + pair[0, m].astype(F32)
            ).astype(BF16)
            over(m).start()

    def total(jj):
        base = half - 1 - jj
        for m in (2 * base + 1, 2 * base):
            halves(m, 1).wait_recv()
            over(m).wait_recv()
            final[m] = (
                part[m, :, col(at.tp)].astype(F32) + pair[1, m].astype(F32) + other[m].astype(F32)
            ).astype(BF16)

            @pl.when(m > 0)
            def _():
                back(m).start()

    def first_turn(jj):
        produce(jj)

        @pl.when(jj > 0)
        def _():
            pass_over(jj - 1)

    def weight_grads(c):
        cols = pl.ds(pl.multiple_of(c * d, d), d)
        inputs = got[0, :, :, cols].reshape(slots, d)
        gate_grad[0, cols, :] = dot_first(inputs, gd[...]).astype(BF16)
        up_grad[0, cols, :] = dot_first(inputs, ud[...]).astype(BF16)
        sent = got[1, :, :, cols].reshape(slots, d)
        down_grad[0, :, cols] = dot_first(hidden[...], sent).astype(BF16)

    loop(0, half, first_turn)
    pass_over(half - 1)
    if half > 1:
        advance(1)

    def last_turn(jj):
        total(jj)

        @pl.when(jj < t)
        def _():
            weight_grads(jj)

    loop(0, half, last_turn)
    for c in range(half, t):
        weight_grads(c)
    loop(1, n, lambda m: totals(m).wait_recv())
    twin_first(0).wait_recv()
    join(0)
    send_along(0)
    if half > 3:
        loop(2, half - 1, advance)
    arr[at.sp] = final[0]
    loop(1, n, lambda i: back(n - i).wait_recv())

    moe_grad = dot(pick[...], arr[...].reshape(slots, d))
    full[:, col(at.tp)] = (c_ref[...].astype(F32) + moe_grad).astype(BF16)

    def rows_to(j):
        here = full.at[:, col(at.across if j == 2 else at.tp)]
        return at.to(here, here, s_r.at[j], r_r.at[j], tp=at.across if j == 0 else at.beside)

    rows_to(0).start()
    rows_to(1).start()
    loads[3].wait()
    rows_to(0).wait_recv()
    rows_to(2).start()
    if half > 2:
        advance(half - 1)
    rows_to(1).wait_recv()
    rows_to(2).wait_recv()

    q = tokens // t
    width = gall.shape[2]
    row = lambda tp: pl.ds(pl.multiple_of(tp * q, q), q)
    quarter = full[row(at.tp), :]
    for o in range(n):
        by[o] = quarter[:, o * width : (o + 1) * width]

    def spread_g(m):
        mate = at.mate(m)
        return at.to(
            by.at[mate], gall.at[at.sp, row(at.tp), :], s_g.at[m], r_g.at[m], sp=mate
        )

    def share_g(m, j):
        here = gall.at[at.mate(m), row(at.across if j == 2 else at.tp), :]
        return at.to(
            here, here, s_gs.at[j, m], r_gs.at[j, m], tp=at.across if j == 0 else at.beside
        )

    gall[at.sp, row(at.tp), :] = by[at.sp]
    out_delta = dot(full[...], pw[...]).astype(BF16).astype(F32)
    loop(1, n, lambda i: spread_g(i).start())
    share_g(0, 0).start()
    share_g(0, 1).start()
    active_gate, slope_gate = silu_parts(og[...].astype(F32))
    delta[...] = (out_delta * active_gate).astype(BF16)
    states(1, rl, delta)
    twin_first(1).start()
    twin_rest(1).start()
    outg[...] = (out_delta * ms[...].astype(F32) * slope_gate).astype(BF16)

    arow = exact(rates[...], (row_id <= col_id).astype(F32))
    inner = []
    scores = []
    for g in range(groups):
        wide = slice(g * STATE, (g + 1) * STATE)
        common = dot_last(wl[:, wide], rl[:, wide])
        score = jnp.zeros((tokens, tokens), F32)
        for h in range(g * per, (g + 1) * per):
            cols = slice(h * HEAD_DIM, (h + 1) * HEAD_DIM)
            fade = jnp.exp(
                -jnp.abs(acol[:, h * HEAD_DIM : h * HEAD_DIM + 1] - arow[h : h + 1, :])
            )
            inner.append(dot((fade * common).astype(BF16), delta[:, cols]))
            score += fade * dot_last(vl[:, cols], delta[:, cols])
        scores.append(score.astype(BF16))

    twin_first(1).wait_recv()
    join(1)
    send_along(1)
    gather_states(0)
    twin_last(0).start()

    def forward_g(m):
        spread_g(m).wait_recv()
        share_g(m, 0).start()
        share_g(m, 1).start()

    loop(1, n, forward_g)
    def relay_g(m):
        share_g(m, 0).wait_recv()
        share_g(m, 2).start()

    loop(0, n, relay_g)
    gather_states(1)
    twin_last(1).start()

    def settle_g(m):
        share_g(m, 1).wait_recv()
        share_g(m, 2).wait_recv()

    loop(0, n, settle_g)
    pair_gated().wait_recv()

    def settle_gated(k):
        @pl.when(z - k >= 0)
        def _():
            side(True, k).wait_recv()

        @pl.when(z + k < half)
        def _():
            side(False, k).wait_recv()

    loop(1, half, settle_gated)
    proj[...] = dot_first(
        gall[...].reshape(n * tokens, width), ga[...].reshape(n * tokens, d)
    )
    twin_rest(0).wait_recv()
    twin_last(0).wait_recv()
    a = acol[...]
    to_end = jnp.exp(a - a[tokens - 1 : tokens, :])
    to_start = jnp.exp(-a)
    w_low, w_high = reach(0)
    value = vl[...].astype(F32)
    moved = delta[...].astype(F32)
    d_start, d_end = (moved * to_start).astype(BF16), (moved * to_end).astype(BF16)
    v_start, v_end = (value * to_start).astype(BF16), (value * to_end).astype(BF16)
    for g in range(groups):
        wide = slice(g * STATE, (g + 1) * STATE)
        cols = slice(g * span, (g + 1) * span)
        rg[:, wide] = (
            dot_first(scores[g], wl[:, wide])
            + dot_last(d_start[:, cols], w_low[:, cols])
            + dot_last(d_end[:, cols], w_high[:, cols])
        ).astype(BF16)

    twin_rest(1).wait_recv()
    twin_last(1).wait_recv()
    r_low, r_high = reach(1)
    for g in range(groups):
        wide = slice(g * STATE, (g + 1) * STATE)
        cols = slice(g * span, (g + 1) * span)
        wg[:, wide] = (
            dot(scores[g], rl[:, wide])
            + dot_last(v_start[:, cols], r_low[:, cols])
            + dot_last(v_end[:, cols], r_high[:, cols])
        ).astype(BF16)
        vg[:, cols] = (
            jnp.concatenate(inner[g * per : (g + 1) * per], axis=1)
            + dot(wl[:, wide], r_low[:, cols]) * to_start[:, cols]
            + dot(wl[:, wide], r_high[:, cols]) * to_end[:, cols]
        ).astype(BF16)

    def finish(m):
        for k in (0, 1):
            for j in (0, 1, 2):
                share(k, m, j).wait_send()
            halves(m, k).wait_send()
        over(m).wait_send()
        for j in (0, 1, 2):
            share_g(m, j).wait_send()

    loop(0, n, finish)

    def finish_sp(m):
        for k in (0, 1):
            spread(k, m).wait_send()
        back(m).wait_send()
        totals(m).wait_send()
        spread_g(m).wait_send()

    loop(1, n, finish_sp)
    for j in (0, 1, 2):
        rows_to(j).wait_send()
    for kind in (0, 1):
        twin_first(kind).wait_send()
        twin_rest(kind).wait_send()
        twin_last(kind).wait_send()
        loop(1, half, lambda o: along(kind, o).wait_send())
    pair_gated().wait_send()

    def drain(k):
        @pl.when(jnp.logical_and(z - k >= 0, z < half - 1))
        def _():
            hop(True, k).wait_send()

        @pl.when(jnp.logical_and(z + k < half, z > 0))
        def _():
            hop(False, k).wait_send()

    loop(0, half, drain)

    def drain_sides(k):
        @pl.when(z - k >= 0)
        def _():
            side(True, k).wait_send()

        @pl.when(z + k < half)
        def _():
            side(False, k).wait_send()

    loop(1, half, drain_sides)


def put_out_kernel(*refs):
    count = len(refs) // 2
    copies = [
        pltpu.make_async_copy(refs[i], refs[count + i], refs[-1].at[i]) for i in range(count)
    ]
    for copy in copies:
        copy.start()
    for copy in copies:
        copy.wait()


def held(scratch):
    shape, size = scratch.shape, jnp.dtype(scratch.dtype).itemsize
    minor = -(-shape[-1] // 128) * 128
    rows = -(-shape[-2] // 16) * 16
    return functools.reduce(lambda a, b: a * b, shape[:-2], minor * rows * size)


def on_device(
    layer_input,
    cotangent,
    routes,
    route_weight,
    gate_weight,
    up_weight,
    down_weight,
    heads_value,
    output_gate,
    mixer_saved,
    proj_weight,
    state_write,
    state_read,
    decay_rate,
):
    n = lax.axis_size("sp")
    t = lax.axis_size("tp")
    tokens, d = layer_input.shape
    top = routes.shape[1]
    capacity = -(-max(2, 3 * tokens * top // (2 * n)) // 16) * 16
    slots = n * capacity
    hid = gate_weight.shape[2]
    half = n // 2
    width = t * d // n
    state_w = state_write.shape[1]
    sds = jax.ShapeDtypeStruct
    block = (n, capacity, d)
    vm = pl.BlockSpec(memory_space=pltpu.VMEM)
    hbm = pl.BlockSpec(memory_space=pltpu.HBM)
    sems = [
        (4,), (2, n), (2, n), (2, 3, n), (2, 3, n), (n,), (n,), (2, n), (2, n), (n,), (n,),
        (n,), (n,), (3,), (3,),
        (2,), (2,), (2,), (2,), (2,), (2,), (2, half), (2, half), (2, half), (2, half),
        (2, half), (2, half), (1,), (1,), (n,), (n,), (3, n), (3, n),
    ]
    outs = (
        sds((1, t * d, hid), BF16),
        sds((1, t * d, hid), BF16),
        sds((1, hid, t * d), BF16),
        sds((width, d), F32),
        sds((tokens, d), BF16),
        sds((tokens, state_w), BF16),
        sds((tokens, state_w), BF16),
        sds((tokens, d), BF16),
    )
    scratch = [
        VMEM((2,) + block, BF16),
        VMEM((2, n, capacity, t * d), BF16),
        VMEM((t * d, hid), BF16),
        VMEM((t * d, hid), BF16),
        VMEM((hid, t * d), BF16),
        VMEM((t * d, d), BF16),
        VMEM((slots, hid), F32),
        VMEM((slots, hid), F32),
        VMEM((slots, hid), BF16),
        VMEM((slots, hid), BF16),
        VMEM((slots, hid), BF16),
        VMEM((n, capacity, t * d), BF16),
        VMEM((2,) + block, BF16),
        VMEM(block, BF16),
        VMEM(block, BF16),
        VMEM(block, BF16),
        VMEM(block, BF16),
        VMEM((tokens, slots), BF16),
        VMEM((n, 1, d), F32),
        VMEM((tokens, d), F32),
        VMEM((2, 2, STATE, d), BF16),
        VMEM((2, 2, STATE, d), BF16),
        VMEM((2, 2, STATE, d // 2), BF16),
        VMEM((2, half, STATE, d // 2), BF16),
        VMEM((2, 2, STATE, d), BF16),
        VMEM((tokens, d), BF16),
        VMEM((n, tokens, d), BF16),
        VMEM((tokens, t * d), BF16),
        VMEM((n, tokens // t, width), BF16),
        VMEM((n, tokens, width), BF16),
    ]
    grads = pl.pallas_call(
        functools.partial(layer_kernel, n, t, capacity),
        out_shape=outs,
        in_specs=[vm] * 10 + [hbm] * 4,
        out_specs=(vm,) * 8,
        scratch_shapes=scratch + [DMA(shape) for shape in sems],
        compiler_params=pltpu.CompilerParams(
            collective_id=1,
            has_side_effects=True,
            vmem_limit_bytes=min(60 * MIB, sum(map(held, scratch)) + 8 * MIB),
        ),
        cost_estimate=pl.CostEstimate(
            flops=4_000_000_000, bytes_accessed=8_000_000, transcendentals=0
        ),
        name="layer",
    )(
        routes.T,
        route_weight.T,
        decay_rate.T,
        layer_input,
        cotangent,
        heads_value,
        output_gate,
        mixer_saved,
        state_write,
        state_read,
        gate_weight,
        up_weight,
        down_weight,
        proj_weight,
    )
    return pl.pallas_call(
        put_out_kernel,
        out_shape=outs,
        in_specs=[vm] * len(outs),
        out_specs=(hbm,) * len(outs),
        scratch_shapes=[DMA((len(outs),))],
        compiler_params=pltpu.CompilerParams(vmem_limit_bytes=12 * MIB),
        name="put_out",
    )(*grads)


def solution(mesh):
    split = P("sp", "tp")
    in_specs = (
        split,
        split,
        P("sp", None),
        P("sp", None),
        P("sp", None, "tp"),
        P("sp", None, "tp"),
        P("sp", "tp", None),
        split,
        split,
        split,
        P(None, "tp"),
        split,
        split,
        split,
    )
    out_specs = (
        P("sp", None, "tp"),
        P("sp", None, "tp"),
        P("sp", "tp", None),
        split,
        split,
        split,
        split,
        split,
    )
    return jax.shard_map(
        on_device, mesh=mesh, in_specs=in_specs, out_specs=out_specs, check_vma=False
    )
```

```python
import functools

import jax
import jax.numpy as jnp
from jax import lax
from jax.experimental import pallas as pl
from jax.experimental.pallas import tpu as pltpu
from jax.sharding import PartitionSpec as P

HEAD_DIM = 64
STATE = 128
MESH = pl.DeviceIdType.MESH
LAST = (((1,), (1,)), ((), ()))
FIRST = (((0,), (0,)), ((), ()))
F32 = jnp.float32
BF16 = jnp.bfloat16
VMEM = pltpu.VMEM
DMA = pltpu.SemaphoreType.DMA
MIB = 1024 * 1024


def silu_parts(value):
    sigma = jax.nn.sigmoid(value)
    return (value * sigma, sigma * (1.0 + value * (1.0 - sigma)))


def dot_first(a, b):
    return lax.dot_general(a, b, FIRST, preferred_element_type=F32)


def dot_last(a, b):
    return lax.dot_general(a, b, LAST, preferred_element_type=F32)


def dot(a, b):
    return jnp.dot(a, b, preferred_element_type=F32)


def exact(a, b, dims=(((1,), (0,)), ((), ()))):
    return lax.dot_general(
        a, b, dims, precision=lax.Precision.HIGHEST, preferred_element_type=F32
    )


def flip(a, b, n):
    out, bit = 0, 1
    while bit < n:
        out = out + lax.rem(lax.div(a, bit) + lax.div(b, bit), 2) * bit
        bit *= 2
    return out


class Place:
    def __init__(self, n, t):
        self.n, self.t = n, t
        self.sp = lax.axis_index("sp")
        self.tp = lax.axis_index("tp")
        self.across = lax.rem(self.tp + t // 2, t)
        self.beside = self.tp + 1 - 2 * lax.rem(self.tp, 2)
        self.cross = lax.rem(self.beside + t // 2, t)

    def mate(self, m):
        return flip(self.sp, jnp.int32(m), self.n)

    def to(self, src, dst, send, recv, sp=None, tp=None):
        return pltpu.make_async_remote_copy(
            src_ref=src,
            dst_ref=dst,
            send_sem=send,
            recv_sem=recv,
            device_id=(self.sp if sp is None else sp, self.tp if tp is None else tp),
            device_id_type=MESH,
        )


def loop(lo, hi, body):
    def step(i, carry):
        body(i)
        return carry

    lax.fori_loop(lo, hi, step, 0)


def layer_kernel(n, t, cap, *refs):
    count = 14
    sources, refs = refs[:count], refs[count:]
    gate_grad, up_grad, down_grad, proj, vg, wg, rg, outg = refs[:8]
    held_in, refs = refs[8 : 8 + count], refs[8 + count :]
    routes, rweight, rates, x_ref, c_ref, vl, og, ms, wl, rl, gate, up, down, pw = held_in
    (
        snd, got, pg, pu, hidden, gd, ud, part, pair, summed, other, final, arr, pick, trow,
        acol, fades, act, slp, ends, twins, joint, lined, lowhigh, delta, ga, full, by, gall,
    ) = refs[:29]
    (
        w_sem, s_a2a, r_a2a, s_sh, r_sh, s_d, r_d, s_p, r_p, s_y, r_y, s_b, r_b, s_r, r_r,
        s_t1, r_t1, s_t2, r_t2, s_t3, r_t3, s_z, r_z, s_l, r_l, s_ls, r_ls, s_x, r_x, s_g, r_g,
        s_gs, r_gs,
    ) = refs[29:]
    at = Place(n, t)
    tokens, d = x_ref.shape
    top = routes.shape[0]
    slots = n * cap
    half = n // 2
    duo = 2 * cap
    heads = rates.shape[0]
    per = heads * STATE // wl.shape[1]
    span = per * HEAD_DIM
    groups = heads // per
    z = lax.div(at.sp, 2)
    bit = lax.rem(at.sp, 2)
    twin = at.sp + 1 - 2 * bit
    col = lambda tp: pl.ds(pl.multiple_of(tp * d, d), d)
    hcol = lambda b: pl.ds(pl.multiple_of(b * (d // 2), d // 2), d // 2)

    barrier = pltpu.get_barrier_semaphore()
    for tp in (at.across, at.beside):
        pl.semaphore_signal(barrier, inc=1, device_id=(at.sp, tp), device_id_type=MESH)

    def hello(o):
        pl.semaphore_signal(
            barrier, inc=1, device_id=(lax.rem(at.sp + o, n), at.tp), device_id_type=MESH
        )

    loop(1, n, hello)
    loads = [
        pltpu.make_async_copy(
            src if len(src.shape) == len(dst.shape) else src.at[0], dst, w_sem.at[i]
        )
        for i, (src, dst) in enumerate(zip(sources, held_in))
    ]
    for load in loads:
        load.start()
    for load in loads[:5]:
        load.wait()

    row_id = lax.broadcasted_iota(jnp.int32, (tokens, tokens), 0)
    col_id = lax.broadcasted_iota(jnp.int32, (tokens, tokens), 1)
    eye = (row_id == col_id).astype(F32)
    named = exact(eye, routes[...].astype(F32), LAST)
    weights = exact(eye, rweight[...], LAST)
    lanes = lax.broadcasted_iota(jnp.int32, (tokens, n), 1).astype(F32)
    onehot = [(named[:, k : k + 1] == lanes).astype(F32) for k in range(top)]
    lower = (row_id > col_id).astype(F32)
    before = dot(lower.astype(BF16), sum(onehot).astype(BF16))
    slot_lane = lax.broadcasted_iota(jnp.int32, (tokens, slots), 1).astype(F32)
    picks = []
    for k in range(top):
        rank = jnp.sum(before * onehot[k], axis=1, keepdims=True)
        picks.append((named[:, k : k + 1] * cap + rank == slot_lane).astype(F32).astype(BF16))
    pick[...] = sum(picks)
    snd[0] = dot_first(pick[...], x_ref[...]).astype(BF16).reshape(n, cap, d)
    cot = c_ref[...].astype(F32)
    weighted = [(cot * weights[:, k : k + 1]).astype(BF16) for k in range(top)]
    snd[1] = dot_first(
        jnp.concatenate(picks, axis=0), jnp.concatenate(weighted, axis=0)
    ).astype(BF16).reshape(n, cap, d)
    for k in (0, 1):
        got[k, 0, :, col(at.tp)] = snd[k, at.sp]
    pl.semaphore_wait(barrier, n + 1)

    def to_columns(value):
        lane = lax.broadcasted_iota(jnp.int32, (heads, d), 1)
        lead = lax.broadcasted_iota(jnp.int32, (heads, d), 0) * HEAD_DIM
        spread_heads = jnp.logical_and(lane >= lead, lane < lead + HEAD_DIM).astype(F32)
        return exact(value, spread_heads, FIRST)

    def prepare():
        upto = (row_id >= col_id).astype(F32)
        acol[...] = exact(upto, to_columns(rates[...]))
        trow[at.sp] = acol[tokens - 1 : tokens, :]
        a = acol[...]
        fades[0] = jnp.exp(a - a[tokens - 1 : tokens, :])
        fades[1] = jnp.exp(-a)
        active_gate, slope_gate = silu_parts(og[...].astype(F32))
        saved = ms[...].astype(F32)
        ga[at.sp] = (saved * active_gate).astype(BF16)
        act[...] = active_gate
        slp[...] = saved * slope_gate

    def states(kind, left, right):
        value = right[...].astype(F32)
        for i in (0, 1):
            faded = (value * fades[i]).astype(BF16)
            for g in range(groups):
                ends[kind, i, :, g * span : (g + 1) * span] = dot_first(
                    left[:, g * STATE : (g + 1) * STATE], faded[:, g * span : (g + 1) * span]
                ).astype(BF16)

    def totals(m):
        mate = at.mate(m)
        return at.to(trow.at[at.sp], trow.at[at.sp], s_d.at[m], r_d.at[m], sp=mate)

    def twin_first(kind):
        cols = hcol(1 - bit)
        return at.to(
            ends.at[kind, :, :, cols], twins.at[kind, :, :, cols], s_t1.at[kind], r_t1.at[kind],
            sp=twin,
        )

    def twin_rest(kind):
        cols = hcol(bit)
        return at.to(
            ends.at[kind, bit, :, cols], twins.at[kind, bit, :, cols], s_t2.at[kind],
            r_t2.at[kind], sp=twin,
        )

    def along(kind, o):
        there = lax.rem(z + o, half)
        return at.to(
            joint.at[kind, jnp.where(there > z, 0, 1)], lined.at[kind, z], s_z.at[kind, o],
            r_z.at[kind, o], sp=there * 2 + bit,
        )

    def twin_last(kind):
        here = lowhigh.at[kind, :, :, hcol(bit)]
        return at.to(here, here, s_t3.at[kind], r_t3.at[kind], sp=twin)

    def join(kind):
        cols = hcol(bit)
        mine = jnp.exp(-trow[at.sp, :, cols])
        his = jnp.exp(-trow[twin, :, cols])
        second = (bit == 1).astype(F32)
        keep_end = second + (1.0 - second) * his
        his_end = (1.0 - second) + second * mine
        keep_start = (1.0 - second) + second * his
        his_start = second + (1.0 - second) * mine
        own = ends[kind, :, :, cols].astype(F32)
        got_twin = twins[kind, :, :, cols].astype(F32)
        joint[kind, 0] = (own[0] * keep_end + got_twin[0] * his_end).astype(BF16)
        joint[kind, 1] = (own[1] * keep_start + got_twin[1] * his_start).astype(BF16)

    def send_along(kind):
        loop(1, half, lambda o: along(kind, o).start())

    def gather_states(kind):
        cols = hcol(bit)
        loop(1, half, lambda o: along(kind, o).wait_recv())

        def both(y):
            return trow[2 * y, :, cols] + trow[2 * y + 1, :, cols]

        zero = jnp.zeros((STATE, d // 2), F32)

        def before_me(i, carry):
            total, fade = carry
            y = z - 1 - i
            total = total + jnp.exp(-fade) * lined[kind, y].astype(F32)
            return total, fade + both(y)

        def after_me(i, carry):
            total, fade = carry
            y = z + 1 + i
            total = total + jnp.exp(-fade) * lined[kind, y].astype(F32)
            return total, fade + both(y)

        none = jnp.zeros((1, d // 2), F32)
        low, _ = lax.fori_loop(0, z, before_me, (zero, none))
        high, _ = lax.fori_loop(0, half - 1 - z, after_me, (zero, none))
        lowhigh[kind, 0, :, cols] = low.astype(BF16)
        lowhigh[kind, 1, :, cols] = high.astype(BF16)

    def reach(kind):
        his = jnp.exp(-trow[twin])
        second = (bit == 1).astype(F32)
        extra = twins[kind, 1 - bit].astype(F32)
        low = lowhigh[kind, 0].astype(F32) * (1.0 - second + second * his) + extra * second
        high = lowhigh[kind, 1].astype(F32) * (second + (1.0 - second) * his) + extra * (
            1.0 - second
        )
        return low.astype(BF16), high.astype(BF16)

    def hop(up, k):
        here = ga.at[(z - k if up else z + k) * 2 + bit]
        i = 0 if up else 1
        peer = z + 1 if up else z - 1
        return at.to(here, here, s_l.at[i, k], r_l.at[i, k], sp=peer * 2 + bit)

    def came(up, k):
        here = ga.at[(z - k if up else z + k) * 2 + bit]
        i = 0 if up else 1
        return at.to(here, here, s_l.at[i, k], r_l.at[i, k - 1], sp=twin)

    def side(up, k):
        here = ga.at[(z - k if up else z + k) * 2 + bit]
        i = 0 if up else 1
        return at.to(here, here, s_ls.at[i, k], r_ls.at[i, k], sp=twin)

    def pair_gated():
        return at.to(ga.at[at.sp], ga.at[at.sp], s_x.at[0], r_x.at[0], sp=twin)

    def begin_gated():
        @pl.when(z < half - 1)
        def _():
            hop(True, 0).start()

        @pl.when(z > 0)
        def _():
            hop(False, 0).start()

    def pass_on(k):
        @pl.when(z - k >= 0)
        def _():
            came(True, k).wait_recv()

            @pl.when(z < half - 1)
            def _():
                hop(True, k).start()

        @pl.when(z + k < half)
        def _():
            came(False, k).wait_recv()

            @pl.when(z > 0)
            def _():
                hop(False, k).start()

    def sides(k):
        @pl.when(z - k >= 0)
        def _():
            side(True, k).start()

        @pl.when(z + k < half)
        def _():
            side(False, k).start()

    def spread(k, m):
        mate = at.mate(m)
        return at.to(
            snd.at[k, mate], got.at[k, m, :, col(at.tp)], s_a2a.at[k, m], r_a2a.at[k, m], sp=mate
        )

    def share(k, m, j):
        here = got.at[k, m, :, col(at.across if j == 2 else at.tp)]
        return at.to(
            here, here, s_sh.at[k, j, m], r_sh.at[k, j, m], tp=at.across if j == 0 else at.beside
        )

    def place_of(k, i):
        return jnp.where(jnp.logical_and(k == 1, i > 1), n + 1 - i, i)

    for k in (0, 1):
        loop(1, n, lambda i: spread(k, place_of(k, i)).start())
    for k in (0, 1):
        share(k, 0, 0).start()
        share(k, 0, 1).start()
    for load in loads[5:10]:
        load.wait()
    prepare()
    states(0, wl, vl)
    loop(1, n, lambda m: totals(m).start())
    twin_first(0).start()
    twin_rest(0).start()
    pair_gated().start()

    lag = 2

    def forward(q):
        k, i = lax.div(q, n), lax.rem(q, n)
        m = place_of(k, i)

        @pl.when(i > 0)
        def _():
            spread(k, m).wait_recv()
            share(k, m, 0).start()
            share(k, m, 1).start()

        @pl.when(q >= lag)
        def _():
            relay(q - lag)

    def relay(q):
        k = lax.div(q, n)
        m = place_of(k, lax.rem(q, n))
        share(k, m, 0).wait_recv()
        share(k, m, 2).start()

    def settled(k, base):
        for m in (2 * base, 2 * base + 1):
            share(k, m, 1).wait_recv()
            share(k, m, 2).wait_recv()

    def base_of(j):
        return jnp.where(jnp.int32(j) < 1, 0, half - j)

    def rows_of(base):
        return pl.ds(pl.multiple_of(base * duo, duo), duo)

    def ahead(j):
        base = base_of(j)
        settled(0, base)
        rows = rows_of(base)
        inputs = got[0, pl.ds(2 * base, 2)].reshape(duo, t * d)
        pg[rows, :] = dot(inputs, gate[...])
        pu[rows, :] = dot(inputs, up[...])

    def behind(j):
        base = base_of(j)
        settled(1, base)
        rows = rows_of(base)
        sent = got[1, pl.ds(2 * base, 2)].reshape(duo, t * d)
        grad = dot_last(sent, down[...])
        active, slope = silu_parts(pg[rows, :])
        ups = pu[rows, :]
        hidden[rows, :] = (active * ups).astype(BF16)
        gd[rows, :] = (grad * ups * slope).astype(BF16)
        ud[rows, :] = (grad * active).astype(BF16)

    loop(1, n, forward)
    for load in loads[10:13]:
        load.wait()

    def halves(m, k):
        c = at.cross if k == 0 else at.beside
        return at.to(
            part.at[m, :, col(c)], pair.at[k, m], s_p.at[k, m], r_p.at[k, m], tp=at.beside
        )

    def over(m):
        return at.to(summed.at[m], other.at[m], s_y.at[m], r_y.at[m], tp=at.across)

    def back(m):
        return at.to(final.at[m], arr.at[at.sp], s_b.at[m], r_b.at[m], sp=at.mate(m))

    def produce(jj):
        base = base_of(jj)
        rows = rows_of(base)
        for c in range(t):
            cols = slice(c * d, (c + 1) * d)
            value = dot_last(gd[rows, :], gate[cols, :]) + dot_last(ud[rows, :], up[cols, :])
            part[pl.ds(2 * base, 2), :, cols] = value.astype(BF16).reshape(2, cap, d)
        for m in (2 * base, 2 * base + 1):
            for k in (0, 1):
                halves(m, k).start()

    def pass_over(jj):
        base = base_of(jj)
        for m in (2 * base, 2 * base + 1):
            halves(m, 0).wait_recv()
            summed[m] = (
                part[m, :, col(at.across)].astype(F32) + pair[0, m].astype(F32)
            ).astype(BF16)
            over(m).start()

    def total(jj):
        base = base_of(jj)
        for m in (2 * base, 2 * base + 1):
            halves(m, 1).wait_recv()
            over(m).wait_recv()
            final[m] = (
                part[m, :, col(at.tp)].astype(F32) + pair[1, m].astype(F32) + other[m].astype(F32)
            ).astype(BF16)

            @pl.when(m > 0)
            def _():
                back(m).start()

    def weight_grads(c):
        cols = pl.ds(pl.multiple_of(c * d, d), d)
        inputs = got[0, :, :, cols].reshape(slots, d)
        gate_grad[0, cols, :] = dot_first(inputs, gd[...]).astype(BF16)
        up_grad[0, cols, :] = dot_first(inputs, ud[...]).astype(BF16)
        sent = got[1, :, :, cols].reshape(slots, d)
        down_grad[0, :, cols] = dot_first(hidden[...], sent).astype(BF16)

    def second(j):
        ahead(j)
        forward(n + 2 * j)
        forward(n + 2 * j + 1)

        @pl.when(j > 0)
        def _():
            behind(j - 1)
            produce(j - 1)

        @pl.when(j > 1)
        def _():
            pass_over(j - 2)

        @pl.when(j > 2)
        def _():
            total(j - 3)

    loop(0, half, second)
    begin_gated()
    loop(2 * n - lag, 2 * n, relay)
    behind(half - 1)
    produce(half - 1)
    if half > 1:
        pass_over(half - 2)
    if half > 2:
        total(half - 3)
    weight_grads(0)
    pass_over(half - 1)
    if half > 1:
        weight_grads(1)
        total(half - 2)
    weight_grads(2)
    total(half - 1)
    for c in range(3, t):
        weight_grads(c)
    if half > 1:
        pass_on(1)
        sides(1)
    loop(1, n, lambda m: totals(m).wait_recv())
    twin_first(0).wait_recv()
    join(0)
    send_along(0)
    arr[at.sp] = final[0]
    loop(1, n, lambda i: back(n - i).wait_recv())

    moe_grad = dot(pick[...], arr[...].reshape(slots, d))
    full[:, col(at.tp)] = (c_ref[...].astype(F32) + moe_grad).astype(BF16)

    def rows_to(j):
        here = full.at[:, col(at.across if j == 2 else at.tp)]
        return at.to(here, here, s_r.at[j], r_r.at[j], tp=at.across if j == 0 else at.beside)

    def through(tp):
        rows = pl.ds(pl.multiple_of(tp * d, d), d)
        return dot(full[:, col(tp)], pw[rows, :])

    rows_to(0).start()
    rows_to(1).start()
    loads[13].wait()
    out_delta = through(at.tp)

    def both(k):
        pass_on(k)
        sides(k)

    if half > 2:
        loop(2, half - 1, both)
    rows_to(1).wait_recv()
    out_delta = out_delta + through(at.beside)
    rows_to(0).wait_recv()
    rows_to(2).start()
    out_delta = out_delta + through(at.across)
    rows_to(2).wait_recv()
    out_delta = (out_delta + through(at.cross)).astype(BF16).astype(F32)
    delta[...] = (out_delta * act[...]).astype(BF16)
    states(1, rl, delta)
    twin_first(1).start()
    twin_rest(1).start()
    outg[...] = (out_delta * slp[...]).astype(BF16)

    q = tokens // t
    width = gall.shape[2]
    row = lambda tp: pl.ds(pl.multiple_of(tp * q, q), q)
    quarter = full[row(at.tp), :]
    for o in range(n):
        by[o] = quarter[:, o * width : (o + 1) * width]

    def spread_g(m):
        mate = at.mate(m)
        return at.to(
            by.at[mate], gall.at[at.sp, row(at.tp), :], s_g.at[m], r_g.at[m], sp=mate
        )

    def share_g(m, j):
        here = gall.at[at.mate(m), row(at.across if j == 2 else at.tp), :]
        return at.to(
            here, here, s_gs.at[j, m], r_gs.at[j, m], tp=at.across if j == 0 else at.beside
        )

    gall[at.sp, row(at.tp), :] = by[at.sp]
    loop(1, n, lambda i: spread_g(i).start())
    share_g(0, 0).start()
    share_g(0, 1).start()

    arow = exact(rates[...], (row_id <= col_id).astype(F32))
    inner = []
    scores = []
    for g in range(groups):
        wide = slice(g * STATE, (g + 1) * STATE)
        common = dot_last(wl[:, wide], rl[:, wide])
        score = jnp.zeros((tokens, tokens), F32)
        for h in range(g * per, (g + 1) * per):
            cols = slice(h * HEAD_DIM, (h + 1) * HEAD_DIM)
            fade = jnp.exp(
                -jnp.abs(acol[:, h * HEAD_DIM : h * HEAD_DIM + 1] - arow[h : h + 1, :])
            )
            inner.append(dot((fade * common).astype(BF16), delta[:, cols]))
            score += fade * dot_last(vl[:, cols], delta[:, cols])
        scores.append(score.astype(BF16))

    twin_first(1).wait_recv()
    join(1)
    send_along(1)
    if half > 2:
        both(half - 1)
    gather_states(0)
    twin_last(0).start()

    def forward_g(m):
        spread_g(m).wait_recv()
        share_g(m, 0).start()
        share_g(m, 1).start()

    loop(1, n, forward_g)

    def relay_g(m):
        share_g(m, 0).wait_recv()
        share_g(m, 2).start()

    loop(0, n, relay_g)
    gather_states(1)
    twin_last(1).start()

    def settle_g(m):
        share_g(m, 1).wait_recv()
        share_g(m, 2).wait_recv()

    loop(0, n, settle_g)
    pair_gated().wait_recv()

    def settle_gated(k):
        @pl.when(z - k >= 0)
        def _():
            side(True, k).wait_recv()

        @pl.when(z + k < half)
        def _():
            side(False, k).wait_recv()

    loop(1, half, settle_gated)
    proj[...] = dot_first(
        gall[...].reshape(n * tokens, width), ga[...].reshape(n * tokens, d)
    )
    twin_rest(0).wait_recv()
    twin_last(0).wait_recv()
    to_end, to_start = fades[0], fades[1]
    w_low, w_high = reach(0)
    value = vl[...].astype(F32)
    moved = delta[...].astype(F32)
    d_start, d_end = (moved * to_start).astype(BF16), (moved * to_end).astype(BF16)
    v_start, v_end = (value * to_start).astype(BF16), (value * to_end).astype(BF16)
    for g in range(groups):
        wide = slice(g * STATE, (g + 1) * STATE)
        cols = slice(g * span, (g + 1) * span)
        rg[:, wide] = (
            dot_first(scores[g], wl[:, wide])
            + dot_last(d_start[:, cols], w_low[:, cols])
            + dot_last(d_end[:, cols], w_high[:, cols])
        ).astype(BF16)

    twin_rest(1).wait_recv()
    twin_last(1).wait_recv()
    r_low, r_high = reach(1)
    for g in range(groups):
        wide = slice(g * STATE, (g + 1) * STATE)
        cols = slice(g * span, (g + 1) * span)
        wg[:, wide] = (
            dot(scores[g], rl[:, wide])
            + dot_last(v_start[:, cols], r_low[:, cols])
            + dot_last(v_end[:, cols], r_high[:, cols])
        ).astype(BF16)
        vg[:, cols] = (
            jnp.concatenate(inner[g * per : (g + 1) * per], axis=1)
            + dot(wl[:, wide], r_low[:, cols]) * to_start[:, cols]
            + dot(wl[:, wide], r_high[:, cols]) * to_end[:, cols]
        ).astype(BF16)

    def finish(m):
        for k in (0, 1):
            for j in (0, 1, 2):
                share(k, m, j).wait_send()
            halves(m, k).wait_send()
        over(m).wait_send()
        for j in (0, 1, 2):
            share_g(m, j).wait_send()

    loop(0, n, finish)

    def finish_sp(m):
        for k in (0, 1):
            spread(k, m).wait_send()
        back(m).wait_send()
        totals(m).wait_send()
        spread_g(m).wait_send()

    loop(1, n, finish_sp)
    for j in (0, 1, 2):
        rows_to(j).wait_send()
    for kind in (0, 1):
        twin_first(kind).wait_send()
        twin_rest(kind).wait_send()
        twin_last(kind).wait_send()
        loop(1, half, lambda o: along(kind, o).wait_send())
    pair_gated().wait_send()

    def drain(k):
        @pl.when(jnp.logical_and(z - k >= 0, z < half - 1))
        def _():
            hop(True, k).wait_send()

        @pl.when(jnp.logical_and(z + k < half, z > 0))
        def _():
            hop(False, k).wait_send()

    loop(0, half, drain)

    def drain_sides(k):
        @pl.when(z - k >= 0)
        def _():
            side(True, k).wait_send()

        @pl.when(z + k < half)
        def _():
            side(False, k).wait_send()

    loop(1, half, drain_sides)


def put_out_kernel(*refs):
    count = len(refs) // 2
    copies = [
        pltpu.make_async_copy(refs[i], refs[count + i], refs[-1].at[i]) for i in range(count)
    ]
    for copy in copies:
        copy.start()
    for copy in copies:
        copy.wait()


def held(scratch):
    shape, size = scratch.shape, jnp.dtype(scratch.dtype).itemsize
    minor = -(-shape[-1] // 128) * 128
    rows = -(-shape[-2] // 16) * 16
    return functools.reduce(lambda a, b: a * b, shape[:-2], minor * rows * size)


def on_device(
    layer_input,
    cotangent,
    routes,
    route_weight,
    gate_weight,
    up_weight,
    down_weight,
    heads_value,
    output_gate,
    mixer_saved,
    proj_weight,
    state_write,
    state_read,
    decay_rate,
):
    n = lax.axis_size("sp")
    t = lax.axis_size("tp")
    tokens, d = layer_input.shape
    top = routes.shape[1]
    capacity = -(-max(2, 3 * tokens * top // (2 * n)) // 16) * 16
    slots = n * capacity
    hid = gate_weight.shape[2]
    half = n // 2
    width = t * d // n
    state_w = state_write.shape[1]
    sds = jax.ShapeDtypeStruct
    block = (n, capacity, d)
    vm = pl.BlockSpec(memory_space=pltpu.VMEM)
    hbm = pl.BlockSpec(memory_space=pltpu.HBM)
    sems = [
        (14,), (2, n), (2, n), (2, 3, n), (2, 3, n), (n,), (n,), (2, n), (2, n), (n,), (n,),
        (n,), (n,), (3,), (3,),
        (2,), (2,), (2,), (2,), (2,), (2,), (2, half), (2, half), (2, half), (2, half),
        (2, half), (2, half), (1,), (1,), (n,), (n,), (3, n), (3, n),
    ]
    outs = (
        sds((1, t * d, hid), BF16),
        sds((1, t * d, hid), BF16),
        sds((1, hid, t * d), BF16),
        sds((width, d), F32),
        sds((tokens, d), BF16),
        sds((tokens, state_w), BF16),
        sds((tokens, state_w), BF16),
        sds((tokens, d), BF16),
    )
    operands = (
        routes.T,
        route_weight.T,
        decay_rate.T,
        layer_input,
        cotangent,
        heads_value,
        output_gate,
        mixer_saved,
        state_write,
        state_read,
        gate_weight,
        up_weight,
        down_weight,
        proj_weight,
    )
    scratch = [VMEM(x.shape[-2:], x.dtype) for x in operands] + [
        VMEM((2,) + block, BF16),
        VMEM((2, n, capacity, t * d), BF16),
        VMEM((slots, hid), F32),
        VMEM((slots, hid), F32),
        VMEM((slots, hid), BF16),
        VMEM((slots, hid), BF16),
        VMEM((slots, hid), BF16),
        VMEM((n, capacity, t * d), BF16),
        VMEM((2,) + block, BF16),
        VMEM(block, BF16),
        VMEM(block, BF16),
        VMEM(block, BF16),
        VMEM(block, BF16),
        VMEM((tokens, slots), BF16),
        VMEM((n, 1, d), F32),
        VMEM((tokens, d), F32),
        VMEM((2, tokens, d), F32),
        VMEM((tokens, d), F32),
        VMEM((tokens, d), F32),
        VMEM((2, 2, STATE, d), BF16),
        VMEM((2, 2, STATE, d), BF16),
        VMEM((2, 2, STATE, d // 2), BF16),
        VMEM((2, half, STATE, d // 2), BF16),
        VMEM((2, 2, STATE, d), BF16),
        VMEM((tokens, d), BF16),
        VMEM((n, tokens, d), BF16),
        VMEM((tokens, t * d), BF16),
        VMEM((n, tokens // t, width), BF16),
        VMEM((n, tokens, width), BF16),
    ]
    grads = pl.pallas_call(
        functools.partial(layer_kernel, n, t, capacity),
        out_shape=outs,
        in_specs=[hbm] * 14,
        out_specs=(vm,) * 8,
        scratch_shapes=scratch + [DMA(shape) for shape in sems],
        compiler_params=pltpu.CompilerParams(
            collective_id=1,
            has_side_effects=True,
            vmem_limit_bytes=min(60 * MIB, sum(map(held, scratch)) + 8 * MIB),
        ),
        cost_estimate=pl.CostEstimate(
            flops=4_000_000_000, bytes_accessed=8_000_000, transcendentals=0
        ),
        name="layer",
    )(*(pltpu.with_memory_space_constraint(x, pltpu.HBM) for x in operands))
    return pl.pallas_call(
        put_out_kernel,
        out_shape=outs,
        in_specs=[vm] * len(outs),
        out_specs=(hbm,) * len(outs),
        scratch_shapes=[DMA((len(outs),))],
        compiler_params=pltpu.CompilerParams(vmem_limit_bytes=12 * MIB),
        name="put_out",
    )(*grads)


def solution(mesh):
    split = P("sp", "tp")
    in_specs = (
        split,
        split,
        P("sp", None),
        P("sp", None),
        P("sp", None, "tp"),
        P("sp", None, "tp"),
        P("sp", "tp", None),
        split,
        split,
        split,
        P(None, "tp"),
        split,
        split,
        split,
    )
    out_specs = (
        P("sp", None, "tp"),
        P("sp", None, "tp"),
        P("sp", "tp", None),
        split,
        split,
        split,
        split,
        split,
    )
    return jax.shard_map(
        on_device, mesh=mesh, in_specs=in_specs, out_specs=out_specs, check_vma=False
    )
```

```python
import functools

import jax
import jax.numpy as jnp
from jax import lax
from jax.experimental import pallas as pl
from jax.experimental.pallas import tpu as pltpu
from jax.sharding import PartitionSpec as P

HEAD_DIM = 64
STATE = 128
MESH = pl.DeviceIdType.MESH
LAST = (((1,), (1,)), ((), ()))
FIRST = (((0,), (0,)), ((), ()))
F32 = jnp.float32
BF16 = jnp.bfloat16
VMEM = pltpu.VMEM
DMA = pltpu.SemaphoreType.DMA
MIB = 1024 * 1024


def silu_parts(value):
    sigma = jax.nn.sigmoid(value)
    return (value * sigma, sigma * (1.0 + value * (1.0 - sigma)))


def dot_first(a, b):
    return lax.dot_general(a, b, FIRST, preferred_element_type=F32)


def dot_last(a, b):
    return lax.dot_general(a, b, LAST, preferred_element_type=F32)


def dot(a, b):
    return jnp.dot(a, b, preferred_element_type=F32)


def exact(a, b, dims=(((1,), (0,)), ((), ()))):
    return lax.dot_general(
        a, b, dims, precision=lax.Precision.HIGHEST, preferred_element_type=F32
    )


def flip(a, b, n):
    out, bit = 0, 1
    while bit < n:
        out = out + lax.rem(lax.div(a, bit) + lax.div(b, bit), 2) * bit
        bit *= 2
    return out


class Place:
    def __init__(self, n, t):
        self.n, self.t = n, t
        self.sp = lax.axis_index("sp")
        self.tp = lax.axis_index("tp")
        self.across = lax.rem(self.tp + t // 2, t)
        self.beside = self.tp + 1 - 2 * lax.rem(self.tp, 2)
        self.cross = lax.rem(self.beside + t // 2, t)

    def mate(self, m):
        return flip(self.sp, jnp.int32(m), self.n)

    def to(self, src, dst, send, recv, sp=None, tp=None):
        return pltpu.make_async_remote_copy(
            src_ref=src,
            dst_ref=dst,
            send_sem=send,
            recv_sem=recv,
            device_id=(self.sp if sp is None else sp, self.tp if tp is None else tp),
            device_id_type=MESH,
        )


def loop(lo, hi, body):
    def step(i, carry):
        body(i)
        return carry

    lax.fori_loop(lo, hi, step, 0)


def layer_kernel(n, t, cap, *refs):
    count = 14
    sources, refs = refs[:count], refs[count:]
    gate_grad, up_grad, down_grad, proj, vg, wg, rg, outg = refs[:8]
    held_in, refs = refs[8 : 8 + count], refs[8 + count :]
    routes, rweight, rates, x_ref, c_ref, vl, og, ms, wl, rl, gate, up, down, pw = held_in
    (
        snd, got, pg, pu, hidden, gd, ud, part, pair, summed, other, final, arr, pick, trow,
        acol, fades, act, slp, ends, twins, joint, lined, lowhigh, delta, ga, full, by, gall,
    ) = refs[:29]
    (
        w_sem, s_a2a, r_a2a, s_sh, r_sh, r_side, s_d, r_d, s_p, r_p, s_y, r_y, s_b, r_b, s_r, r_r,
        s_t1, r_t1, s_t2, r_t2, s_t3, r_t3, s_z, r_z, s_l, r_l, s_ls, r_ls, s_x, r_x, s_g, r_g,
        s_gs, r_gs,
    ) = refs[29:]
    at = Place(n, t)
    tokens, d = x_ref.shape
    top = routes.shape[0]
    slots = n * cap
    half = n // 2
    duo = 2 * cap
    heads = rates.shape[0]
    per = heads * STATE // wl.shape[1]
    span = per * HEAD_DIM
    groups = heads // per
    z = lax.div(at.sp, 2)
    bit = lax.rem(at.sp, 2)
    twin = at.sp + 1 - 2 * bit
    mate_one = twin
    col = lambda tp: pl.ds(pl.multiple_of(tp * d, d), d)
    hcol = lambda b: pl.ds(pl.multiple_of(b * (d // 2), d // 2), d // 2)

    barrier = pltpu.get_barrier_semaphore()
    for tp in (at.across, at.beside):
        pl.semaphore_signal(barrier, inc=1, device_id=(at.sp, tp), device_id_type=MESH)

    def hello(o):
        pl.semaphore_signal(
            barrier, inc=1, device_id=(lax.rem(at.sp + o, n), at.tp), device_id_type=MESH
        )

    loop(1, n, hello)
    loads = [
        pltpu.make_async_copy(
            src if len(src.shape) == len(dst.shape) else src.at[0], dst, w_sem.at[i]
        )
        for i, (src, dst) in enumerate(zip(sources, held_in))
    ]
    for load in loads:
        load.start()
    for load in loads[:5]:
        load.wait()

    row_id = lax.broadcasted_iota(jnp.int32, (tokens, tokens), 0)
    col_id = lax.broadcasted_iota(jnp.int32, (tokens, tokens), 1)
    eye = (row_id == col_id).astype(F32)
    named = exact(eye, routes[...].astype(F32), LAST)
    weights = exact(eye, rweight[...], LAST)
    lanes = lax.broadcasted_iota(jnp.int32, (tokens, n), 1).astype(F32)
    onehot = [(named[:, k : k + 1] == lanes).astype(F32) for k in range(top)]
    lower = (row_id > col_id).astype(F32)
    before = dot(lower.astype(BF16), sum(onehot).astype(BF16))
    slot_lane = lax.broadcasted_iota(jnp.int32, (tokens, slots), 1).astype(F32)
    picks = []
    for k in range(top):
        rank = jnp.sum(before * onehot[k], axis=1, keepdims=True)
        picks.append((named[:, k : k + 1] * cap + rank == slot_lane).astype(F32).astype(BF16))
    pick[...] = sum(picks)
    snd[0] = dot_first(pick[...], x_ref[...]).astype(BF16).reshape(n, cap, d)
    cot = c_ref[...].astype(F32)
    weighted = [(cot * weights[:, k : k + 1]).astype(BF16) for k in range(top)]
    snd[1] = dot_first(
        jnp.concatenate(picks, axis=0), jnp.concatenate(weighted, axis=0)
    ).astype(BF16).reshape(n, cap, d)
    for k in (0, 1):
        got[k, 0, :, col(at.tp)] = snd[k, at.sp]
    pl.semaphore_wait(barrier, n + 1)

    def whole(ref, sem):
        return at.to(ref, ref, sem, sem, sp=mate_one)

    def to_columns(value):
        lane = lax.broadcasted_iota(jnp.int32, (heads, d), 1)
        lead = lax.broadcasted_iota(jnp.int32, (heads, d), 0) * HEAD_DIM
        spread_heads = jnp.logical_and(lane >= lead, lane < lead + HEAD_DIM).astype(F32)
        return exact(value, spread_heads, FIRST)

    def prepare():
        upto = (row_id >= col_id).astype(F32)
        acol[...] = exact(upto, to_columns(rates[...]))
        trow[at.sp] = acol[tokens - 1 : tokens, :]
        a = acol[...]
        fades[0] = jnp.exp(a - a[tokens - 1 : tokens, :])
        fades[1] = jnp.exp(-a)
        active_gate, slope_gate = silu_parts(og[...].astype(F32))
        saved = ms[...].astype(F32)
        ga[at.sp] = (saved * active_gate).astype(BF16)
        act[...] = active_gate
        slp[...] = saved * slope_gate

    def states(kind, left, right):
        value = right[...].astype(F32)
        for i in (0, 1):
            faded = (value * fades[i]).astype(BF16)
            for g in range(groups):
                ends[kind, i, :, g * span : (g + 1) * span] = dot_first(
                    left[:, g * STATE : (g + 1) * STATE], faded[:, g * span : (g + 1) * span]
                ).astype(BF16)

    def totals(m):
        mate = at.mate(m)
        return at.to(trow.at[at.sp], trow.at[at.sp], s_d.at[0], r_d.at[0], sp=mate)

    def twin_first(kind):
        cols = hcol(1 - bit)
        return at.to(
            ends.at[kind, :, :, cols], twins.at[kind, :, :, cols], s_t1.at[0], r_t1.at[kind],
            sp=twin,
        )

    def twin_rest(kind):
        cols = hcol(bit)
        return at.to(
            ends.at[kind, bit, :, cols], twins.at[kind, bit, :, cols], s_t2.at[0],
            r_t2.at[kind], sp=twin,
        )

    def along(kind, o):
        there = lax.rem(z + o, half)
        return at.to(
            joint.at[kind, jnp.where(there > z, 0, 1)], lined.at[kind, z], s_z.at[0],
            r_z.at[kind], sp=there * 2 + bit,
        )

    def twin_last(kind):
        here = lowhigh.at[kind, :, :, hcol(bit)]
        return at.to(here, here, s_t3.at[0], r_t3.at[kind], sp=twin)

    def join(kind):
        cols = hcol(bit)
        mine = jnp.exp(-trow[at.sp, :, cols])
        his = jnp.exp(-trow[twin, :, cols])
        second = (bit == 1).astype(F32)
        keep_end = second + (1.0 - second) * his
        his_end = (1.0 - second) + second * mine
        keep_start = (1.0 - second) + second * his
        his_start = second + (1.0 - second) * mine
        own = ends[kind, :, :, cols].astype(F32)
        got_twin = twins[kind, :, :, cols].astype(F32)
        joint[kind, 0] = (own[0] * keep_end + got_twin[0] * his_end).astype(BF16)
        joint[kind, 1] = (own[1] * keep_start + got_twin[1] * his_start).astype(BF16)

    def send_along(kind):
        loop(1, half, lambda o: along(kind, o).start())

    def gather_states(kind):
        cols = hcol(bit)
        whole(lined.at[kind, pl.ds(1, half - 1)], r_z.at[kind]).wait_recv()

        def both(y):
            return trow[2 * y, :, cols] + trow[2 * y + 1, :, cols]

        zero = jnp.zeros((STATE, d // 2), F32)

        def before_me(i, carry):
            total, fade = carry
            y = z - 1 - i
            total = total + jnp.exp(-fade) * lined[kind, y].astype(F32)
            return total, fade + both(y)

        def after_me(i, carry):
            total, fade = carry
            y = z + 1 + i
            total = total + jnp.exp(-fade) * lined[kind, y].astype(F32)
            return total, fade + both(y)

        none = jnp.zeros((1, d // 2), F32)
        low, _ = lax.fori_loop(0, z, before_me, (zero, none))
        high, _ = lax.fori_loop(0, half - 1 - z, after_me, (zero, none))
        lowhigh[kind, 0, :, cols] = low.astype(BF16)
        lowhigh[kind, 1, :, cols] = high.astype(BF16)

    def reach(kind):
        his = jnp.exp(-trow[twin])
        second = (bit == 1).astype(F32)
        extra = twins[kind, 1 - bit].astype(F32)
        low = lowhigh[kind, 0].astype(F32) * (1.0 - second + second * his) + extra * second
        high = lowhigh[kind, 1].astype(F32) * (second + (1.0 - second) * his) + extra * (
            1.0 - second
        )
        return low.astype(BF16), high.astype(BF16)

    def hop(up, k):
        here = ga.at[(z - k if up else z + k) * 2 + bit]
        i = 0 if up else 1
        peer = z + 1 if up else z - 1
        return at.to(here, here, s_l.at[i, k], r_l.at[i, k], sp=peer * 2 + bit)

    def came(up, k):
        here = ga.at[(z - k if up else z + k) * 2 + bit]
        i = 0 if up else 1
        return at.to(here, here, s_l.at[i, k], r_l.at[i, k - 1], sp=twin)

    def side(up, k):
        here = ga.at[(z - k if up else z + k) * 2 + bit]
        i = 0 if up else 1
        return at.to(here, here, s_ls.at[0], r_ls.at[0], sp=twin)

    def pair_gated():
        return at.to(ga.at[at.sp], ga.at[at.sp], s_x.at[0], r_x.at[0], sp=twin)

    outer_up = jnp.logical_or(z == 0, z == half - 2)
    outer_down = jnp.logical_or(z == half - 1, z == 1)

    def begin_gated(outer):
        @pl.when(jnp.logical_and(z < half - 1, outer_up == outer))
        def _():
            hop(True, 0).start()

        @pl.when(jnp.logical_and(z > 0, outer_down == outer))
        def _():
            hop(False, 0).start()

    def pass_on(k, up_if=None, down_if=None):
        up, down = z - k >= 0, z + k < half
        if up_if is not None:
            up, down = jnp.logical_and(up, up_if), jnp.logical_and(down, down_if)

        @pl.when(up)
        def _():
            came(True, k).wait_recv()

            @pl.when(z < half - 1)
            def _():
                hop(True, k).start()

        @pl.when(down)
        def _():
            came(False, k).wait_recv()

            @pl.when(z > 0)
            def _():
                hop(False, k).start()

    def sides(k):
        @pl.when(z - k >= 0)
        def _():
            side(True, k).start()

        @pl.when(z + k < half)
        def _():
            side(False, k).start()

    def spread(k, m):
        mate = at.mate(m)
        return at.to(
            snd.at[k, mate], got.at[k, m, :, col(at.tp)], s_a2a.at[0], r_a2a.at[k, m], sp=mate
        )

    def share(k, m, j):
        here = got.at[k, m, :, col(at.across if j == 2 else at.tp)]
        came_sem = r_sh.at[k, m] if j == 0 else r_side.at[k, lax.div(m, 2)]
        return at.to(here, here, s_sh.at[0], came_sem, tp=at.across if j == 0 else at.beside)

    def place_of(k, i):
        return jnp.where(jnp.logical_and(k == 1, i > 1), n + 1 - i, i)

    for k in (0, 1):
        loop(1, n, lambda i: spread(k, place_of(k, i)).start())
    for k in (0, 1):
        share(k, jnp.int32(0), 0).start()
        share(k, jnp.int32(0), 1).start()
    for load in loads[5:10]:
        load.wait()
    prepare()
    states(0, wl, vl)
    loop(1, n, lambda m: totals(m).start())
    twin_first(0).start()
    twin_rest(0).start()
    pair_gated().start()
    begin_gated(True)

    lag = 3

    def forward(q):
        k, i = lax.div(q, n), lax.rem(q, n)
        m = place_of(k, i)

        @pl.when(i > 0)
        def _():
            spread(k, m).wait_recv()
            share(k, m, 0).start()
            share(k, m, 1).start()

        @pl.when(q >= lag)
        def _():
            relay(q - lag)

    def relay(q):
        k = lax.div(q, n)
        m = place_of(k, lax.rem(q, n))
        share(k, jnp.int32(m), 0).wait_recv()
        share(k, m, 2).start()

    def settled(k, base):
        whole(got.at[k, pl.ds(2 * base, 2), :, 0 : 2 * d], r_side.at[k, base]).wait_recv()

    def base_of(j):
        return jnp.where(jnp.int32(j) < 1, 0, half - j)

    def rows_of(base):
        return pl.ds(pl.multiple_of(base * duo, duo), duo)

    def ahead(j):
        base = base_of(j)
        settled(0, base)
        rows = rows_of(base)
        inputs = got[0, pl.ds(2 * base, 2)].reshape(duo, t * d)
        pg[rows, :] = dot(inputs, gate[...])
        pu[rows, :] = dot(inputs, up[...])

    def behind(j):
        base = base_of(j)
        settled(1, base)
        rows = rows_of(base)
        sent = got[1, pl.ds(2 * base, 2)].reshape(duo, t * d)
        grad = dot_last(sent, down[...])
        active, slope = silu_parts(pg[rows, :])
        ups = pu[rows, :]
        hidden[rows, :] = (active * ups).astype(BF16)
        gd[rows, :] = (grad * ups * slope).astype(BF16)
        ud[rows, :] = (grad * active).astype(BF16)

    loop(1, n, forward)
    for load in loads[10:13]:
        load.wait()

    def halves(m, k):
        c = at.cross if k == 0 else at.beside
        return at.to(
            part.at[m, :, col(c)], pair.at[k, m], s_p.at[0], r_p.at[k, lax.div(m, 2)], tp=at.beside
        )

    def over(m):
        return at.to(summed.at[m], other.at[m], s_y.at[0], r_y.at[lax.div(m, 2)], tp=at.across)

    def back(m):
        return at.to(final.at[m], arr.at[at.sp], s_b.at[0], r_b.at[0], sp=at.mate(m))

    def produce(jj):
        base = base_of(jj)
        rows = rows_of(base)
        for c in range(t):
            cols = slice(c * d, (c + 1) * d)
            value = dot_last(gd[rows, :], gate[cols, :]) + dot_last(ud[rows, :], up[cols, :])
            part[pl.ds(2 * base, 2), :, cols] = value.astype(BF16).reshape(2, cap, d)
        for m in (2 * base, 2 * base + 1):
            for k in (0, 1):
                halves(m, k).start()

    def pass_over(jj):
        base = base_of(jj)
        whole(pair.at[0, pl.ds(2 * base, 2)], r_p.at[0, base]).wait_recv()
        for m in (2 * base, 2 * base + 1):
            summed[m] = (
                part[m, :, col(at.across)].astype(F32) + pair[0, m].astype(F32)
            ).astype(BF16)
            over(m).start()

    def total(jj):
        base = base_of(jj)
        whole(pair.at[1, pl.ds(2 * base, 2)], r_p.at[1, base]).wait_recv()
        whole(other.at[pl.ds(2 * base, 2)], r_y.at[base]).wait_recv()
        for m in (2 * base, 2 * base + 1):
            final[m] = (
                part[m, :, col(at.tp)].astype(F32) + pair[1, m].astype(F32) + other[m].astype(F32)
            ).astype(BF16)

            @pl.when(m > 0)
            def _():
                back(m).start()

    def weight_grads(c):
        cols = pl.ds(pl.multiple_of(c * d, d), d)
        inputs = got[0, :, :, cols].reshape(slots, d)
        gate_grad[0, cols, :] = dot_first(inputs, gd[...]).astype(BF16)
        up_grad[0, cols, :] = dot_first(inputs, ud[...]).astype(BF16)
        sent = got[1, :, :, cols].reshape(slots, d)
        down_grad[0, :, cols] = dot_first(hidden[...], sent).astype(BF16)

    def second(j):
        forward(n + 2 * j)
        forward(n + 2 * j + 1)
        ahead(j)

        @pl.when(j > 1)
        def _():
            behind(j - 2)
            produce(j - 2)

        @pl.when(j > 3)
        def _():
            pass_over(j - 3)

        @pl.when(j > 4)
        def _():
            total(j - 4)

    loop(0, half, second)
    loop(2 * n - lag, 2 * n, relay)
    begin_gated(False)
    pass_on(1, z == 1, z == half - 2)
    pass_over(half - 3)
    behind(half - 2)
    produce(half - 2)
    if half > 4:
        total(half - 4)
    behind(half - 1)
    produce(half - 1)
    pass_over(half - 2)
    total(half - 3)
    pass_over(half - 1)
    pass_over(0)
    weight_grads(0)
    total(half - 2)
    weight_grads(1)
    total(half - 1)
    total(0)
    pass_on(1, z != 1, z != half - 2)
    sides(1)
    for c in range(2, t):
        weight_grads(c)
    arr[at.sp] = final[0]
    whole(arr.at[pl.ds(1, n - 1)], r_b.at[0]).wait_recv()

    moe_grad = dot(pick[...], arr[...].reshape(slots, d))
    full[:, col(at.tp)] = (c_ref[...].astype(F32) + moe_grad).astype(BF16)

    def rows_to(j):
        here = full.at[:, col(at.across if j == 2 else at.tp)]
        return at.to(here, here, s_r.at[0], r_r.at[j], tp=at.across if j == 0 else at.beside)

    def through(tp):
        rows = pl.ds(pl.multiple_of(tp * d, d), d)
        return dot(full[:, col(tp)], pw[rows, :])

    rows_to(0).start()
    rows_to(1).start()
    loads[13].wait()
    out_delta = through(at.tp)

    rows_to(1).wait_recv()
    whole(trow.at[pl.ds(1, n - 1)], r_d.at[0]).wait_recv()
    twin_first(0).wait_recv()
    join(0)
    send_along(0)
    out_delta = out_delta + through(at.beside)
    rows_to(0).wait_recv()
    rows_to(2).start()
    out_delta = out_delta + through(at.across)
    rows_to(2).wait_recv()
    out_delta = (out_delta + through(at.cross)).astype(BF16).astype(F32)
    delta[...] = (out_delta * act[...]).astype(BF16)
    states(1, rl, delta)
    twin_first(1).start()
    twin_rest(1).start()
    outg[...] = (out_delta * slp[...]).astype(BF16)

    q = tokens // t
    width = gall.shape[2]
    row = lambda tp: pl.ds(pl.multiple_of(tp * q, q), q)
    quarter = full[row(at.tp), :]
    for o in range(n):
        by[o] = quarter[:, o * width : (o + 1) * width]

    def spread_g(m):
        mate = at.mate(m)
        return at.to(
            by.at[mate], gall.at[at.sp, row(at.tp), :], s_g.at[0], r_g.at[0], sp=mate
        )

    def share_g(m, j):
        here = gall.at[at.mate(m), row(at.across if j == 2 else at.tp), :]
        came_sem = r_gs.at[0 if j == 0 else 1]
        return at.to(here, here, s_gs.at[0], came_sem, tp=at.across if j == 0 else at.beside)

    gall[at.sp, row(at.tp), :] = by[at.sp]
    loop(1, n, lambda i: spread_g(i).start())
    share_g(0, 0).start()
    share_g(0, 1).start()
    loop(2, half - 1, pass_on)

    arow = exact(rates[...], (row_id <= col_id).astype(F32))
    inner = []
    scores = []
    for g in range(groups):
        wide = slice(g * STATE, (g + 1) * STATE)
        common = dot_last(wl[:, wide], rl[:, wide])
        score = jnp.zeros((tokens, tokens), F32)
        for h in range(g * per, (g + 1) * per):
            cols = slice(h * HEAD_DIM, (h + 1) * HEAD_DIM)
            fade = jnp.exp(
                -jnp.abs(acol[:, h * HEAD_DIM : h * HEAD_DIM + 1] - arow[h : h + 1, :])
            )
            inner.append(dot((fade * common).astype(BF16), delta[:, cols]))
            score += fade * dot_last(vl[:, cols], delta[:, cols])
        scores.append(score.astype(BF16))

    twin_first(1).wait_recv()
    join(1)
    send_along(1)
    gather_states(0)
    twin_last(0).start()
    pass_on(half - 1)
    loop(2, half, sides)
    whole(gall.at[pl.ds(1, n - 1), 0:q, :], r_g.at[0]).wait_recv()

    def forward_g(m):
        share_g(m, 0).start()
        share_g(m, 1).start()

    loop(1, n, forward_g)
    whole(gall.at[:, 0:q, :], r_gs.at[0]).wait_recv()
    loop(0, n, lambda m: share_g(m, 2).start())
    gather_states(1)
    twin_last(1).start()

    whole(gall.at[:, 0 : 2 * q, :], r_gs.at[1]).wait_recv()
    pair_gated().wait_recv()
    whole(ga.at[pl.ds(1, half - 1)], r_ls.at[0]).wait_recv()
    proj[...] = dot_first(
        gall[...].reshape(n * tokens, width), ga[...].reshape(n * tokens, d)
    )
    twin_rest(0).wait_recv()
    twin_last(0).wait_recv()
    to_end, to_start = fades[0], fades[1]
    w_low, w_high = reach(0)
    value = vl[...].astype(F32)
    moved = delta[...].astype(F32)
    d_start, d_end = (moved * to_start).astype(BF16), (moved * to_end).astype(BF16)
    v_start, v_end = (value * to_start).astype(BF16), (value * to_end).astype(BF16)
    for g in range(groups):
        wide = slice(g * STATE, (g + 1) * STATE)
        cols = slice(g * span, (g + 1) * span)
        rg[:, wide] = (
            dot_first(scores[g], wl[:, wide])
            + dot_last(d_start[:, cols], w_low[:, cols])
            + dot_last(d_end[:, cols], w_high[:, cols])
        ).astype(BF16)

    twin_rest(1).wait_recv()
    twin_last(1).wait_recv()
    r_low, r_high = reach(1)
    for g in range(groups):
        wide = slice(g * STATE, (g + 1) * STATE)
        cols = slice(g * span, (g + 1) * span)
        wg[:, wide] = (
            dot(scores[g], rl[:, wide])
            + dot_last(v_start[:, cols], r_low[:, cols])
            + dot_last(v_end[:, cols], r_high[:, cols])
        ).astype(BF16)
        vg[:, cols] = (
            jnp.concatenate(inner[g * per : (g + 1) * per], axis=1)
            + dot(wl[:, wide], r_low[:, cols]) * to_start[:, cols]
            + dot(wl[:, wide], r_high[:, cols]) * to_end[:, cols]
        ).astype(BF16)

    cols = hcol(bit)
    for ref, sem in (
        (got.at[:, :, :, 0 : 3 * d], s_sh),
        (snd.at[:, pl.ds(1, n - 1)], s_a2a),
        (trow.at[pl.ds(1, n - 1)], s_d),
        (pair, s_p),
        (summed, s_y),
        (final.at[pl.ds(1, n - 1)], s_b),
        (full.at[:, 0 : 3 * d], s_r),
        (ends.at[:, :, :, cols], s_t1),
        (ends.at[:, 0, :, cols], s_t2),
        (lowhigh.at[:, :, :, cols], s_t3),
        (lined.at[:, pl.ds(1, half - 1)], s_z),
        (ga.at[pl.ds(1, half - 1)], s_ls),
        (by.at[pl.ds(1, n - 1)], s_g),
        (gall.at[:, 0 : 3 * q, :], s_gs),
    ):
        whole(ref, sem.at[0]).wait_send()
    pair_gated().wait_send()

    def drain(k):
        @pl.when(jnp.logical_and(z - k >= 0, z < half - 1))
        def _():
            hop(True, k).wait_send()

        @pl.when(jnp.logical_and(z + k < half, z > 0))
        def _():
            hop(False, k).wait_send()

    loop(0, half, drain)


def put_out_kernel(*refs):
    count = len(refs) // 2
    copies = [
        pltpu.make_async_copy(refs[i], refs[count + i], refs[-1].at[i]) for i in range(count)
    ]
    for copy in copies:
        copy.start()
    for copy in copies:
        copy.wait()


def held(scratch):
    shape, size = scratch.shape, jnp.dtype(scratch.dtype).itemsize
    minor = -(-shape[-1] // 128) * 128
    rows = -(-shape[-2] // 16) * 16
    return functools.reduce(lambda a, b: a * b, shape[:-2], minor * rows * size)


def on_device(
    layer_input,
    cotangent,
    routes,
    route_weight,
    gate_weight,
    up_weight,
    down_weight,
    heads_value,
    output_gate,
    mixer_saved,
    proj_weight,
    state_write,
    state_read,
    decay_rate,
):
    n = lax.axis_size("sp")
    t = lax.axis_size("tp")
    tokens, d = layer_input.shape
    top = routes.shape[1]
    capacity = -(-max(2, 3 * tokens * top // (2 * n)) // 16) * 16
    slots = n * capacity
    hid = gate_weight.shape[2]
    half = n // 2
    width = t * d // n
    state_w = state_write.shape[1]
    sds = jax.ShapeDtypeStruct
    block = (n, capacity, d)
    vm = pl.BlockSpec(memory_space=pltpu.VMEM)
    hbm = pl.BlockSpec(memory_space=pltpu.HBM)
    one = (1,)
    sems = [
        (14,), one, (2, n), one, (2, n), (2, half), one, one, one, (2, half), one, (half,),
        one, one, one, (3,),
        one, (2,), one, (2,), one, (2,), one, (2,), (2, half), (2, half),
        one, one, one, one, one, one, one, (2,),
    ]
    outs = (
        sds((1, t * d, hid), BF16),
        sds((1, t * d, hid), BF16),
        sds((1, hid, t * d), BF16),
        sds((width, d), F32),
        sds((tokens, d), BF16),
        sds((tokens, state_w), BF16),
        sds((tokens, state_w), BF16),
        sds((tokens, d), BF16),
    )
    operands = (
        routes.T,
        route_weight.T,
        decay_rate.T,
        layer_input,
        cotangent,
        heads_value,
        output_gate,
        mixer_saved,
        state_write,
        state_read,
        gate_weight,
        up_weight,
        down_weight,
        proj_weight,
    )
    scratch = [VMEM(x.shape[-2:], x.dtype) for x in operands] + [
        VMEM((2,) + block, BF16),
        VMEM((2, n, capacity, t * d), BF16),
        VMEM((slots, hid), F32),
        VMEM((slots, hid), F32),
        VMEM((slots, hid), BF16),
        VMEM((slots, hid), BF16),
        VMEM((slots, hid), BF16),
        VMEM((n, capacity, t * d), BF16),
        VMEM((2,) + block, BF16),
        VMEM(block, BF16),
        VMEM(block, BF16),
        VMEM(block, BF16),
        VMEM(block, BF16),
        VMEM((tokens, slots), BF16),
        VMEM((n, 1, d), F32),
        VMEM((tokens, d), F32),
        VMEM((2, tokens, d), F32),
        VMEM((tokens, d), F32),
        VMEM((tokens, d), F32),
        VMEM((2, 2, STATE, d), BF16),
        VMEM((2, 2, STATE, d), BF16),
        VMEM((2, 2, STATE, d // 2), BF16),
        VMEM((2, half, STATE, d // 2), BF16),
        VMEM((2, 2, STATE, d), BF16),
        VMEM((tokens, d), BF16),
        VMEM((n, tokens, d), BF16),
        VMEM((tokens, t * d), BF16),
        VMEM((n, tokens // t, width), BF16),
        VMEM((n, tokens, width), BF16),
    ]
    grads = pl.pallas_call(
        functools.partial(layer_kernel, n, t, capacity),
        out_shape=outs,
        in_specs=[hbm] * 14,
        out_specs=(vm,) * 8,
        scratch_shapes=scratch + [DMA(shape) for shape in sems],
        compiler_params=pltpu.CompilerParams(
            collective_id=1,
            has_side_effects=True,
            vmem_limit_bytes=min(60 * MIB, sum(map(held, scratch)) + 8 * MIB),
        ),
        cost_estimate=pl.CostEstimate(
            flops=4_000_000_000, bytes_accessed=8_000_000, transcendentals=0
        ),
        name="layer",
    )(*(pltpu.with_memory_space_constraint(x, pltpu.HBM) for x in operands))
    return pl.pallas_call(
        put_out_kernel,
        out_shape=outs,
        in_specs=[vm] * len(outs),
        out_specs=(hbm,) * len(outs),
        scratch_shapes=[DMA((len(outs),))],
        compiler_params=pltpu.CompilerParams(vmem_limit_bytes=12 * MIB),
        name="put_out",
    )(*grads)


def solution(mesh):
    split = P("sp", "tp")
    in_specs = (
        split,
        split,
        P("sp", None),
        P("sp", None),
        P("sp", None, "tp"),
        P("sp", None, "tp"),
        P("sp", "tp", None),
        split,
        split,
        split,
        P(None, "tp"),
        split,
        split,
        split,
    )
    out_specs = (
        P("sp", None, "tp"),
        P("sp", None, "tp"),
        P("sp", "tp", None),
        split,
        split,
        split,
        split,
        split,
    )
    return jax.shard_map(
        on_device, mesh=mesh, in_specs=in_specs, out_specs=out_specs, check_vma=False
    )
```

```python
import functools

import jax
import jax.numpy as jnp
from jax import lax
from jax.experimental import pallas as pl
from jax.experimental.pallas import tpu as pltpu
from jax.sharding import PartitionSpec as P

HEAD_DIM = 64
STATE = 128
MESH = pl.DeviceIdType.MESH
LAST = (((1,), (1,)), ((), ()))
FIRST = (((0,), (0,)), ((), ()))
F32 = jnp.float32
BF16 = jnp.bfloat16
VMEM = pltpu.VMEM
DMA = pltpu.SemaphoreType.DMA
MIB = 1024 * 1024


def silu_parts(value):
    sigma = jax.nn.sigmoid(value)
    return (value * sigma, sigma * (1.0 + value * (1.0 - sigma)))


def dot_first(a, b):
    return lax.dot_general(a, b, FIRST, preferred_element_type=F32)


def dot_last(a, b):
    return lax.dot_general(a, b, LAST, preferred_element_type=F32)


def dot(a, b):
    return jnp.dot(a, b, preferred_element_type=F32)


def exact(a, b, dims=(((1,), (0,)), ((), ()))):
    return lax.dot_general(
        a, b, dims, precision=lax.Precision.HIGHEST, preferred_element_type=F32
    )


def flip(a, b, n):
    out, bit = 0, 1
    while bit < n:
        out = out + lax.rem(lax.div(a, bit) + lax.div(b, bit), 2) * bit
        bit *= 2
    return out


class Place:
    def __init__(self, n, t):
        self.n, self.t = n, t
        self.sp = lax.axis_index("sp")
        self.tp = lax.axis_index("tp")
        self.across = lax.rem(self.tp + t // 2, t)
        self.beside = self.tp + 1 - 2 * lax.rem(self.tp, 2)
        self.cross = lax.rem(self.beside + t // 2, t)

    def mate(self, m):
        return flip(self.sp, jnp.int32(m), self.n)

    def to(self, src, dst, send, recv, sp=None, tp=None):
        return pltpu.make_async_remote_copy(
            src_ref=src,
            dst_ref=dst,
            send_sem=send,
            recv_sem=recv,
            device_id=(self.sp if sp is None else sp, self.tp if tp is None else tp),
            device_id_type=MESH,
        )


def loop(lo, hi, body):
    def step(i, carry):
        body(i)
        return carry

    lax.fori_loop(lo, hi, step, 0)


def layer_kernel(n, t, cap, *refs):
    count = 14
    sources, refs = refs[:count], refs[count:]
    gate_grad, up_grad, down_grad, proj, vg, wg, rg, outg = refs[:8]
    held_in, refs = refs[8 : 8 + count], refs[8 + count :]
    routes, rweight, rates, x_ref, c_ref, vl, og, ms, wl, rl, gate, up, down, pw = held_in
    (
        snd, got, pg, pu, hidden, gd, ud, part, pair, summed, other, final, arr, pick, trow,
        acol, fades, act, slp, ends, twins, joint, lined, lowhigh, delta, ga, full, by, gall,
        gate_t, up_t, down_t,
    ) = refs[:32]
    (
        w_sem, s_a2a, r_a2a, s_sh, r_sh, r_side, s_d, r_d, s_p, r_p, s_y, r_y, s_b, r_b, s_r, r_r,
        s_t1, r_t1, s_t2, r_t2, s_t3, r_t3, s_z, r_z, s_l, r_l, s_ls, r_ls, s_x, r_x, s_g, r_g,
        s_gs, r_gs,
    ) = refs[32:]
    at = Place(n, t)
    tokens, d = x_ref.shape
    top = routes.shape[0]
    slots = n * cap
    half = n // 2
    duo = 2 * cap
    heads = rates.shape[0]
    per = heads * STATE // wl.shape[1]
    span = per * HEAD_DIM
    groups = heads // per
    z = lax.div(at.sp, 2)
    bit = lax.rem(at.sp, 2)
    twin = at.sp + 1 - 2 * bit
    mate_one = twin
    col = lambda tp: pl.ds(pl.multiple_of(tp * d, d), d)
    hcol = lambda b: pl.ds(pl.multiple_of(b * (d // 2), d // 2), d // 2)

    barrier = pltpu.get_barrier_semaphore()
    for tp in (at.across, at.beside):
        pl.semaphore_signal(barrier, inc=1, device_id=(at.sp, tp), device_id_type=MESH)

    def hello(o):
        pl.semaphore_signal(
            barrier, inc=1, device_id=(lax.rem(at.sp + o, n), at.tp), device_id_type=MESH
        )

    loop(1, n, hello)
    loads = [
        pltpu.make_async_copy(
            src if len(src.shape) == len(dst.shape) else src.at[0], dst, w_sem.at[i]
        )
        for i, (src, dst) in enumerate(zip(sources, held_in))
    ]
    for load in loads:
        load.start()
    for load in loads[:5]:
        load.wait()

    row_id = lax.broadcasted_iota(jnp.int32, (tokens, tokens), 0)
    col_id = lax.broadcasted_iota(jnp.int32, (tokens, tokens), 1)
    eye = (row_id == col_id).astype(F32)
    named = exact(eye, routes[...].astype(F32), LAST)
    weights = exact(eye, rweight[...], LAST)
    lanes = lax.broadcasted_iota(jnp.int32, (tokens, n), 1).astype(F32)
    onehot = [(named[:, k : k + 1] == lanes).astype(F32) for k in range(top)]
    lower = (row_id > col_id).astype(F32)
    before = dot(lower.astype(BF16), sum(onehot).astype(BF16))
    slot_lane = lax.broadcasted_iota(jnp.int32, (tokens, slots), 1).astype(F32)
    picks = []
    for k in range(top):
        rank = jnp.sum(before * onehot[k], axis=1, keepdims=True)
        picks.append((named[:, k : k + 1] * cap + rank == slot_lane).astype(F32).astype(BF16))
    pick[...] = sum(picks)
    snd[0] = dot_first(pick[...], x_ref[...]).astype(BF16).reshape(n, cap, d)
    cot = c_ref[...].astype(F32)
    weighted = [(cot * weights[:, k : k + 1]).astype(BF16) for k in range(top)]
    snd[1] = dot_first(
        jnp.concatenate(picks, axis=0), jnp.concatenate(weighted, axis=0)
    ).astype(BF16).reshape(n, cap, d)
    for k in (0, 1):
        got[k, 0, :, col(at.tp)] = snd[k, at.sp]
    pl.semaphore_wait(barrier, n + 1)

    def whole(ref, sem):
        return at.to(ref, ref, sem, sem, sp=mate_one)

    def to_columns(value):
        lane = lax.broadcasted_iota(jnp.int32, (heads, d), 1)
        lead = lax.broadcasted_iota(jnp.int32, (heads, d), 0) * HEAD_DIM
        spread_heads = jnp.logical_and(lane >= lead, lane < lead + HEAD_DIM).astype(F32)
        return exact(value, spread_heads, FIRST)

    def prepare():
        upto = (row_id >= col_id).astype(F32)
        acol[...] = exact(upto, to_columns(rates[...]))
        trow[at.sp] = acol[tokens - 1 : tokens, :]
        a = acol[...]
        fades[0] = jnp.exp(a - a[tokens - 1 : tokens, :])
        fades[1] = jnp.exp(-a)
        active_gate, slope_gate = silu_parts(og[...].astype(F32))
        saved = ms[...].astype(F32)
        ga[at.sp] = (saved * active_gate).astype(BF16)
        act[...] = active_gate
        slp[...] = saved * slope_gate

    def states(kind, left, right):
        value = right[...].astype(F32)
        for i in (0, 1):
            faded = (value * fades[i]).astype(BF16)
            for g in range(groups):
                ends[kind, i, :, g * span : (g + 1) * span] = dot_first(
                    left[:, g * STATE : (g + 1) * STATE], faded[:, g * span : (g + 1) * span]
                ).astype(BF16)

    def totals(m):
        mate = at.mate(m)
        return at.to(trow.at[at.sp], trow.at[at.sp], s_d.at[0], r_d.at[0], sp=mate)

    def twin_first(kind):
        cols = hcol(1 - bit)
        return at.to(
            ends.at[kind, :, :, cols], twins.at[kind, :, :, cols], s_t1.at[0], r_t1.at[kind],
            sp=twin,
        )

    def twin_rest(kind):
        cols = hcol(bit)
        return at.to(
            ends.at[kind, bit, :, cols], twins.at[kind, bit, :, cols], s_t2.at[0],
            r_t2.at[kind], sp=twin,
        )

    def along(kind, o):
        there = lax.rem(z + o, half)
        return at.to(
            joint.at[kind, jnp.where(there > z, 0, 1)], lined.at[kind, z], s_z.at[0],
            r_z.at[kind], sp=there * 2 + bit,
        )

    def twin_last(kind):
        here = lowhigh.at[kind, :, :, hcol(bit)]
        return at.to(here, here, s_t3.at[0], r_t3.at[kind], sp=twin)

    def join(kind):
        cols = hcol(bit)
        mine = jnp.exp(-trow[at.sp, :, cols])
        his = jnp.exp(-trow[twin, :, cols])
        second = (bit == 1).astype(F32)
        keep_end = second + (1.0 - second) * his
        his_end = (1.0 - second) + second * mine
        keep_start = (1.0 - second) + second * his
        his_start = second + (1.0 - second) * mine
        own = ends[kind, :, :, cols].astype(F32)
        got_twin = twins[kind, :, :, cols].astype(F32)
        joint[kind, 0] = (own[0] * keep_end + got_twin[0] * his_end).astype(BF16)
        joint[kind, 1] = (own[1] * keep_start + got_twin[1] * his_start).astype(BF16)

    def send_along(kind):
        loop(1, half, lambda o: along(kind, o).start())

    def gather_states(kind):
        cols = hcol(bit)
        whole(lined.at[kind, pl.ds(1, half - 1)], r_z.at[kind]).wait_recv()

        def both(y):
            return trow[2 * y, :, cols] + trow[2 * y + 1, :, cols]

        zero = jnp.zeros((STATE, d // 2), F32)

        def before_me(i, carry):
            total, fade = carry
            y = z - 1 - i
            total = total + jnp.exp(-fade) * lined[kind, y].astype(F32)
            return total, fade + both(y)

        def after_me(i, carry):
            total, fade = carry
            y = z + 1 + i
            total = total + jnp.exp(-fade) * lined[kind, y].astype(F32)
            return total, fade + both(y)

        none = jnp.zeros((1, d // 2), F32)
        low, _ = lax.fori_loop(0, z, before_me, (zero, none))
        high, _ = lax.fori_loop(0, half - 1 - z, after_me, (zero, none))
        lowhigh[kind, 0, :, cols] = low.astype(BF16)
        lowhigh[kind, 1, :, cols] = high.astype(BF16)

    def reach(kind):
        his = jnp.exp(-trow[twin])
        second = (bit == 1).astype(F32)
        extra = twins[kind, 1 - bit].astype(F32)
        low = lowhigh[kind, 0].astype(F32) * (1.0 - second + second * his) + extra * second
        high = lowhigh[kind, 1].astype(F32) * (second + (1.0 - second) * his) + extra * (
            1.0 - second
        )
        return low.astype(BF16), high.astype(BF16)

    def hop(up, k):
        here = ga.at[(z - k if up else z + k) * 2 + bit]
        i = 0 if up else 1
        peer = z + 1 if up else z - 1
        return at.to(here, here, s_l.at[i, k], r_l.at[i, k], sp=peer * 2 + bit)

    def came(up, k):
        here = ga.at[(z - k if up else z + k) * 2 + bit]
        i = 0 if up else 1
        return at.to(here, here, s_l.at[i, k], r_l.at[i, k - 1], sp=twin)

    def side(up, k):
        here = ga.at[(z - k if up else z + k) * 2 + bit]
        i = 0 if up else 1
        return at.to(here, here, s_ls.at[0], r_ls.at[0], sp=twin)

    def pair_gated():
        return at.to(ga.at[at.sp], ga.at[at.sp], s_x.at[0], r_x.at[0], sp=twin)

    outer_up = jnp.logical_or(z == 0, z == half - 2)
    outer_down = jnp.logical_or(z == half - 1, z == 1)

    def begin_gated(outer):
        @pl.when(jnp.logical_and(z < half - 1, outer_up == outer))
        def _():
            hop(True, 0).start()

        @pl.when(jnp.logical_and(z > 0, outer_down == outer))
        def _():
            hop(False, 0).start()

    def each_way(k, up_if, down_if, act):
        @pl.when(jnp.logical_and(z - k >= 0, up_if))
        def _():
            act(True)

        @pl.when(jnp.logical_and(z + k < half, down_if))
        def _():
            act(False)

    def carry(k, up_if, down_if):
        each_way(k, jnp.logical_and(up_if, z < half - 1), jnp.logical_and(down_if, z > 0),
                 lambda up: hop(up, k).start())

    def sides(k, up_if, down_if):
        def act(up):
            came(up, k).wait_recv()
            side(up, k).start()

        each_way(k, up_if, down_if, act)

    def spread(k, m):
        mate = at.mate(m)
        return at.to(
            snd.at[k, mate], got.at[k, m, :, col(at.tp)], s_a2a.at[0], r_a2a.at[k, m], sp=mate
        )

    def share(k, m, j):
        here = got.at[k, m, :, col(at.across if j == 2 else at.tp)]
        came_sem = r_sh.at[k, m] if j == 0 else r_side.at[k, lax.div(m, 2)]
        return at.to(here, here, s_sh.at[0], came_sem, tp=at.across if j == 0 else at.beside)

    loop(1, n, lambda i: spread(0, i).start())
    for k in (0, 1):
        share(k, jnp.int32(0), 0).start()
        share(k, jnp.int32(0), 1).start()
    for load in loads[5:10]:
        load.wait()
    prepare()
    states(0, wl, vl)
    loop(1, n, lambda m: totals(m).start())
    begin_gated(True)

    lag = 2

    def forward(q):
        k, i = lax.div(q, n), lax.rem(q, n)
        m = i

        @pl.when(i > 0)
        def _():
            spread(k, m).wait_recv()
            share(k, m, 0).start()
            share(k, m, 1).start()

        @pl.when(jnp.logical_and(k == 0, i > 0))
        def _():
            spread(1, i).start()

        @pl.when(q >= lag)
        def _():
            relay(q - lag)

    def relay(q):
        k, m = lax.div(q, n), lax.rem(q, n)
        share(k, jnp.int32(m), 0).wait_recv()
        share(k, m, 2).start()

    def settled(k, base):
        whole(got.at[k, pl.ds(2 * base, 2), :, 0 : 2 * d], r_side.at[k, base]).wait_recv()

    def base_of(j):
        return jnp.int32(j)

    def rows_of(base):
        return pl.ds(pl.multiple_of(base * duo, duo), duo)

    def ahead(j):
        base = base_of(j)
        settled(0, base)
        rows = rows_of(base)
        inputs = got[0, pl.ds(2 * base, 2)].reshape(duo, t * d)
        pg[rows, :] = dot(inputs, gate[...])
        pu[rows, :] = dot(inputs, up[...])

    def behind(j):
        base = base_of(j)
        settled(1, base)
        rows = rows_of(base)
        sent = got[1, pl.ds(2 * base, 2)].reshape(duo, t * d)
        grad = dot(sent, down_t[...])
        active, slope = silu_parts(pg[rows, :])
        ups = pu[rows, :]
        hidden[rows, :] = (active * ups).astype(BF16)
        gd[rows, :] = (grad * ups * slope).astype(BF16)
        ud[rows, :] = (grad * active).astype(BF16)

    for load in loads[10:13]:
        load.wait()

    def turn(c):
        cols = pl.ds(pl.multiple_of(c * d, d), d)
        gate_t[:, cols] = gate[cols, :].T
        up_t[:, cols] = up[cols, :].T
        down_t[cols, :] = down[:, cols].T

    share_of = n // t

    def first(i):
        forward(i)

        @pl.when(lax.rem(i, share_of) == share_of - 1)
        def _():
            turn(lax.div(i, share_of))

    loop(1, n, first)

    def halves(m, k):
        c = at.cross if k == 0 else at.beside
        return at.to(
            part.at[m, :, col(c)], pair.at[k, m], s_p.at[0], r_p.at[k, lax.div(m, 2)], tp=at.beside
        )

    def over(m):
        return at.to(summed.at[m], other.at[m], s_y.at[0], r_y.at[lax.div(m, 2)], tp=at.across)

    def back(m):
        return at.to(final.at[m], arr.at[at.sp], s_b.at[0], r_b.at[0], sp=at.mate(m))

    def produce(jj):
        base = base_of(jj)
        rows = rows_of(base)
        for c in range(t):
            cols = slice(c * d, (c + 1) * d)
            value = dot(gd[rows, :], gate_t[:, cols]) + dot(ud[rows, :], up_t[:, cols])
            part[pl.ds(2 * base, 2), :, cols] = value.astype(BF16).reshape(2, cap, d)
        for m in (2 * base, 2 * base + 1):
            for k in (0, 1):
                halves(m, k).start()

    def pass_over(jj):
        base = base_of(jj)
        whole(pair.at[0, pl.ds(2 * base, 2)], r_p.at[0, base]).wait_recv()
        for m in (2 * base, 2 * base + 1):
            summed[m] = (
                part[m, :, col(at.across)].astype(F32) + pair[0, m].astype(F32)
            ).astype(BF16)
            over(m).start()

    def total(jj):
        base = base_of(jj)
        whole(pair.at[1, pl.ds(2 * base, 2)], r_p.at[1, base]).wait_recv()
        whole(other.at[pl.ds(2 * base, 2)], r_y.at[base]).wait_recv()
        for m in (2 * base, 2 * base + 1):
            final[m] = (
                part[m, :, col(at.tp)].astype(F32) + pair[1, m].astype(F32) + other[m].astype(F32)
            ).astype(BF16)

            @pl.when(m > 0)
            def _():
                back(m).start()

    def weight_grads(c):
        cols = pl.ds(pl.multiple_of(c * d, d), d)
        inputs = got[0, :, :, cols].reshape(slots, d)
        gate_grad[0, cols, :] = dot_first(inputs, gd[...]).astype(BF16)
        up_grad[0, cols, :] = dot_first(inputs, ud[...]).astype(BF16)
        sent = got[1, :, :, cols].reshape(slots, d)
        down_grad[0, :, cols] = dot_first(hidden[...], sent).astype(BF16)

    def second(j):
        @pl.when(j > 1)
        def _():
            behind(j - 2)
            produce(j - 2)

        @pl.when(j > 2)
        def _():
            pass_over(j - 3)

        @pl.when(j > 4)
        def _():
            total(j - 5)

        forward(n + 2 * j)
        forward(n + 2 * j + 1)
        ahead(j)

    loop(0, half, second)
    begin_gated(False)
    pair_gated().start()
    twin_first(0).start()
    twin_rest(0).start()
    pass_over(half - 3)
    behind(half - 2)
    produce(half - 2)
    soon_up = jnp.logical_or(z == 1, z == half - 1)
    soon_down = jnp.logical_or(z == half - 2, z == 0)
    sides(1, soon_up, soon_down)
    if half > 4:
        total(half - 5)
    loop(2 * n - lag, 2 * n, relay)
    carry(1, soon_up, soon_down)
    pass_over(half - 2)
    total(half - 4)
    behind(half - 1)
    produce(half - 1)
    total(half - 3)
    pass_over(half - 1)
    late_up, late_down = jnp.logical_not(soon_up), jnp.logical_not(soon_down)
    sides(1, late_up, late_down)
    carry(1, late_up, late_down)
    weight_grads(0)
    weight_grads(1)
    front_up = jnp.logical_and(z == 2, z < half - 1)
    front_down = jnp.logical_and(z == half - 3, z > 0)
    sides(2, front_up, front_down)
    carry(2, front_up, front_down)
    total(half - 2)
    weight_grads(2)
    total(half - 1)
    for c in range(3, t):
        weight_grads(c)
    arr[at.sp] = final[0]
    whole(arr.at[pl.ds(1, n - 1)], r_b.at[0]).wait_recv()

    moe_grad = dot(pick[...], arr[...].reshape(slots, d))
    full[:, col(at.tp)] = (c_ref[...].astype(F32) + moe_grad).astype(BF16)

    def rows_to(j):
        here = full.at[:, col(at.across if j == 2 else at.tp)]
        return at.to(here, here, s_r.at[0], r_r.at[j], tp=at.across if j == 0 else at.beside)

    def through(tp):
        rows = pl.ds(pl.multiple_of(tp * d, d), d)
        return dot(full[:, col(tp)], pw[rows, :])

    rows_to(0).start()
    rows_to(1).start()
    loads[13].wait()
    out_delta = through(at.tp)

    rows_to(1).wait_recv()
    whole(trow.at[pl.ds(1, n - 1)], r_d.at[0]).wait_recv()
    twin_first(0).wait_recv()
    join(0)
    send_along(0)
    rest_up, rest_down = jnp.logical_not(front_up), jnp.logical_not(front_down)
    sides(2, rest_up, rest_down)
    carry(2, rest_up, rest_down)

    def side_and_carry(k):
        sides(k, True, True)
        carry(k, True, True)

    loop(3, half, side_and_carry)
    out_delta = out_delta + through(at.beside)
    rows_to(0).wait_recv()
    rows_to(2).start()
    out_delta = out_delta + through(at.across)
    rows_to(2).wait_recv()
    out_delta = (out_delta + through(at.cross)).astype(BF16).astype(F32)
    delta[...] = (out_delta * act[...]).astype(BF16)
    states(1, rl, delta)
    twin_first(1).start()
    outg[...] = (out_delta * slp[...]).astype(BF16)

    q = tokens // t
    width = gall.shape[2]
    row = lambda tp: pl.ds(pl.multiple_of(tp * q, q), q)
    quarter = full[row(at.tp), :]
    for o in range(n):
        by[o] = quarter[:, o * width : (o + 1) * width]

    def spread_g(m):
        mate = at.mate(m)
        return at.to(
            by.at[mate], gall.at[at.sp, row(at.tp), :], s_g.at[0], r_g.at[0], sp=mate
        )

    def share_g(m, j):
        here = gall.at[at.mate(m), row(at.across if j == 2 else at.tp), :]
        came_sem = r_gs.at[0 if j == 0 else 1]
        return at.to(here, here, s_gs.at[0], came_sem, tp=at.across if j == 0 else at.beside)

    gall[at.sp, row(at.tp), :] = by[at.sp]
    loop(1, n, lambda i: spread_g(i).start())
    share_g(0, 0).start()
    share_g(0, 1).start()

    arow = exact(rates[...], (row_id <= col_id).astype(F32))
    inner = []
    scores = []
    for g in range(groups):
        wide = slice(g * STATE, (g + 1) * STATE)
        common = dot_last(wl[:, wide], rl[:, wide])
        score = jnp.zeros((tokens, tokens), F32)
        for h in range(g * per, (g + 1) * per):
            cols = slice(h * HEAD_DIM, (h + 1) * HEAD_DIM)
            fade = jnp.exp(
                -jnp.abs(acol[:, h * HEAD_DIM : h * HEAD_DIM + 1] - arow[h : h + 1, :])
            )
            inner.append(dot((fade * common).astype(BF16), delta[:, cols]))
            score += fade * dot_last(vl[:, cols], delta[:, cols])
        scores.append(score.astype(BF16))

    twin_first(1).wait_recv()
    join(1)
    send_along(1)
    twin_rest(1).start()
    gather_states(0)
    twin_last(0).start()
    whole(gall.at[pl.ds(1, n - 1), 0:q, :], r_g.at[0]).wait_recv()

    def forward_g(m):
        share_g(m, 0).start()
        share_g(m, 1).start()

    loop(1, n, forward_g)
    gather_states(1)
    twin_last(1).start()
    whole(gall.at[:, 0:q, :], r_gs.at[0]).wait_recv()
    loop(0, n, lambda m: share_g(m, 2).start())
    whole(gall.at[:, 0 : 2 * q, :], r_gs.at[1]).wait_recv()
    pair_gated().wait_recv()
    whole(ga.at[pl.ds(1, half - 1)], r_ls.at[0]).wait_recv()
    proj[...] = dot_first(
        gall[...].reshape(n * tokens, width), ga[...].reshape(n * tokens, d)
    )
    twin_rest(0).wait_recv()
    twin_last(0).wait_recv()
    to_end, to_start = fades[0], fades[1]
    w_low, w_high = reach(0)
    value = vl[...].astype(F32)
    moved = delta[...].astype(F32)
    d_start, d_end = (moved * to_start).astype(BF16), (moved * to_end).astype(BF16)
    v_start, v_end = (value * to_start).astype(BF16), (value * to_end).astype(BF16)
    for g in range(groups):
        wide = slice(g * STATE, (g + 1) * STATE)
        cols = slice(g * span, (g + 1) * span)
        rg[:, wide] = (
            dot_first(scores[g], wl[:, wide])
            + dot_last(d_start[:, cols], w_low[:, cols])
            + dot_last(d_end[:, cols], w_high[:, cols])
        ).astype(BF16)

    twin_rest(1).wait_recv()
    twin_last(1).wait_recv()
    r_low, r_high = reach(1)
    for g in range(groups):
        wide = slice(g * STATE, (g + 1) * STATE)
        cols = slice(g * span, (g + 1) * span)
        wg[:, wide] = (
            dot(scores[g], rl[:, wide])
            + dot_last(v_start[:, cols], r_low[:, cols])
            + dot_last(v_end[:, cols], r_high[:, cols])
        ).astype(BF16)
        vg[:, cols] = (
            jnp.concatenate(inner[g * per : (g + 1) * per], axis=1)
            + dot(wl[:, wide], r_low[:, cols]) * to_start[:, cols]
            + dot(wl[:, wide], r_high[:, cols]) * to_end[:, cols]
        ).astype(BF16)

    cols = hcol(bit)
    for ref, sem in (
        (got.at[:, :, :, 0 : 3 * d], s_sh),
        (snd.at[:, pl.ds(1, n - 1)], s_a2a),
        (trow.at[pl.ds(1, n - 1)], s_d),
        (pair, s_p),
        (summed, s_y),
        (final.at[pl.ds(1, n - 1)], s_b),
        (full.at[:, 0 : 3 * d], s_r),
        (ends.at[:, :, :, cols], s_t1),
        (ends.at[:, 0, :, cols], s_t2),
        (lowhigh.at[:, :, :, cols], s_t3),
        (lined.at[:, pl.ds(1, half - 1)], s_z),
        (ga.at[pl.ds(1, half - 1)], s_ls),
        (by.at[pl.ds(1, n - 1)], s_g),
        (gall.at[:, 0 : 3 * q, :], s_gs),
    ):
        whole(ref, sem.at[0]).wait_send()
    pair_gated().wait_send()

    def drain(k):
        @pl.when(jnp.logical_and(z - k >= 0, z < half - 1))
        def _():
            hop(True, k).wait_send()

        @pl.when(jnp.logical_and(z + k < half, z > 0))
        def _():
            hop(False, k).wait_send()

    loop(0, half, drain)


def put_out_kernel(*refs):
    count = len(refs) // 2
    copies = [
        pltpu.make_async_copy(refs[i], refs[count + i], refs[-1].at[i]) for i in range(count)
    ]
    for copy in copies:
        copy.start()
    for copy in copies:
        copy.wait()


def held(scratch):
    shape, size = scratch.shape, jnp.dtype(scratch.dtype).itemsize
    minor = -(-shape[-1] // 128) * 128
    rows = -(-shape[-2] // 16) * 16
    return functools.reduce(lambda a, b: a * b, shape[:-2], minor * rows * size)


def on_device(
    layer_input,
    cotangent,
    routes,
    route_weight,
    gate_weight,
    up_weight,
    down_weight,
    heads_value,
    output_gate,
    mixer_saved,
    proj_weight,
    state_write,
    state_read,
    decay_rate,
):
    n = lax.axis_size("sp")
    t = lax.axis_size("tp")
    tokens, d = layer_input.shape
    top = routes.shape[1]
    capacity = -(-max(2, 3 * tokens * top // (2 * n)) // 16) * 16
    slots = n * capacity
    hid = gate_weight.shape[2]
    half = n // 2
    width = t * d // n
    state_w = state_write.shape[1]
    sds = jax.ShapeDtypeStruct
    block = (n, capacity, d)
    vm = pl.BlockSpec(memory_space=pltpu.VMEM)
    hbm = pl.BlockSpec(memory_space=pltpu.HBM)
    one = (1,)
    sems = [
        (14,), one, (2, n), one, (2, n), (2, half), one, one, one, (2, half), one, (half,),
        one, one, one, (3,),
        one, (2,), one, (2,), one, (2,), one, (2,), (2, half), (2, half),
        one, one, one, one, one, one, one, (2,),
    ]
    outs = (
        sds((1, t * d, hid), BF16),
        sds((1, t * d, hid), BF16),
        sds((1, hid, t * d), BF16),
        sds((width, d), F32),
        sds((tokens, d), BF16),
        sds((tokens, state_w), BF16),
        sds((tokens, state_w), BF16),
        sds((tokens, d), BF16),
    )
    operands = (
        routes.T,
        route_weight.T,
        decay_rate.T,
        layer_input,
        cotangent,
        heads_value,
        output_gate,
        mixer_saved,
        state_write,
        state_read,
        gate_weight,
        up_weight,
        down_weight,
        proj_weight,
    )
    scratch = [VMEM(x.shape[-2:], x.dtype) for x in operands] + [
        VMEM((2,) + block, BF16),
        VMEM((2, n, capacity, t * d), BF16),
        VMEM((slots, hid), F32),
        VMEM((slots, hid), F32),
        VMEM((slots, hid), BF16),
        VMEM((slots, hid), BF16),
        VMEM((slots, hid), BF16),
        VMEM((n, capacity, t * d), BF16),
        VMEM((2,) + block, BF16),
        VMEM(block, BF16),
        VMEM(block, BF16),
        VMEM(block, BF16),
        VMEM(block, BF16),
        VMEM((tokens, slots), BF16),
        VMEM((n, 1, d), F32),
        VMEM((tokens, d), F32),
        VMEM((2, tokens, d), F32),
        VMEM((tokens, d), F32),
        VMEM((tokens, d), F32),
        VMEM((2, 2, STATE, d), BF16),
        VMEM((2, 2, STATE, d), BF16),
        VMEM((2, 2, STATE, d // 2), BF16),
        VMEM((2, half, STATE, d // 2), BF16),
        VMEM((2, 2, STATE, d), BF16),
        VMEM((tokens, d), BF16),
        VMEM((n, tokens, d), BF16),
        VMEM((tokens, t * d), BF16),
        VMEM((n, tokens // t, width), BF16),
        VMEM((n, tokens, width), BF16),
        VMEM((hid, t * d), BF16),
        VMEM((hid, t * d), BF16),
        VMEM((t * d, hid), BF16),
    ]
    grads = pl.pallas_call(
        functools.partial(layer_kernel, n, t, capacity),
        out_shape=outs,
        in_specs=[hbm] * 14,
        out_specs=(vm,) * 8,
        scratch_shapes=scratch + [DMA(shape) for shape in sems],
        compiler_params=pltpu.CompilerParams(
            collective_id=1,
            has_side_effects=True,
            vmem_limit_bytes=min(60 * MIB, sum(map(held, scratch)) + 8 * MIB),
        ),
        cost_estimate=pl.CostEstimate(
            flops=4_000_000_000, bytes_accessed=8_000_000, transcendentals=0
        ),
        name="layer",
    )(*(pltpu.with_memory_space_constraint(x, pltpu.HBM) for x in operands))
    return pl.pallas_call(
        put_out_kernel,
        out_shape=outs,
        in_specs=[vm] * len(outs),
        out_specs=(hbm,) * len(outs),
        scratch_shapes=[DMA((len(outs),))],
        compiler_params=pltpu.CompilerParams(vmem_limit_bytes=12 * MIB),
        name="put_out",
    )(*grads)


def solution(mesh):
    split = P("sp", "tp")
    in_specs = (
        split,
        split,
        P("sp", None),
        P("sp", None),
        P("sp", None, "tp"),
        P("sp", None, "tp"),
        P("sp", "tp", None),
        split,
        split,
        split,
        P(None, "tp"),
        split,
        split,
        split,
    )
    out_specs = (
        P("sp", None, "tp"),
        P("sp", None, "tp"),
        P("sp", "tp", None),
        split,
        split,
        split,
        split,
        split,
    )
    return jax.shard_map(
        on_device, mesh=mesh, in_specs=in_specs, out_specs=out_specs, check_vma=False
    )
```

```python
import functools

import jax
import jax.numpy as jnp
from jax import lax
from jax.experimental import pallas as pl
from jax.experimental.pallas import tpu as pltpu
from jax.sharding import PartitionSpec as P

HEAD_DIM = 64
STATE = 128
MESH = pl.DeviceIdType.MESH
LAST = (((1,), (1,)), ((), ()))
FIRST = (((0,), (0,)), ((), ()))
F32 = jnp.float32
BF16 = jnp.bfloat16
VMEM = pltpu.VMEM
DMA = pltpu.SemaphoreType.DMA
MIB = 1024 * 1024


def silu_parts(value):
    sigma = jax.nn.sigmoid(value)
    return (value * sigma, sigma * (1.0 + value * (1.0 - sigma)))


def dot_first(a, b):
    return lax.dot_general(a, b, FIRST, preferred_element_type=F32)


def dot_last(a, b):
    return lax.dot_general(a, b, LAST, preferred_element_type=F32)


def dot(a, b):
    return jnp.dot(a, b, preferred_element_type=F32)


def exact(a, b, dims=(((1,), (0,)), ((), ()))):
    return lax.dot_general(
        a, b, dims, precision=lax.Precision.HIGHEST, preferred_element_type=F32
    )


def flip(a, b, n):
    out, bit = 0, 1
    while bit < n:
        out = out + lax.rem(lax.div(a, bit) + lax.div(b, bit), 2) * bit
        bit *= 2
    return out


class Place:
    def __init__(self, n, t):
        self.n, self.t = n, t
        self.sp = lax.axis_index("sp")
        self.tp = lax.axis_index("tp")
        self.across = lax.rem(self.tp + t // 2, t)
        self.beside = self.tp + 1 - 2 * lax.rem(self.tp, 2)
        self.cross = lax.rem(self.beside + t // 2, t)

    def mate(self, m):
        return flip(self.sp, jnp.int32(m), self.n)

    def to(self, src, dst, send, recv, sp=None, tp=None):
        return pltpu.make_async_remote_copy(
            src_ref=src,
            dst_ref=dst,
            send_sem=send,
            recv_sem=recv,
            device_id=(self.sp if sp is None else sp, self.tp if tp is None else tp),
            device_id_type=MESH,
        )


def loop(lo, hi, body):
    def step(i, carry):
        body(i)
        return carry

    lax.fori_loop(lo, hi, step, 0)


def layer_kernel(n, t, cap, *refs):
    count = 14
    sources, refs = refs[:count], refs[count:]
    gate_grad, up_grad, down_grad, proj, vg, wg, rg, outg = refs[:8]
    held_in, refs = refs[8 : 8 + count], refs[8 + count :]
    routes, rweight, rates, x_ref, c_ref, vl, og, ms, wl, rl, gate, up, down, pw = held_in
    (
        snd, got, pg, pu, hidden, gd, ud, part, pair, summed, other, final, arr, pick, trow,
        acol, fades, act, slp, ends, twins, joint, lined, lowhigh, delta, ga, full, by, gall,
        gate_t, up_t, down_t,
    ) = refs[:32]
    (
        w_sem, s_a2a, r_a2a, s_sh, r_sh, r_side, s_d, r_d, s_p, r_p, s_y, r_y, s_b, r_b, s_r, r_r,
        s_t1, r_t1, s_t2, r_t2, s_t3, r_t3, s_z, r_z, s_l, r_l, s_ls, r_ls, s_x, r_x, s_g, r_g,
        s_gs, r_gs,
    ) = refs[32:]
    at = Place(n, t)
    tokens, d = x_ref.shape
    top = routes.shape[0]
    slots = n * cap
    half = n // 2
    duo = 2 * cap
    heads = rates.shape[0]
    per = heads * STATE // wl.shape[1]
    span = per * HEAD_DIM
    groups = heads // per
    z = lax.div(at.sp, 2)
    bit = lax.rem(at.sp, 2)
    twin = at.sp + 1 - 2 * bit
    mate_one = twin
    col = lambda tp: pl.ds(pl.multiple_of(tp * d, d), d)
    hcol = lambda b: pl.ds(pl.multiple_of(b * (d // 2), d // 2), d // 2)

    barrier = pltpu.get_barrier_semaphore()
    for tp in (at.across, at.beside):
        pl.semaphore_signal(barrier, inc=1, device_id=(at.sp, tp), device_id_type=MESH)

    def hello(o):
        pl.semaphore_signal(
            barrier, inc=1, device_id=(lax.rem(at.sp + o, n), at.tp), device_id_type=MESH
        )

    loop(1, n, hello)
    loads = [
        pltpu.make_async_copy(
            src if len(src.shape) == len(dst.shape) else src.at[0], dst, w_sem.at[i]
        )
        for i, (src, dst) in enumerate(zip(sources, held_in))
    ]
    for load in loads:
        load.start()
    for load in loads[:3]:
        load.wait()

    row_id = lax.broadcasted_iota(jnp.int32, (tokens, tokens), 0)
    col_id = lax.broadcasted_iota(jnp.int32, (tokens, tokens), 1)
    eye = (row_id == col_id).astype(F32)
    named = exact(eye, routes[...].astype(F32), LAST)
    weights = exact(eye, rweight[...], LAST)
    lanes = lax.broadcasted_iota(jnp.int32, (tokens, n), 1).astype(F32)
    onehot = [(named[:, k : k + 1] == lanes).astype(F32) for k in range(top)]
    lower = (row_id > col_id).astype(F32)
    before = dot(lower.astype(BF16), sum(onehot).astype(BF16))
    slot_lane = lax.broadcasted_iota(jnp.int32, (tokens, slots), 1).astype(F32)
    picks = []
    for k in range(top):
        rank = jnp.sum(before * onehot[k], axis=1, keepdims=True)
        picks.append((named[:, k : k + 1] * cap + rank == slot_lane).astype(F32).astype(BF16))
    pick[...] = sum(picks)
    for load in loads[3:5]:
        load.wait()
    snd[0] = dot_first(pick[...], x_ref[...]).astype(BF16).reshape(n, cap, d)
    got[0, 0, :, col(at.tp)] = snd[0, at.sp]
    pl.semaphore_wait(barrier, n + 1)

    def whole(ref, sem):
        return at.to(ref, ref, sem, sem, sp=mate_one)

    def to_columns(value):
        lane = lax.broadcasted_iota(jnp.int32, (heads, d), 1)
        lead = lax.broadcasted_iota(jnp.int32, (heads, d), 0) * HEAD_DIM
        spread_heads = jnp.logical_and(lane >= lead, lane < lead + HEAD_DIM).astype(F32)
        return exact(value, spread_heads, FIRST)

    def prepare():
        upto = (row_id >= col_id).astype(F32)
        acol[...] = exact(upto, to_columns(rates[...]))
        trow[at.sp] = acol[tokens - 1 : tokens, :]
        a = acol[...]
        fades[0] = jnp.exp(a - a[tokens - 1 : tokens, :])
        fades[1] = jnp.exp(-a)
        active_gate, slope_gate = silu_parts(og[...].astype(F32))
        saved = ms[...].astype(F32)
        ga[at.sp] = (saved * active_gate).astype(BF16)
        act[...] = active_gate
        slp[...] = saved * slope_gate

    def states(kind, left, right):
        value = right[...].astype(F32)
        for i in (0, 1):
            faded = (value * fades[i]).astype(BF16)
            for g in range(groups):
                ends[kind, i, :, g * span : (g + 1) * span] = dot_first(
                    left[:, g * STATE : (g + 1) * STATE], faded[:, g * span : (g + 1) * span]
                ).astype(BF16)

    def totals(m):
        mate = at.mate(m)
        return at.to(trow.at[at.sp], trow.at[at.sp], s_d.at[0], r_d.at[0], sp=mate)

    def twin_first(kind):
        cols = hcol(1 - bit)
        return at.to(
            ends.at[kind, :, :, cols], twins.at[kind, :, :, cols], s_t1.at[0], r_t1.at[kind],
            sp=twin,
        )

    def twin_rest(kind):
        cols = hcol(bit)
        return at.to(
            ends.at[kind, bit, :, cols], twins.at[kind, bit, :, cols], s_t2.at[0],
            r_t2.at[kind], sp=twin,
        )

    def along(kind, o):
        there = lax.rem(z + o, half)
        return at.to(
            joint.at[kind, jnp.where(there > z, 0, 1)], lined.at[kind, z], s_z.at[0],
            r_z.at[kind], sp=there * 2 + bit,
        )

    def twin_last(kind):
        here = lowhigh.at[kind, :, :, hcol(bit)]
        return at.to(here, here, s_t3.at[0], r_t3.at[kind], sp=twin)

    def join(kind):
        cols = hcol(bit)
        mine = jnp.exp(-trow[at.sp, :, cols])
        his = jnp.exp(-trow[twin, :, cols])
        second = (bit == 1).astype(F32)
        keep_end = second + (1.0 - second) * his
        his_end = (1.0 - second) + second * mine
        keep_start = (1.0 - second) + second * his
        his_start = second + (1.0 - second) * mine
        own = ends[kind, :, :, cols].astype(F32)
        got_twin = twins[kind, :, :, cols].astype(F32)
        joint[kind, 0] = (own[0] * keep_end + got_twin[0] * his_end).astype(BF16)
        joint[kind, 1] = (own[1] * keep_start + got_twin[1] * his_start).astype(BF16)

    def send_along(kind):
        loop(1, half, lambda o: along(kind, o).start())

    def gather_states(kind):
        cols = hcol(bit)
        whole(lined.at[kind, pl.ds(1, half - 1)], r_z.at[kind]).wait_recv()

        def both(y):
            return trow[2 * y, :, cols] + trow[2 * y + 1, :, cols]

        zero = jnp.zeros((STATE, d // 2), F32)

        def before_me(i, carry):
            total, fade = carry
            y = z - 1 - i
            total = total + jnp.exp(-fade) * lined[kind, y].astype(F32)
            return total, fade + both(y)

        def after_me(i, carry):
            total, fade = carry
            y = z + 1 + i
            total = total + jnp.exp(-fade) * lined[kind, y].astype(F32)
            return total, fade + both(y)

        none = jnp.zeros((1, d // 2), F32)
        low, _ = lax.fori_loop(0, z, before_me, (zero, none))
        high, _ = lax.fori_loop(0, half - 1 - z, after_me, (zero, none))
        lowhigh[kind, 0, :, cols] = low.astype(BF16)
        lowhigh[kind, 1, :, cols] = high.astype(BF16)

    def reach(kind):
        his = jnp.exp(-trow[twin])
        second = (bit == 1).astype(F32)
        extra = twins[kind, 1 - bit].astype(F32)
        low = lowhigh[kind, 0].astype(F32) * (1.0 - second + second * his) + extra * second
        high = lowhigh[kind, 1].astype(F32) * (second + (1.0 - second) * his) + extra * (
            1.0 - second
        )
        return low.astype(BF16), high.astype(BF16)

    def hop(up, k):
        here = ga.at[(z - k if up else z + k) * 2 + bit]
        i = 0 if up else 1
        peer = z + 1 if up else z - 1
        return at.to(here, here, s_l.at[i, k], r_l.at[i, k], sp=peer * 2 + bit)

    def came(up, k):
        here = ga.at[(z - k if up else z + k) * 2 + bit]
        i = 0 if up else 1
        return at.to(here, here, s_l.at[i, k], r_l.at[i, k - 1], sp=twin)

    def side(up, k):
        here = ga.at[(z - k if up else z + k) * 2 + bit]
        i = 0 if up else 1
        return at.to(here, here, s_ls.at[0], r_ls.at[0], sp=twin)

    def pair_gated():
        return at.to(ga.at[at.sp], ga.at[at.sp], s_x.at[0], r_x.at[0], sp=twin)

    outer_up = jnp.logical_or(z == 0, z == half - 2)
    outer_down = jnp.logical_or(z == half - 1, z == 1)

    def begin_gated(outer):
        @pl.when(jnp.logical_and(z < half - 1, outer_up == outer))
        def _():
            hop(True, 0).start()

        @pl.when(jnp.logical_and(z > 0, outer_down == outer))
        def _():
            hop(False, 0).start()

    def each_way(k, up_if, down_if, act):
        @pl.when(jnp.logical_and(z - k >= 0, up_if))
        def _():
            act(True)

        @pl.when(jnp.logical_and(z + k < half, down_if))
        def _():
            act(False)

    def carry(k, up_if, down_if):
        each_way(k, jnp.logical_and(up_if, z < half - 1), jnp.logical_and(down_if, z > 0),
                 lambda up: hop(up, k).start())

    def sides(k, up_if, down_if):
        def act(up):
            came(up, k).wait_recv()
            side(up, k).start()

        each_way(k, up_if, down_if, act)

    def spread(k, m):
        mate = at.mate(m)
        return at.to(
            snd.at[k, mate], got.at[k, m, :, col(at.tp)], s_a2a.at[0], r_a2a.at[k, m], sp=mate
        )

    def share(k, m, j):
        here = got.at[k, m, :, col(at.across if j == 2 else at.tp)]
        came_sem = r_sh.at[k, m] if j == 0 else r_side.at[k, lax.div(m, 2)]
        return at.to(here, here, s_sh.at[0], came_sem, tp=at.across if j == 0 else at.beside)

    loop(1, n, lambda i: spread(0, i).start())
    own = jnp.int32(0)
    share(0, own, 0).start()
    share(0, own, 1).start()
    cot = c_ref[...].astype(F32)
    weighted = [(cot * weights[:, k : k + 1]).astype(BF16) for k in range(top)]
    snd[1] = dot_first(
        jnp.concatenate(picks, axis=0), jnp.concatenate(weighted, axis=0)
    ).astype(BF16).reshape(n, cap, d)
    got[1, 0, :, col(at.tp)] = snd[1, at.sp]
    for load in loads[5:10]:
        load.wait()
    prepare()
    states(0, wl, vl)
    loop(1, n, lambda m: totals(m).start())
    begin_gated(True)
    share(1, own, 0).start()
    share(1, own, 1).start()

    lag = 2

    def forward(q):
        k, i = lax.div(q, n), lax.rem(q, n)
        m = i

        @pl.when(i > 0)
        def _():
            spread(k, m).wait_recv()
            share(k, m, 0).start()
            share(k, m, 1).start()

        @pl.when(jnp.logical_and(k == 0, i > 0))
        def _():
            spread(1, i).start()

        @pl.when(q >= lag)
        def _():
            relay(q - lag)

    def relay(q):
        k, m = lax.div(q, n), lax.rem(q, n)
        share(k, jnp.int32(m), 0).wait_recv()
        share(k, m, 2).start()

    def settled(k, base):
        whole(got.at[k, pl.ds(2 * base, 2), :, 0 : 2 * d], r_side.at[k, base]).wait_recv()

    def base_of(j):
        return jnp.int32(j)

    def rows_of(base):
        return pl.ds(pl.multiple_of(base * duo, duo), duo)

    def ahead(j):
        base = base_of(j)
        settled(0, base)
        rows = rows_of(base)
        inputs = got[0, pl.ds(2 * base, 2)].reshape(duo, t * d)
        pg[rows, :] = dot(inputs, gate[...])
        pu[rows, :] = dot(inputs, up[...])

    def behind(j):
        base = base_of(j)
        settled(1, base)
        rows = rows_of(base)
        sent = got[1, pl.ds(2 * base, 2)].reshape(duo, t * d)
        grad = dot(sent, down_t[...])
        active, slope = silu_parts(pg[rows, :])
        ups = pu[rows, :]
        hidden[rows, :] = (active * ups).astype(BF16)
        gd[rows, :] = (grad * ups * slope).astype(BF16)
        ud[rows, :] = (grad * active).astype(BF16)

    for load in loads[10:13]:
        load.wait()

    def turn(c):
        cols = pl.ds(pl.multiple_of(c * d, d), d)
        gate_t[:, cols] = gate[cols, :].T
        up_t[:, cols] = up[cols, :].T
        down_t[cols, :] = down[:, cols].T

    share_of = n // t

    def first(i):
        forward(i)

        @pl.when(lax.rem(i, share_of) == share_of - 1)
        def _():
            turn(lax.div(i, share_of))

    loop(1, n, first)

    def halves(m, k):
        c = at.cross if k == 0 else at.beside
        return at.to(
            part.at[m, :, col(c)], pair.at[k, m], s_p.at[0], r_p.at[k, lax.div(m, 2)], tp=at.beside
        )

    def over(m):
        return at.to(summed.at[m], other.at[m], s_y.at[0], r_y.at[lax.div(m, 2)], tp=at.across)

    def back(m):
        return at.to(final.at[m], arr.at[at.sp], s_b.at[0], r_b.at[0], sp=at.mate(m))

    def produce(jj):
        base = base_of(jj)
        rows = rows_of(base)
        for c in range(t):
            cols = slice(c * d, (c + 1) * d)
            value = dot(gd[rows, :], gate_t[:, cols]) + dot(ud[rows, :], up_t[:, cols])
            part[pl.ds(2 * base, 2), :, cols] = value.astype(BF16).reshape(2, cap, d)
        for m in (2 * base, 2 * base + 1):
            for k in (0, 1):
                halves(m, k).start()

    def pass_over(jj):
        base = base_of(jj)
        whole(pair.at[0, pl.ds(2 * base, 2)], r_p.at[0, base]).wait_recv()
        for m in (2 * base, 2 * base + 1):
            summed[m] = (
                part[m, :, col(at.across)].astype(F32) + pair[0, m].astype(F32)
            ).astype(BF16)
            over(m).start()

    def total(jj):
        base = base_of(jj)
        whole(pair.at[1, pl.ds(2 * base, 2)], r_p.at[1, base]).wait_recv()
        whole(other.at[pl.ds(2 * base, 2)], r_y.at[base]).wait_recv()
        for m in (2 * base, 2 * base + 1):
            final[m] = (
                part[m, :, col(at.tp)].astype(F32) + pair[1, m].astype(F32) + other[m].astype(F32)
            ).astype(BF16)

            @pl.when(m > 0)
            def _():
                back(m).start()

    def weight_grads(c):
        cols = pl.ds(pl.multiple_of(c * d, d), d)
        inputs = got[0, :, :, cols].reshape(slots, d)
        gate_grad[0, cols, :] = dot_first(inputs, gd[...]).astype(BF16)
        up_grad[0, cols, :] = dot_first(inputs, ud[...]).astype(BF16)
        sent = got[1, :, :, cols].reshape(slots, d)
        down_grad[0, :, cols] = dot_first(hidden[...], sent).astype(BF16)

    def second(j):
        @pl.when(j > 1)
        def _():
            behind(j - 2)
            produce(j - 2)

        @pl.when(j > 2)
        def _():
            pass_over(j - 3)

        @pl.when(j > 4)
        def _():
            total(j - 5)

        forward(n + 2 * j)
        forward(n + 2 * j + 1)
        ahead(j)

    loop(0, half, second)
    begin_gated(False)
    pair_gated().start()
    twin_first(0).start()
    twin_rest(0).start()
    pass_over(half - 3)
    behind(half - 2)
    produce(half - 2)
    soon_up = jnp.logical_or(z == 1, z == half - 1)
    soon_down = jnp.logical_or(z == half - 2, z == 0)
    sides(1, soon_up, soon_down)
    if half > 4:
        total(half - 5)
    loop(2 * n - lag, 2 * n, relay)
    carry(1, soon_up, soon_down)
    pass_over(half - 2)
    total(half - 4)
    behind(half - 1)
    produce(half - 1)
    total(half - 3)
    pass_over(half - 1)
    late_up, late_down = jnp.logical_not(soon_up), jnp.logical_not(soon_down)
    sides(1, late_up, late_down)
    carry(1, late_up, late_down)
    weight_grads(0)
    weight_grads(1)
    front_up = jnp.logical_and(z == 2, z < half - 1)
    front_down = jnp.logical_and(z == half - 3, z > 0)
    sides(2, front_up, front_down)
    carry(2, front_up, front_down)
    total(half - 2)
    weight_grads(2)
    total(half - 1)
    for c in range(3, t):
        weight_grads(c)
    arr[at.sp] = final[0]
    whole(arr.at[pl.ds(1, n - 1)], r_b.at[0]).wait_recv()

    moe_grad = dot(pick[...], arr[...].reshape(slots, d))
    full[:, col(at.tp)] = (c_ref[...].astype(F32) + moe_grad).astype(BF16)

    def rows_to(j):
        here = full.at[:, col(at.across if j == 2 else at.tp)]
        return at.to(here, here, s_r.at[0], r_r.at[j], tp=at.across if j == 0 else at.beside)

    def through(tp):
        rows = pl.ds(pl.multiple_of(tp * d, d), d)
        return dot(full[:, col(tp)], pw[rows, :])

    rows_to(0).start()
    rows_to(1).start()
    loads[13].wait()
    out_delta = through(at.tp)

    rows_to(1).wait_recv()
    whole(trow.at[pl.ds(1, n - 1)], r_d.at[0]).wait_recv()
    twin_first(0).wait_recv()
    join(0)
    send_along(0)
    rest_up, rest_down = jnp.logical_not(front_up), jnp.logical_not(front_down)
    sides(2, rest_up, rest_down)
    carry(2, rest_up, rest_down)
    out_delta = out_delta + through(at.beside)
    rows_to(0).wait_recv()
    rows_to(2).start()
    out_delta = out_delta + through(at.across)
    rows_to(2).wait_recv()
    out_delta = (out_delta + through(at.cross)).astype(BF16).astype(F32)
    delta[...] = (out_delta * act[...]).astype(BF16)
    states(1, rl, delta)
    twin_first(1).start()
    outg[...] = (out_delta * slp[...]).astype(BF16)

    q = tokens // t
    width = gall.shape[2]
    row = lambda tp: pl.ds(pl.multiple_of(tp * q, q), q)
    quarter = full[row(at.tp), :]
    for o in range(n):
        by[o] = quarter[:, o * width : (o + 1) * width]

    def spread_g(m):
        mate = at.mate(m)
        return at.to(
            by.at[mate], gall.at[at.sp, row(at.tp), :], s_g.at[0], r_g.at[0], sp=mate
        )

    def share_g(m, j):
        here = gall.at[at.mate(m), row(at.across if j == 2 else at.tp), :]
        came_sem = r_gs.at[0 if j == 0 else 1]
        return at.to(here, here, s_gs.at[0], came_sem, tp=at.across if j == 0 else at.beside)

    gall[at.sp, row(at.tp), :] = by[at.sp]
    loop(1, n, lambda i: spread_g(i).start())
    share_g(0, 0).start()
    share_g(0, 1).start()

    arow = exact(rates[...], (row_id <= col_id).astype(F32))
    inner = []
    scores = []
    for g in range(groups):
        wide = slice(g * STATE, (g + 1) * STATE)
        common = dot_last(wl[:, wide], rl[:, wide])
        score = jnp.zeros((tokens, tokens), F32)
        for h in range(g * per, (g + 1) * per):
            cols = slice(h * HEAD_DIM, (h + 1) * HEAD_DIM)
            fade = jnp.exp(
                -jnp.abs(acol[:, h * HEAD_DIM : h * HEAD_DIM + 1] - arow[h : h + 1, :])
            )
            inner.append(dot((fade * common).astype(BF16), delta[:, cols]))
            score += fade * dot_last(vl[:, cols], delta[:, cols])
        scores.append(score.astype(BF16))

    twin_first(1).wait_recv()
    join(1)
    send_along(1)
    twin_rest(1).start()
    def side_and_carry(k):
        sides(k, True, True)
        carry(k, True, True)

    loop(3, half, side_and_carry)
    gather_states(0)
    twin_last(0).start()
    whole(gall.at[pl.ds(1, n - 1), 0:q, :], r_g.at[0]).wait_recv()

    def forward_g(m):
        share_g(m, 0).start()
        share_g(m, 1).start()

    loop(1, n, forward_g)
    gather_states(1)
    twin_last(1).start()
    whole(gall.at[:, 0:q, :], r_gs.at[0]).wait_recv()
    loop(0, n, lambda m: share_g(m, 2).start())
    whole(gall.at[:, 0 : 2 * q, :], r_gs.at[1]).wait_recv()
    pair_gated().wait_recv()
    whole(ga.at[pl.ds(1, half - 1)], r_ls.at[0]).wait_recv()
    proj[...] = dot_first(
        gall[...].reshape(n * tokens, width), ga[...].reshape(n * tokens, d)
    )
    twin_rest(0).wait_recv()
    twin_last(0).wait_recv()
    to_end, to_start = fades[0], fades[1]
    w_low, w_high = reach(0)
    value = vl[...].astype(F32)
    moved = delta[...].astype(F32)
    d_start, d_end = (moved * to_start).astype(BF16), (moved * to_end).astype(BF16)
    v_start, v_end = (value * to_start).astype(BF16), (value * to_end).astype(BF16)
    for g in range(groups):
        wide = slice(g * STATE, (g + 1) * STATE)
        cols = slice(g * span, (g + 1) * span)
        rg[:, wide] = (
            dot_first(scores[g], wl[:, wide])
            + dot_last(d_start[:, cols], w_low[:, cols])
            + dot_last(d_end[:, cols], w_high[:, cols])
        ).astype(BF16)

    twin_rest(1).wait_recv()
    twin_last(1).wait_recv()
    r_low, r_high = reach(1)
    for g in range(groups):
        wide = slice(g * STATE, (g + 1) * STATE)
        cols = slice(g * span, (g + 1) * span)
        wg[:, wide] = (
            dot(scores[g], rl[:, wide])
            + dot_last(v_start[:, cols], r_low[:, cols])
            + dot_last(v_end[:, cols], r_high[:, cols])
        ).astype(BF16)
        vg[:, cols] = (
            jnp.concatenate(inner[g * per : (g + 1) * per], axis=1)
            + dot(wl[:, wide], r_low[:, cols]) * to_start[:, cols]
            + dot(wl[:, wide], r_high[:, cols]) * to_end[:, cols]
        ).astype(BF16)

    cols = hcol(bit)
    for ref, sem in (
        (got.at[:, :, :, 0 : 3 * d], s_sh),
        (snd.at[:, pl.ds(1, n - 1)], s_a2a),
        (trow.at[pl.ds(1, n - 1)], s_d),
        (pair, s_p),
        (summed, s_y),
        (final.at[pl.ds(1, n - 1)], s_b),
        (full.at[:, 0 : 3 * d], s_r),
        (ends.at[:, :, :, cols], s_t1),
        (ends.at[:, 0, :, cols], s_t2),
        (lowhigh.at[:, :, :, cols], s_t3),
        (lined.at[:, pl.ds(1, half - 1)], s_z),
        (ga.at[pl.ds(1, half - 1)], s_ls),
        (by.at[pl.ds(1, n - 1)], s_g),
        (gall.at[:, 0 : 3 * q, :], s_gs),
    ):
        whole(ref, sem.at[0]).wait_send()
    pair_gated().wait_send()

    def drain(k):
        @pl.when(jnp.logical_and(z - k >= 0, z < half - 1))
        def _():
            hop(True, k).wait_send()

        @pl.when(jnp.logical_and(z + k < half, z > 0))
        def _():
            hop(False, k).wait_send()

    loop(0, half, drain)


def put_out_kernel(*refs):
    count = len(refs) // 2
    copies = [
        pltpu.make_async_copy(refs[i], refs[count + i], refs[-1].at[i]) for i in range(count)
    ]
    for copy in copies:
        copy.start()
    for copy in copies:
        copy.wait()


def held(scratch):
    shape, size = scratch.shape, jnp.dtype(scratch.dtype).itemsize
    minor = -(-shape[-1] // 128) * 128
    rows = -(-shape[-2] // 16) * 16
    return functools.reduce(lambda a, b: a * b, shape[:-2], minor * rows * size)


def on_device(
    layer_input,
    cotangent,
    routes,
    route_weight,
    gate_weight,
    up_weight,
    down_weight,
    heads_value,
    output_gate,
    mixer_saved,
    proj_weight,
    state_write,
    state_read,
    decay_rate,
):
    n = lax.axis_size("sp")
    t = lax.axis_size("tp")
    tokens, d = layer_input.shape
    top = routes.shape[1]
    capacity = -(-max(2, 3 * tokens * top // (2 * n)) // 16) * 16
    slots = n * capacity
    hid = gate_weight.shape[2]
    half = n // 2
    width = t * d // n
    state_w = state_write.shape[1]
    sds = jax.ShapeDtypeStruct
    block = (n, capacity, d)
    vm = pl.BlockSpec(memory_space=pltpu.VMEM)
    hbm = pl.BlockSpec(memory_space=pltpu.HBM)
    one = (1,)
    sems = [
        (14,), one, (2, n), one, (2, n), (2, half), one, one, one, (2, half), one, (half,),
        one, one, one, (3,),
        one, (2,), one, (2,), one, (2,), one, (2,), (2, half), (2, half),
        one, one, one, one, one, one, one, (2,),
    ]
    outs = (
        sds((1, t * d, hid), BF16),
        sds((1, t * d, hid), BF16),
        sds((1, hid, t * d), BF16),
        sds((width, d), F32),
        sds((tokens, d), BF16),
        sds((tokens, state_w), BF16),
        sds((tokens, state_w), BF16),
        sds((tokens, d), BF16),
    )
    operands = (
        routes.T,
        route_weight.T,
        decay_rate.T,
        layer_input,
        cotangent,
        heads_value,
        output_gate,
        mixer_saved,
        state_write,
        state_read,
        gate_weight,
        up_weight,
        down_weight,
        proj_weight,
    )
    scratch = [VMEM(x.shape[-2:], x.dtype) for x in operands] + [
        VMEM((2,) + block, BF16),
        VMEM((2, n, capacity, t * d), BF16),
        VMEM((slots, hid), F32),
        VMEM((slots, hid), F32),
        VMEM((slots, hid), BF16),
        VMEM((slots, hid), BF16),
        VMEM((slots, hid), BF16),
        VMEM((n, capacity, t * d), BF16),
        VMEM((2,) + block, BF16),
        VMEM(block, BF16),
        VMEM(block, BF16),
        VMEM(block, BF16),
        VMEM(block, BF16),
        VMEM((tokens, slots), BF16),
        VMEM((n, 1, d), F32),
        VMEM((tokens, d), F32),
        VMEM((2, tokens, d), F32),
        VMEM((tokens, d), F32),
        VMEM((tokens, d), F32),
        VMEM((2, 2, STATE, d), BF16),
        VMEM((2, 2, STATE, d), BF16),
        VMEM((2, 2, STATE, d // 2), BF16),
        VMEM((2, half, STATE, d // 2), BF16),
        VMEM((2, 2, STATE, d), BF16),
        VMEM((tokens, d), BF16),
        VMEM((n, tokens, d), BF16),
        VMEM((tokens, t * d), BF16),
        VMEM((n, tokens // t, width), BF16),
        VMEM((n, tokens, width), BF16),
        VMEM((hid, t * d), BF16),
        VMEM((hid, t * d), BF16),
        VMEM((t * d, hid), BF16),
    ]
    grads = pl.pallas_call(
        functools.partial(layer_kernel, n, t, capacity),
        out_shape=outs,
        in_specs=[hbm] * 14,
        out_specs=(vm,) * 8,
        scratch_shapes=scratch + [DMA(shape) for shape in sems],
        compiler_params=pltpu.CompilerParams(
            collective_id=1,
            has_side_effects=True,
            vmem_limit_bytes=min(60 * MIB, sum(map(held, scratch)) + 8 * MIB),
        ),
        cost_estimate=pl.CostEstimate(
            flops=4_000_000_000, bytes_accessed=8_000_000, transcendentals=0
        ),
        name="layer",
    )(*(pltpu.with_memory_space_constraint(x, pltpu.HBM) for x in operands))
    return pl.pallas_call(
        put_out_kernel,
        out_shape=outs,
        in_specs=[vm] * len(outs),
        out_specs=(hbm,) * len(outs),
        scratch_shapes=[DMA((len(outs),))],
        compiler_params=pltpu.CompilerParams(vmem_limit_bytes=12 * MIB),
        name="put_out",
    )(*grads)


def solution(mesh):
    split = P("sp", "tp")
    in_specs = (
        split,
        split,
        P("sp", None),
        P("sp", None),
        P("sp", None, "tp"),
        P("sp", None, "tp"),
        P("sp", "tp", None),
        split,
        split,
        split,
        P(None, "tp"),
        split,
        split,
        split,
    )
    out_specs = (
        P("sp", None, "tp"),
        P("sp", None, "tp"),
        P("sp", "tp", None),
        split,
        split,
        split,
        split,
        split,
    )
    return jax.shard_map(
        on_device, mesh=mesh, in_specs=in_specs, out_specs=out_specs, check_vma=False
    )
```

```python
import functools

import jax
import jax.numpy as jnp
from jax import lax
from jax.experimental import pallas as pl
from jax.experimental.pallas import tpu as pltpu
from jax.sharding import PartitionSpec as P

HEAD_DIM = 64
STATE = 128
MESH = pl.DeviceIdType.MESH
LAST = (((1,), (1,)), ((), ()))
FIRST = (((0,), (0,)), ((), ()))
F32 = jnp.float32
BF16 = jnp.bfloat16
VMEM = pltpu.VMEM
DMA = pltpu.SemaphoreType.DMA
MIB = 1024 * 1024


def silu_parts(value):
    sigma = jax.nn.sigmoid(value)
    return (value * sigma, sigma * (1.0 + value * (1.0 - sigma)))


def dot_first(a, b):
    return lax.dot_general(a, b, FIRST, preferred_element_type=F32)


def dot_last(a, b):
    return lax.dot_general(a, b, LAST, preferred_element_type=F32)


def dot(a, b):
    return jnp.dot(a, b, preferred_element_type=F32)


def exact(a, b, dims=(((1,), (0,)), ((), ()))):
    return lax.dot_general(
        a, b, dims, precision=lax.Precision.HIGHEST, preferred_element_type=F32
    )


def flip(a, b, n):
    out, bit = 0, 1
    while bit < n:
        out = out + lax.rem(lax.div(a, bit) + lax.div(b, bit), 2) * bit
        bit *= 2
    return out


class Place:
    def __init__(self, n, t):
        self.n, self.t = n, t
        self.sp = lax.axis_index("sp")
        self.tp = lax.axis_index("tp")
        self.across = lax.rem(self.tp + t // 2, t)
        self.beside = self.tp + 1 - 2 * lax.rem(self.tp, 2)
        self.cross = lax.rem(self.beside + t // 2, t)

    def mate(self, m):
        return flip(self.sp, jnp.int32(m), self.n)

    def to(self, src, dst, send, recv, sp=None, tp=None):
        return pltpu.make_async_remote_copy(
            src_ref=src,
            dst_ref=dst,
            send_sem=send,
            recv_sem=recv,
            device_id=(self.sp if sp is None else sp, self.tp if tp is None else tp),
            device_id_type=MESH,
        )


def loop(lo, hi, body):
    def step(i, carry):
        body(i)
        return carry

    lax.fori_loop(lo, hi, step, 0)


def layer_kernel(n, t, cap, *refs):
    count = 14
    sources, refs = refs[:count], refs[count:]
    gate_grad, up_grad, down_grad, proj, vg, wg, rg, outg = refs[:8]
    held_in, refs = refs[8 : 8 + count], refs[8 + count :]
    routes, rweight, rates, x_ref, c_ref, vl, og, ms, wl, rl, gate, up, down, pw = held_in
    (
        snd, got, pg, pu, hidden, gd, ud, part, pair, summed, other, final, arr, pick, trow,
        acol, fades, act, slp, ends, twins, joint, lined, lowhigh, delta, ga, full, by, gall,
        gate_t, up_t, down_t,
    ) = refs[:32]
    (
        w_sem, s_a2a, r_a2a, s_sh, r_sh, r_side, s_d, r_d, s_p, r_p, s_y, r_y, s_b, r_b, s_r, r_r,
        s_t1, r_t1, s_t2, r_t2, s_t3, r_t3, s_z, r_z, s_l, r_l, s_ls, r_ls, s_x, r_x, s_g, r_g,
        s_gs, r_gs,
    ) = refs[32:]
    at = Place(n, t)
    tokens, d = x_ref.shape
    top = routes.shape[0]
    slots = n * cap
    half = n // 2
    duo = 2 * cap
    heads = rates.shape[0]
    per = heads * STATE // wl.shape[1]
    span = per * HEAD_DIM
    groups = heads // per
    z = lax.div(at.sp, 2)
    bit = lax.rem(at.sp, 2)
    twin = at.sp + 1 - 2 * bit
    mate_one = twin
    col = lambda tp: pl.ds(pl.multiple_of(tp * d, d), d)
    hcol = lambda b: pl.ds(pl.multiple_of(b * (d // 2), d // 2), d // 2)

    barrier = pltpu.get_barrier_semaphore()
    for tp in (at.across, at.beside):
        pl.semaphore_signal(barrier, inc=1, device_id=(at.sp, tp), device_id_type=MESH)

    def hello(o):
        pl.semaphore_signal(
            barrier, inc=1, device_id=(lax.rem(at.sp + o, n), at.tp), device_id_type=MESH
        )

    loop(1, n, hello)
    loads = [
        pltpu.make_async_copy(
            src if len(src.shape) == len(dst.shape) else src.at[0], dst, w_sem.at[i]
        )
        for i, (src, dst) in enumerate(zip(sources, held_in))
    ]
    for load in loads:
        load.start()
    for load in loads[:3]:
        load.wait()

    row_id = lax.broadcasted_iota(jnp.int32, (tokens, tokens), 0)
    col_id = lax.broadcasted_iota(jnp.int32, (tokens, tokens), 1)
    eye = (row_id == col_id).astype(F32)
    named = exact(eye, routes[...].astype(F32), LAST)
    weights = exact(eye, rweight[...], LAST)
    lanes = lax.broadcasted_iota(jnp.int32, (tokens, n), 1).astype(F32)
    onehot = [(named[:, k : k + 1] == lanes).astype(F32) for k in range(top)]
    lower = (row_id > col_id).astype(F32)
    before = dot(lower.astype(BF16), sum(onehot).astype(BF16))
    slot_lane = lax.broadcasted_iota(jnp.int32, (tokens, slots), 1).astype(F32)
    picks = []
    for k in range(top):
        rank = jnp.sum(before * onehot[k], axis=1, keepdims=True)
        picks.append((named[:, k : k + 1] * cap + rank == slot_lane).astype(F32).astype(BF16))
    pick[...] = sum(picks)
    for load in loads[3:5]:
        load.wait()
    snd[0] = dot_first(pick[...], x_ref[...]).astype(BF16).reshape(n, cap, d)
    got[0, 0, :, col(at.tp)] = snd[0, at.sp]
    pl.semaphore_wait(barrier, n + 1)

    def whole(ref, sem):
        return at.to(ref, ref, sem, sem, sp=mate_one)

    def to_columns(value):
        lane = lax.broadcasted_iota(jnp.int32, (heads, d), 1)
        lead = lax.broadcasted_iota(jnp.int32, (heads, d), 0) * HEAD_DIM
        spread_heads = jnp.logical_and(lane >= lead, lane < lead + HEAD_DIM).astype(F32)
        return exact(value, spread_heads, FIRST)

    def prepare():
        upto = (row_id >= col_id).astype(F32)
        acol[...] = exact(upto, to_columns(rates[...]))
        trow[at.sp] = acol[tokens - 1 : tokens, :]
        a = acol[...]
        fades[0] = jnp.exp(a - a[tokens - 1 : tokens, :])
        fades[1] = jnp.exp(-a)
        active_gate, slope_gate = silu_parts(og[...].astype(F32))
        saved = ms[...].astype(F32)
        ga[at.sp] = (saved * active_gate).astype(BF16)
        act[...] = active_gate
        slp[...] = saved * slope_gate

    def states(kind, left, right):
        value = right[...].astype(F32)
        for i in (0, 1):
            faded = (value * fades[i]).astype(BF16)
            for g in range(groups):
                ends[kind, i, :, g * span : (g + 1) * span] = dot_first(
                    left[:, g * STATE : (g + 1) * STATE], faded[:, g * span : (g + 1) * span]
                ).astype(BF16)

    def totals(m):
        mate = at.mate(m)
        return at.to(trow.at[at.sp], trow.at[at.sp], s_d.at[0], r_d.at[0], sp=mate)

    def twin_first(kind):
        cols = hcol(1 - bit)
        return at.to(
            ends.at[kind, :, :, cols], twins.at[kind, :, :, cols], s_t1.at[0], r_t1.at[kind],
            sp=twin,
        )

    def twin_rest(kind):
        cols = hcol(bit)
        return at.to(
            ends.at[kind, bit, :, cols], twins.at[kind, bit, :, cols], s_t2.at[0],
            r_t2.at[kind], sp=twin,
        )

    def along(kind, o):
        there = lax.rem(z + o, half)
        return at.to(
            joint.at[kind, jnp.where(there > z, 0, 1)], lined.at[kind, z], s_z.at[0],
            r_z.at[kind], sp=there * 2 + bit,
        )

    def twin_last(kind):
        here = lowhigh.at[kind, :, :, hcol(bit)]
        return at.to(here, here, s_t3.at[0], r_t3.at[kind], sp=twin)

    def join(kind):
        cols = hcol(bit)
        mine = jnp.exp(-trow[at.sp, :, cols])
        his = jnp.exp(-trow[twin, :, cols])
        second = (bit == 1).astype(F32)
        keep_end = second + (1.0 - second) * his
        his_end = (1.0 - second) + second * mine
        keep_start = (1.0 - second) + second * his
        his_start = second + (1.0 - second) * mine
        own = ends[kind, :, :, cols].astype(F32)
        got_twin = twins[kind, :, :, cols].astype(F32)
        joint[kind, 0] = (own[0] * keep_end + got_twin[0] * his_end).astype(BF16)
        joint[kind, 1] = (own[1] * keep_start + got_twin[1] * his_start).astype(BF16)

    def send_along(kind):
        loop(1, half, lambda o: along(kind, o).start())

    def gather_states(kind):
        cols = hcol(bit)
        whole(lined.at[kind, pl.ds(1, half - 1)], r_z.at[kind]).wait_recv()

        def both(y):
            return trow[2 * y, :, cols] + trow[2 * y + 1, :, cols]

        zero = jnp.zeros((STATE, d // 2), F32)

        def before_me(i, carry):
            total, fade = carry
            y = z - 1 - i
            total = total + jnp.exp(-fade) * lined[kind, y].astype(F32)
            return total, fade + both(y)

        def after_me(i, carry):
            total, fade = carry
            y = z + 1 + i
            total = total + jnp.exp(-fade) * lined[kind, y].astype(F32)
            return total, fade + both(y)

        none = jnp.zeros((1, d // 2), F32)
        low, _ = lax.fori_loop(0, z, before_me, (zero, none))
        high, _ = lax.fori_loop(0, half - 1 - z, after_me, (zero, none))
        lowhigh[kind, 0, :, cols] = low.astype(BF16)
        lowhigh[kind, 1, :, cols] = high.astype(BF16)

    def reach(kind):
        his = jnp.exp(-trow[twin])
        second = (bit == 1).astype(F32)
        extra = twins[kind, 1 - bit].astype(F32)
        low = lowhigh[kind, 0].astype(F32) * (1.0 - second + second * his) + extra * second
        high = lowhigh[kind, 1].astype(F32) * (second + (1.0 - second) * his) + extra * (
            1.0 - second
        )
        return low.astype(BF16), high.astype(BF16)

    def hop(up, k):
        here = ga.at[(z - k if up else z + k) * 2 + bit]
        i = 0 if up else 1
        peer = z + 1 if up else z - 1
        return at.to(here, here, s_l.at[i, k], r_l.at[i, k], sp=peer * 2 + bit)

    def came(up, k):
        here = ga.at[(z - k if up else z + k) * 2 + bit]
        i = 0 if up else 1
        return at.to(here, here, s_l.at[i, k], r_l.at[i, k - 1], sp=twin)

    def side(up, k):
        here = ga.at[(z - k if up else z + k) * 2 + bit]
        i = 0 if up else 1
        return at.to(here, here, s_ls.at[0], r_ls.at[0], sp=twin)

    def pair_gated():
        return at.to(ga.at[at.sp], ga.at[at.sp], s_x.at[0], r_x.at[0], sp=twin)

    outer_up = jnp.logical_or(z == 0, z == half - 2)
    outer_down = jnp.logical_or(z == half - 1, z == 1)

    def begin_gated(outer):
        @pl.when(jnp.logical_and(z < half - 1, outer_up == outer))
        def _():
            hop(True, 0).start()

        @pl.when(jnp.logical_and(z > 0, outer_down == outer))
        def _():
            hop(False, 0).start()

    def each_way(k, up_if, down_if, act):
        @pl.when(jnp.logical_and(z - k >= 0, up_if))
        def _():
            act(True)

        @pl.when(jnp.logical_and(z + k < half, down_if))
        def _():
            act(False)

    def carry(k, up_if, down_if):
        each_way(k, jnp.logical_and(up_if, z < half - 1), jnp.logical_and(down_if, z > 0),
                 lambda up: hop(up, k).start())

    def sides(k, up_if, down_if):
        def act(up):
            came(up, k).wait_recv()
            side(up, k).start()

        each_way(k, up_if, down_if, act)

    def spread(k, m):
        mate = at.mate(m)
        return at.to(
            snd.at[k, mate], got.at[k, m, :, col(at.tp)], s_a2a.at[0], r_a2a.at[k, m], sp=mate
        )

    def share(k, m, j):
        here = got.at[k, m, :, col(at.across if j == 2 else at.tp)]
        came_sem = r_sh.at[k, m] if j == 0 else r_side.at[k, lax.div(m, 2)]
        return at.to(here, here, s_sh.at[0], came_sem, tp=at.across if j == 0 else at.beside)

    loop(1, n, lambda i: spread(0, i).start())
    own = jnp.int32(0)
    share(0, own, 0).start()
    share(0, own, 1).start()
    cot = c_ref[...].astype(F32)
    weighted = [(cot * weights[:, k : k + 1]).astype(BF16) for k in range(top)]
    snd[1] = dot_first(
        jnp.concatenate(picks, axis=0), jnp.concatenate(weighted, axis=0)
    ).astype(BF16).reshape(n, cap, d)
    got[1, 0, :, col(at.tp)] = snd[1, at.sp]
    for load in loads[5:10]:
        load.wait()
    prepare()
    states(0, wl, vl)
    loop(1, n, lambda m: totals(m).start())
    begin_gated(True)
    share(1, own, 0).start()
    share(1, own, 1).start()

    lag = 2

    def forward(q):
        k, i = lax.div(q, n), lax.rem(q, n)
        m = i

        @pl.when(i > 0)
        def _():
            spread(k, m).wait_recv()
            share(k, m, 0).start()
            share(k, m, 1).start()

        @pl.when(jnp.logical_and(k == 0, i > 0))
        def _():
            spread(1, i).start()

        @pl.when(q >= lag)
        def _():
            relay(q - lag)

    def relay(q):
        k, m = lax.div(q, n), lax.rem(q, n)
        share(k, jnp.int32(m), 0).wait_recv()
        share(k, m, 2).start()

    def settled(k, base):
        whole(got.at[k, pl.ds(2 * base, 2), :, 0 : 2 * d], r_side.at[k, base]).wait_recv()

    def base_of(j):
        return jnp.int32(j)

    def rows_of(base):
        return pl.ds(pl.multiple_of(base * duo, duo), duo)

    def ahead(j):
        base = base_of(j)
        settled(0, base)
        rows = rows_of(base)
        inputs = got[0, pl.ds(2 * base, 2)].reshape(duo, t * d)
        pg[rows, :] = dot(inputs, gate[...])
        pu[rows, :] = dot(inputs, up[...])

    def behind(j):
        base = base_of(j)
        settled(1, base)
        rows = rows_of(base)
        sent = got[1, pl.ds(2 * base, 2)].reshape(duo, t * d)
        grad = dot(sent, down_t[...])
        active, slope = silu_parts(pg[rows, :])
        ups = pu[rows, :]
        hidden[rows, :] = (active * ups).astype(BF16)
        gd[rows, :] = (grad * ups * slope).astype(BF16)
        ud[rows, :] = (grad * active).astype(BF16)

    for load in loads[10:13]:
        load.wait()

    def turn(c):
        cols = pl.ds(pl.multiple_of(c * d, d), d)
        gate_t[:, cols] = gate[cols, :].T
        up_t[:, cols] = up[cols, :].T
        down_t[cols, :] = down[:, cols].T

    share_of = n // t

    def first(i):
        forward(i)

        @pl.when(lax.rem(i, share_of) == share_of - 1)
        def _():
            turn(lax.div(i, share_of))

    loop(1, n, first)

    def halves(m, k):
        c = at.cross if k == 0 else at.beside
        return at.to(
            part.at[m, :, col(c)], pair.at[k, m], s_p.at[0], r_p.at[k, lax.div(m, 2)], tp=at.beside
        )

    def over(m):
        return at.to(summed.at[m], other.at[m], s_y.at[0], r_y.at[lax.div(m, 2)], tp=at.across)

    def back(m):
        return at.to(final.at[m], arr.at[at.sp], s_b.at[0], r_b.at[0], sp=at.mate(m))

    def produce(jj):
        base = base_of(jj)
        rows = rows_of(base)
        for c in range(t):
            cols = slice(c * d, (c + 1) * d)
            value = dot(gd[rows, :], gate_t[:, cols]) + dot(ud[rows, :], up_t[:, cols])
            part[pl.ds(2 * base, 2), :, cols] = value.astype(BF16).reshape(2, cap, d)
        for m in (2 * base, 2 * base + 1):
            for k in (0, 1):
                halves(m, k).start()

    def pass_over(jj):
        base = base_of(jj)
        whole(pair.at[0, pl.ds(2 * base, 2)], r_p.at[0, base]).wait_recv()
        for m in (2 * base, 2 * base + 1):
            summed[m] = (
                part[m, :, col(at.across)].astype(F32) + pair[0, m].astype(F32)
            ).astype(BF16)
            over(m).start()

    def total(jj):
        base = base_of(jj)
        whole(pair.at[1, pl.ds(2 * base, 2)], r_p.at[1, base]).wait_recv()
        whole(other.at[pl.ds(2 * base, 2)], r_y.at[base]).wait_recv()
        for m in (2 * base, 2 * base + 1):
            final[m] = (
                part[m, :, col(at.tp)].astype(F32) + pair[1, m].astype(F32) + other[m].astype(F32)
            ).astype(BF16)

            @pl.when(m > 0)
            def _():
                back(m).start()

    def weight_grads(c):
        cols = pl.ds(pl.multiple_of(c * d, d), d)
        inputs = got[0, :, :, cols].reshape(slots, d)
        gate_grad[0, cols, :] = dot_first(inputs, gd[...]).astype(BF16)
        up_grad[0, cols, :] = dot_first(inputs, ud[...]).astype(BF16)
        sent = got[1, :, :, cols].reshape(slots, d)
        down_grad[0, :, cols] = dot_first(hidden[...], sent).astype(BF16)

    def second(j):
        @pl.when(j > 1)
        def _():
            behind(j - 2)
            produce(j - 2)

        @pl.when(j > 2)
        def _():
            pass_over(j - 3)

        @pl.when(j > 4)
        def _():
            total(j - 5)

        forward(n + 2 * j)
        forward(n + 2 * j + 1)
        ahead(j)

    loop(0, half, second)
    begin_gated(False)
    pair_gated().start()
    twin_first(0).start()
    twin_rest(0).start()
    pass_over(half - 3)
    behind(half - 2)
    produce(half - 2)
    soon_up = jnp.logical_or(z == 1, z == half - 1)
    soon_down = jnp.logical_or(z == half - 2, z == 0)
    sides(1, soon_up, soon_down)
    if half > 4:
        total(half - 5)
    loop(2 * n - lag, 2 * n, relay)
    carry(1, soon_up, soon_down)
    pass_over(half - 2)
    total(half - 4)
    behind(half - 1)
    produce(half - 1)
    total(half - 3)
    pass_over(half - 1)
    late_up, late_down = jnp.logical_not(soon_up), jnp.logical_not(soon_down)
    sides(1, late_up, late_down)
    carry(1, late_up, late_down)
    weight_grads(0)
    weight_grads(1)
    front_up = jnp.logical_and(z == 2, z < half - 1)
    front_down = jnp.logical_and(z == half - 3, z > 0)
    sides(2, front_up, front_down)
    carry(2, front_up, front_down)
    total(half - 2)
    weight_grads(2)
    total(half - 1)
    for c in range(3, t):
        weight_grads(c)
    arr[at.sp] = final[0]
    whole(arr.at[pl.ds(1, n - 1)], r_b.at[0]).wait_recv()

    moe_grad = dot(pick[...], arr[...].reshape(slots, d))
    full[:, col(at.tp)] = (c_ref[...].astype(F32) + moe_grad).astype(BF16)

    def rows_to(j):
        here = full.at[:, col(at.across if j == 2 else at.tp)]
        return at.to(here, here, s_r.at[0], r_r.at[j], tp=at.across if j == 0 else at.beside)

    def through(tp):
        rows = pl.ds(pl.multiple_of(tp * d, d), d)
        return dot(full[:, col(tp)], pw[rows, :])

    rows_to(0).start()
    rows_to(1).start()
    loads[13].wait()
    out_delta = through(at.tp)

    rows_to(1).wait_recv()
    whole(trow.at[pl.ds(1, n - 1)], r_d.at[0]).wait_recv()
    twin_first(0).wait_recv()
    join(0)
    send_along(0)
    rest_up, rest_down = jnp.logical_not(front_up), jnp.logical_not(front_down)
    sides(2, rest_up, rest_down)
    carry(2, rest_up, rest_down)
    out_delta = out_delta + through(at.beside)
    rows_to(0).wait_recv()
    rows_to(2).start()
    out_delta = out_delta + through(at.across)
    rows_to(2).wait_recv()
    out_delta = (out_delta + through(at.cross)).astype(BF16).astype(F32)
    delta[...] = (out_delta * act[...]).astype(BF16)
    states(1, rl, delta)
    twin_first(1).start()
    outg[...] = (out_delta * slp[...]).astype(BF16)

    q = tokens // t
    width = gall.shape[2]
    row = lambda tp: pl.ds(pl.multiple_of(tp * q, q), q)
    quarter = full[row(at.tp), :]
    for o in range(n):
        by[o] = quarter[:, o * width : (o + 1) * width]

    def spread_g(m):
        mate = at.mate(m)
        return at.to(
            by.at[mate], gall.at[at.sp, row(at.tp), :], s_g.at[0], r_g.at[0], sp=mate
        )

    def share_g(m, j):
        here = gall.at[at.mate(m), row(at.across if j == 2 else at.tp), :]
        came_sem = r_gs.at[0 if j == 0 else 1]
        return at.to(here, here, s_gs.at[0], came_sem, tp=at.across if j == 0 else at.beside)

    gall[at.sp, row(at.tp), :] = by[at.sp]
    loop(1, n, lambda i: spread_g(i).start())
    share_g(0, 0).start()
    share_g(0, 1).start()

    arow = exact(rates[...], (row_id <= col_id).astype(F32))
    inner = []
    scores = []
    for g in range(groups):
        wide = slice(g * STATE, (g + 1) * STATE)
        common = dot_last(wl[:, wide], rl[:, wide])
        score = jnp.zeros((tokens, tokens), F32)
        for h in range(g * per, (g + 1) * per):
            cols = slice(h * HEAD_DIM, (h + 1) * HEAD_DIM)
            fade = jnp.exp(
                -jnp.abs(acol[:, h * HEAD_DIM : h * HEAD_DIM + 1] - arow[h : h + 1, :])
            )
            inner.append(dot((fade * common).astype(BF16), delta[:, cols]))
            score += fade * dot_last(vl[:, cols], delta[:, cols])
        scores.append(score.astype(BF16))

    twin_first(1).wait_recv()
    join(1)
    send_along(1)
    twin_rest(1).start()
    def side_and_carry(k):
        sides(k, True, True)
        carry(k, True, True)

    loop(3, half, side_and_carry)
    gather_states(0)
    twin_last(0).start()
    whole(gall.at[pl.ds(1, n - 1), 0:q, :], r_g.at[0]).wait_recv()

    def forward_g(m):
        share_g(m, 0).start()
        share_g(m, 1).start()

    loop(1, n, forward_g)
    gather_states(1)
    twin_last(1).start()
    whole(gall.at[:, 0:q, :], r_gs.at[0]).wait_recv()
    loop(0, n, lambda m: share_g(m, 2).start())
    whole(gall.at[:, 0 : 2 * q, :], r_gs.at[1]).wait_recv()
    pair_gated().wait_recv()
    whole(ga.at[pl.ds(1, half - 1)], r_ls.at[0]).wait_recv()
    proj[...] = dot_first(
        gall[...].reshape(n * tokens, width), ga[...].reshape(n * tokens, d)
    )
    twin_rest(0).wait_recv()
    twin_last(0).wait_recv()
    to_end, to_start = fades[0], fades[1]
    w_low, w_high = reach(0)
    value = vl[...].astype(F32)
    moved = delta[...].astype(F32)
    d_start, d_end = (moved * to_start).astype(BF16), (moved * to_end).astype(BF16)
    v_start, v_end = (value * to_start).astype(BF16), (value * to_end).astype(BF16)
    for g in range(groups):
        wide = slice(g * STATE, (g + 1) * STATE)
        cols = slice(g * span, (g + 1) * span)
        rg[:, wide] = (
            dot_first(scores[g], wl[:, wide])
            + dot_last(d_start[:, cols], w_low[:, cols])
            + dot_last(d_end[:, cols], w_high[:, cols])
        ).astype(BF16)

    twin_rest(1).wait_recv()
    twin_last(1).wait_recv()
    r_low, r_high = reach(1)
    for g in range(groups):
        wide = slice(g * STATE, (g + 1) * STATE)
        cols = slice(g * span, (g + 1) * span)
        wg[:, wide] = (
            dot(scores[g], rl[:, wide])
            + dot_last(v_start[:, cols], r_low[:, cols])
            + dot_last(v_end[:, cols], r_high[:, cols])
        ).astype(BF16)
        vg[:, cols] = (
            jnp.concatenate(inner[g * per : (g + 1) * per], axis=1)
            + dot(wl[:, wide], r_low[:, cols]) * to_start[:, cols]
            + dot(wl[:, wide], r_high[:, cols]) * to_end[:, cols]
        ).astype(BF16)

    cols = hcol(bit)
    for ref, sem in (
        (got.at[:, :, :, 0 : 3 * d], s_sh),
        (snd.at[:, pl.ds(1, n - 1)], s_a2a),
        (trow.at[pl.ds(1, n - 1)], s_d),
        (pair, s_p),
        (summed, s_y),
        (final.at[pl.ds(1, n - 1)], s_b),
        (full.at[:, 0 : 3 * d], s_r),
        (ends.at[:, :, :, cols], s_t1),
        (ends.at[:, 0, :, cols], s_t2),
        (lowhigh.at[:, :, :, cols], s_t3),
        (lined.at[:, pl.ds(1, half - 1)], s_z),
        (ga.at[pl.ds(1, half - 1)], s_ls),
        (by.at[pl.ds(1, n - 1)], s_g),
        (gall.at[:, 0 : 3 * q, :], s_gs),
    ):
        whole(ref, sem.at[0]).wait_send()
    pair_gated().wait_send()

    def drain(k):
        @pl.when(jnp.logical_and(z - k >= 0, z < half - 1))
        def _():
            hop(True, k).wait_send()

        @pl.when(jnp.logical_and(z + k < half, z > 0))
        def _():
            hop(False, k).wait_send()

    loop(0, half, drain)


def put_out_kernel(*refs):
    count = len(refs) // 2
    copies = [
        pltpu.make_async_copy(refs[i], refs[count + i], refs[-1].at[i]) for i in range(count)
    ]
    for i, copy in enumerate(copies):
        rows = refs[i].shape[-2]
        if rows < 256:
            copy.start()
            continue
        for j in range(4):
            piece = (slice(None),) * (len(refs[i].shape) - 2) + (pl.ds(j * rows // 4, rows // 4),)
            pltpu.make_async_copy(
                refs[i].at[piece], refs[count + i].at[piece], refs[-1].at[i]
            ).start()
    for copy in copies:
        copy.wait()


def held(scratch):
    shape, size = scratch.shape, jnp.dtype(scratch.dtype).itemsize
    minor = -(-shape[-1] // 128) * 128
    rows = -(-shape[-2] // 16) * 16
    return functools.reduce(lambda a, b: a * b, shape[:-2], minor * rows * size)


def on_device(
    layer_input,
    cotangent,
    routes,
    route_weight,
    gate_weight,
    up_weight,
    down_weight,
    heads_value,
    output_gate,
    mixer_saved,
    proj_weight,
    state_write,
    state_read,
    decay_rate,
):
    n = lax.axis_size("sp")
    t = lax.axis_size("tp")
    tokens, d = layer_input.shape
    top = routes.shape[1]
    capacity = -(-max(2, 3 * tokens * top // (2 * n)) // 16) * 16
    slots = n * capacity
    hid = gate_weight.shape[2]
    half = n // 2
    width = t * d // n
    state_w = state_write.shape[1]
    sds = jax.ShapeDtypeStruct
    block = (n, capacity, d)
    vm = pl.BlockSpec(memory_space=pltpu.VMEM)
    hbm = pl.BlockSpec(memory_space=pltpu.HBM)
    one = (1,)
    sems = [
        (14,), one, (2, n), one, (2, n), (2, half), one, one, one, (2, half), one, (half,),
        one, one, one, (3,),
        one, (2,), one, (2,), one, (2,), one, (2,), (2, half), (2, half),
        one, one, one, one, one, one, one, (2,),
    ]
    outs = (
        sds((1, t * d, hid), BF16),
        sds((1, t * d, hid), BF16),
        sds((1, hid, t * d), BF16),
        sds((width, d), F32),
        sds((tokens, d), BF16),
        sds((tokens, state_w), BF16),
        sds((tokens, state_w), BF16),
        sds((tokens, d), BF16),
    )
    operands = (
        routes.T,
        route_weight.T,
        decay_rate.T,
        layer_input,
        cotangent,
        heads_value,
        output_gate,
        mixer_saved,
        state_write,
        state_read,
        gate_weight,
        up_weight,
        down_weight,
        proj_weight,
    )
    scratch = [VMEM(x.shape[-2:], x.dtype) for x in operands] + [
        VMEM((2,) + block, BF16),
        VMEM((2, n, capacity, t * d), BF16),
        VMEM((slots, hid), F32),
        VMEM((slots, hid), F32),
        VMEM((slots, hid), BF16),
        VMEM((slots, hid), BF16),
        VMEM((slots, hid), BF16),
        VMEM((n, capacity, t * d), BF16),
        VMEM((2,) + block, BF16),
        VMEM(block, BF16),
        VMEM(block, BF16),
        VMEM(block, BF16),
        VMEM(block, BF16),
        VMEM((tokens, slots), BF16),
        VMEM((n, 1, d), F32),
        VMEM((tokens, d), F32),
        VMEM((2, tokens, d), F32),
        VMEM((tokens, d), F32),
        VMEM((tokens, d), F32),
        VMEM((2, 2, STATE, d), BF16),
        VMEM((2, 2, STATE, d), BF16),
        VMEM((2, 2, STATE, d // 2), BF16),
        VMEM((2, half, STATE, d // 2), BF16),
        VMEM((2, 2, STATE, d), BF16),
        VMEM((tokens, d), BF16),
        VMEM((n, tokens, d), BF16),
        VMEM((tokens, t * d), BF16),
        VMEM((n, tokens // t, width), BF16),
        VMEM((n, tokens, width), BF16),
        VMEM((hid, t * d), BF16),
        VMEM((hid, t * d), BF16),
        VMEM((t * d, hid), BF16),
    ]
    grads = pl.pallas_call(
        functools.partial(layer_kernel, n, t, capacity),
        out_shape=outs,
        in_specs=[hbm] * 14,
        out_specs=(vm,) * 8,
        scratch_shapes=scratch + [DMA(shape) for shape in sems],
        compiler_params=pltpu.CompilerParams(
            collective_id=1,
            has_side_effects=True,
            vmem_limit_bytes=min(60 * MIB, sum(map(held, scratch)) + 8 * MIB),
        ),
        cost_estimate=pl.CostEstimate(
            flops=4_000_000_000, bytes_accessed=8_000_000, transcendentals=0
        ),
        name="layer",
    )(*(pltpu.with_memory_space_constraint(x, pltpu.HBM) for x in operands))
    return pl.pallas_call(
        put_out_kernel,
        out_shape=outs,
        in_specs=[vm] * len(outs),
        out_specs=(hbm,) * len(outs),
        scratch_shapes=[DMA((len(outs),))],
        compiler_params=pltpu.CompilerParams(vmem_limit_bytes=12 * MIB),
        name="put_out",
    )(*grads)


def solution(mesh):
    split = P("sp", "tp")
    in_specs = (
        split,
        split,
        P("sp", None),
        P("sp", None),
        P("sp", None, "tp"),
        P("sp", None, "tp"),
        P("sp", "tp", None),
        split,
        split,
        split,
        P(None, "tp"),
        split,
        split,
        split,
    )
    out_specs = (
        P("sp", None, "tp"),
        P("sp", None, "tp"),
        P("sp", "tp", None),
        split,
        split,
        split,
        split,
        split,
    )
    return jax.shard_map(
        on_device, mesh=mesh, in_specs=in_specs, out_specs=out_specs, check_vma=False
    )
```
